128 devices in a mesh: sp: 16 (over z, x), fs: 4 (over y), tp: 2 (over core).
Axes of the slice: x: 4, y: 4, z: 4, core: 2. Of those that a mesh axis runs over, the one named last changes fastest.
Arguments:
- tokens: bfloat16 [4, 8192, 2048], P('fs', 'sp', 'tp'), may hold values from -6 to 6
- norm_gain: float32 [2048], replicated, may hold values from 0.1 to 1.9
- w_pool_in: bfloat16 [2048, 512], P('fs', 'tp'), may hold values from -0.125 to 0.125
- w_query: bfloat16 [2048, 1024], P('fs', 'tp'), may hold values from -0.125 to 0.125
- w_key: bfloat16 [2048, 1024], P('fs', 'tp'), may hold values from -0.125 to 0.125
- w_value: bfloat16 [2048, 1024], P('fs', 'tp'), may hold values from -0.125 to 0.125
- query_gain: float32 [64], replicated, may hold values from 1.5 to 2.5
- key_gain: float32 [64], replicated, may hold values from 1.5 to 2.5
- stick_offset: float32 [16], P('tp'), as said below
- pool_mix: bfloat16 [4, 128, 128], P('tp'), may hold values from -0.5 to 0.5
- pool_scale: float32 [512], P('tp'), may hold values from 0.2 to 4, as said below
- pool_gain: bfloat16 [512], P('tp'), may hold values from 0.099609375 to 1.8984375
- attn_gain: bfloat16 [1024], P('tp'), may hold values from 0.099609375 to 1.8984375
- w_out_pool: bfloat16 [512, 2048], P('tp', 'fs'), may hold values from -0.15625 to 0.15625
- w_out_attn: bfloat16 [1024, 2048], P('tp', 'fs'), may hold values from -0.15625 to 0.15625
Outputs:
- mixed: bfloat16 [4, 8192, 2048], P('fs', ('sp', 'tp'))
The draws below stay inside these ranges and needn't reach their ends.
Inputs may be any that keep to these rules, and one draw needn't show every extreme that they name: `stick_offset`: per head, negative. `pool_scale`: positive channel scales.
All inputs are finite; a program needn't handle non-finite values.
Results may differ from the reference program's by a relative error of at most 0.013.
Values may be sent and summed in bfloat16 or wider, within the bound.
A program may use at most 192 MiB of HBM per device.

```python
import math
import jax
import jax.numpy as jnp
from jax import lax

D = 2048
HEADS = 16
HEAD_DIM = 64
POOL = 512
POOL_GROUPS = 4
TOK_DEV = 512
ATTN = 1024
LEN = 8192
SEQS = 4


def draw_stick_offset(key, part):
    key_fast = jax.random.fold_in(key, 11)
    key_slow = jax.random.fold_in(key, 12)
    key_quick = jax.random.fold_in(key, 13)
    chosen = jax.random.bernoulli(key_fast, 0.5, (HEADS,))
    slow_value = -(math.log(LEN) + jax.random.uniform(key_slow, (HEADS,), jnp.float32, 4.5, 5.5))
    fast_value = jax.random.uniform(key_quick, (HEADS,), jnp.float32, -8.5, -7.0)
    return jnp.where(chosen, fast_value, slow_value).astype(jnp.float32)


def draw_pool_scale(key, part):
    key_group = jax.random.fold_in(key, 21)
    key_channel = jax.random.fold_in(key, 22)
    group_factor = jnp.exp(jax.random.uniform(key_group, (POOL_GROUPS,), jnp.float32, math.log(0.3), math.log(3.0)))
    channel_factor = 1.0 + 0.18 * jax.random.uniform(key_channel, (POOL_GROUPS, POOL // POOL_GROUPS), jnp.float32, -1.0, 1.0)
    return (group_factor[:, None] * channel_factor).reshape(POOL).astype(jnp.float32)


def shard_levels(stream_key, shape, cuts, low, top_value):
    loudness = 1.0
    for axis_at, parts in cuts:
        heights = jax.random.uniform(jax.random.fold_in(jax.random.fold_in(stream_key, 6), axis_at), (parts,), jnp.float32, low / len(cuts), top_value / len(cuts))
        loudness = loudness * jnp.repeat(jnp.exp(heights), shape[axis_at] // parts).reshape((-1,) + (1,) * (len(shape) - 1 - axis_at))
    return loudness


def noise(rng, dims, width, bound, cuts=(), held_as=jnp.bfloat16):
    level = shard_levels(rng, dims, cuts, -0.22, 0.18) if cuts else 1.0
    values = jax.random.normal(rng, dims, jnp.float32) * width * level
    return jnp.minimum(jnp.maximum(values, -bound), bound).astype(held_as)


def setup_inputs(seed: int = 0) -> dict:
    streams_of = jax.random.split(jax.random.key(seed), 16)
    return {
        "tokens": noise(streams_of[0], (SEQS, LEN, D), 1.0, 6.0, ((0, 4), (1, 16), (2, 2))),
        "norm_gain": jnp.clip(1.0 + 0.18 * jax.random.normal(streams_of[1], (D,), jnp.float32), 0.1, 1.9),
        "w_pool_in": noise(streams_of[2], (D, POOL), D ** -0.5, 0.125, ((0, 4), (1, 2))),
        "w_query": noise(streams_of[3], (D, ATTN), D ** -0.5, 0.125, ((0, 4), (1, 2))),
        "w_key": noise(streams_of[4], (D, ATTN), D ** -0.5, 0.125, ((0, 4), (1, 2))),
        "w_value": noise(streams_of[5], (D, ATTN), D ** -0.5, 0.125, ((0, 4), (1, 2))),
        "query_gain": jnp.clip(jax.random.uniform(streams_of[6], (HEAD_DIM,), jnp.float32, 1.5, 2.5), 1.5, 2.5),
        "key_gain": jnp.clip(jax.random.uniform(streams_of[7], (HEAD_DIM,), jnp.float32, 1.5, 2.5), 1.5, 2.5),
        "stick_offset": draw_stick_offset(jax.random.fold_in(streams_of[15], 71), 0),
        "pool_mix": noise(streams_of[9], (POOL_GROUPS, POOL // POOL_GROUPS, POOL // POOL_GROUPS), (POOL // POOL_GROUPS) ** -0.5, 0.5, ((0, 2),)),
        "pool_scale": draw_pool_scale(jax.random.fold_in(streams_of[15], 71), 0),
        "pool_gain": jnp.clip(1.0 + 0.18 * jax.random.normal(streams_of[11], (POOL,), jnp.float32), 0.099609375, 1.8984375).astype(jnp.bfloat16),
        "attn_gain": jnp.clip(1.0 + 0.18 * jax.random.normal(streams_of[12], (ATTN,), jnp.float32), 0.099609375, 1.8984375).astype(jnp.bfloat16),
        "w_out_pool": noise(streams_of[13], (POOL, D), (POOL + ATTN) ** -0.5, 0.15625, ((0, 2), (1, 4))),
        "w_out_attn": noise(streams_of[14], (ATTN, D), (POOL + ATTN) ** -0.5, 0.15625, ((0, 2), (1, 4))),
    }


EPS = 1e-06
windows = (2, 4, 8, 16)

def row_norm(values_in, gain):
    values_f = values_in.astype(jnp.float32)
    factor = lax.rsqrt(lax.optimization_barrier(jnp.mean(values_f * values_f, axis=-1, keepdims=True)) + EPS)
    return (values_f * factor * gain.astype(jnp.float32)).astype(jnp.bfloat16)

def pool_branch(pool_in, pool_mix, pool_scale):
    group_ch = POOL // POOL_GROUPS
    values_f = pool_in.astype(jnp.float32).reshape(LEN, POOL_GROUPS, group_ch)
    position = jnp.arange(LEN, dtype=jnp.int32)
    pieces = []
    for group, window in enumerate(windows):
        column = values_f[:, group]
        padded = jnp.pad(column, ((window, 0), (0, 0)))
        summed = padded[window:window + LEN]
        for behind in range(1, window):
            summed = summed + padded[window - behind:window - behind + LEN]
        counted = jnp.minimum(position + 1, window).astype(jnp.float32)[:, None]
        pieces.append(summed / counted - column)
    centered = jnp.stack(pieces, axis=1).astype(jnp.bfloat16)
    pooled = jnp.einsum('sgc,gcd->sgd', centered.astype(jnp.float32), pool_mix.astype(jnp.float32))
    return (pooled.reshape(LEN, POOL) * pool_scale).astype(jnp.bfloat16)

def stick_branch(query, key_heads, value_heads, stick_offset):
    block_rows = TOK_DEV
    blocks = LEN // block_rows
    score_scale = 1.0 / math.sqrt(HEAD_DIM)
    query_h = query.transpose(1, 0, 2).reshape(HEADS, blocks, block_rows, HEAD_DIM)
    key_h = key_heads.transpose(1, 0, 2)
    value_h = value_heads.transpose(1, 0, 2)
    key_pos = jnp.arange(LEN, dtype=jnp.int32)

    def per_head(head_args):
        query_blocks, key_one, value_one, offset = head_args

        def per_block(block_args):
            query_block, block_index = block_args
            scores = jnp.dot(query_block, key_one.T, preferred_element_type=jnp.float32) * score_scale + offset
            query_pos = block_index * block_rows + jnp.arange(block_rows, dtype=jnp.int32)
            causal = key_pos[None, :] < query_pos[:, None]
            keep = jnp.where(causal, jax.nn.log_sigmoid(-scores), 0.0)
            running = jnp.cumsum(keep, axis=-1)
            log_weight = jax.nn.log_sigmoid(scores) + running[:, -1:] - running
            weight = jnp.where(causal, jnp.exp(log_weight), 0.0).astype(jnp.bfloat16)
            return jnp.dot(weight, value_one, preferred_element_type=jnp.float32)
        return lax.map(per_block, (query_blocks, jnp.arange(blocks, dtype=jnp.int32)))
    result = lax.map(per_head, (query_h, key_h, value_h, stick_offset))
    result = result.reshape(HEADS, LEN, HEAD_DIM).transpose(1, 0, 2)
    return result.reshape(LEN, ATTN).astype(jnp.bfloat16)

def head_norm(projected, gain):
    split = projected.reshape(LEN, HEADS, HEAD_DIM)
    factor = lax.rsqrt(lax.optimization_barrier(jnp.mean(split * split, axis=-1, keepdims=True)) + EPS)
    return (split * factor * gain).astype(jnp.bfloat16)

def one_sequence(tokens, norm_gain, w_pool_in, w_query, w_key, w_value, query_gain, key_gain, stick_offset, pool_mix, pool_scale, pool_gain, attn_gain, w_out_pool, w_out_attn):
    normed = row_norm(tokens, norm_gain)
    pool_in = jnp.dot(normed, w_pool_in, preferred_element_type=jnp.float32).astype(jnp.bfloat16)
    query = head_norm(jnp.dot(normed, w_query, preferred_element_type=jnp.float32), query_gain)
    key_heads = head_norm(jnp.dot(normed, w_key, preferred_element_type=jnp.float32), key_gain)
    value_heads = jnp.dot(normed, w_value, preferred_element_type=jnp.float32).astype(jnp.bfloat16).reshape(LEN, HEADS, HEAD_DIM)
    pooled = pool_branch(pool_in, pool_mix, pool_scale)
    attended = stick_branch(query, key_heads, value_heads, stick_offset)
    pool_normed = row_norm(pooled, pool_gain)
    attn_normed = row_norm(attended, attn_gain)
    summed = jnp.dot(pool_normed, w_out_pool, preferred_element_type=jnp.float32) + jnp.dot(attn_normed, w_out_attn, preferred_element_type=jnp.float32)
    return summed.astype(jnp.bfloat16)

def reference(tokens, norm_gain, w_pool_in, w_query, w_key, w_value, query_gain, key_gain, stick_offset, pool_mix, pool_scale, pool_gain, attn_gain, w_out_pool, w_out_attn):
    results = []
    for sequence in range(SEQS):
        results.append(one_sequence(tokens[sequence], norm_gain, w_pool_in, w_query, w_key, w_value, query_gain, key_gain, stick_offset, pool_mix, pool_scale, pool_gain, attn_gain, w_out_pool, w_out_attn))
    return jnp.stack(results)
```

```python
import functools
import math

import jax
import jax.numpy as jnp
from jax import lax
from jax.experimental import pallas as pl
from jax.experimental.pallas import tpu as pltpu
from jax.sharding import PartitionSpec as P

HEADS = 16
HEAD_DIM = 64
POOL = 512
POOL_GROUPS = 4
BLOCKS = 16
HALF = 256
BLOCK = 512

EPS = 1e-06
LOG2E = 1.4426950408889634


def sent_to_all(shard, axis):
    devices = lax.axis_size(axis)
    return lax.all_to_all(
        jnp.broadcast_to(shard[None], (devices, *shard.shape)), axis, 0, 0, tiled=True
    )


def in_order(parts, dim):
    lengths = list(parts.shape[1:])
    lengths[dim] *= parts.shape[0]
    return jnp.moveaxis(parts, 0, dim).reshape(lengths)


def gathered_copies(shard, axis, dim):
    parts = sent_to_all(shard, axis)
    return in_order(parts, dim)


def shifted_2(value, axis, steps):
    count = lax.axis_size(axis)
    initial, last = (max(0, -steps), min(count, count - steps))
    return lax.ppermute(value, axis, [(source, source + steps) for source in range(initial, last)])


def branch_norm(values_in, squares, width, gain):
    values_f = values_in.astype(jnp.float32)
    factor = lax.rsqrt(squares / width + EPS)
    return (values_f * factor[:, None] * gain.astype(jnp.float32)).astype(jnp.bfloat16)


def split_terms(value):
    high = value.astype(jnp.bfloat16)
    rest = value - high.astype(jnp.float32)
    middle = rest.astype(jnp.bfloat16)
    low = (rest - middle.astype(jnp.float32)).astype(jnp.bfloat16)
    return (high, middle, low)


def attention_kernel(half_ref, offset_ref, x_ref, o_ref, q_s, k_s, v_s, tri_s, acc_s, carry_s, z0, z1, l0, l1):
    scale = LOG2E / math.sqrt(HEAD_DIM)
    half = half_ref[0]
    offset = offset_ref[0] * math.sqrt(HEAD_DIM)

    row16 = lax.broadcasted_iota(jnp.int32, (64, BLOCK), 0)
    terms = split_terms(jnp.full((64, BLOCK), offset, jnp.float32))
    extra = jnp.where(
        row16 == 0,
        terms[0].astype(jnp.float32),
        jnp.where(
            row16 == 1,
            terms[1].astype(jnp.float32),
            jnp.where(row16 == 2, terms[2].astype(jnp.float32), 0.0),
        ),
    ).astype(jnp.bfloat16)
    lane = lax.broadcasted_iota(jnp.int32, (HALF, 64), 1)
    ones = jnp.where(lane < 3, 1.0, 0.0).astype(jnp.bfloat16)
    tri_s[...] = jnp.where(
        lax.broadcasted_iota(jnp.int32, (HALF, HALF), 0)
        >= lax.broadcasted_iota(jnp.int32, (HALF, HALF), 1),
        1.0,
        0.0,
    ).astype(jnp.bfloat16)

    def prepare(r, unused):
        k_s[r, 0:64, 0:HALF] = x_ref[r, 0:64, :]
        k_s[r, 0:64, HALF:BLOCK] = x_ref[r, 128:192, :]
        k_s[r, 64:128, :] = extra
        v_s[r, 0:HALF, :] = x_ref[r, 64:128, :].astype(jnp.float32).T.astype(jnp.bfloat16)
        v_s[r, HALF:BLOCK, :] = x_ref[r, 192:256, :].astype(jnp.float32).T.astype(jnp.bfloat16)
        q_s[r, :, 0:64] = x_ref[r, 256:320, :].astype(jnp.float32).T.astype(jnp.bfloat16)
        q_s[r, :, 64:128] = ones
        return unused

    lax.fori_loop(0, BLOCKS, prepare, 0)

    def scores(r, g, z_ref, l_ref, masked):
        z = (
            jnp.dot(q_s[r], k_s[g], preferred_element_type=jnp.float32) * scale
        )
        soft = jnp.log2(1.0 + jnp.exp2(z))
        if masked:
            earlier = (
                lax.broadcasted_iota(jnp.int32, (HALF, BLOCK), 1)
                < lax.broadcasted_iota(jnp.int32, (HALF, BLOCK), 0) + half * HALF
            )
            soft = jnp.where(earlier, soft, 0.0)
            z = jnp.where(earlier, z, -1e30)
        z_ref[...] = z
        l_ref[...] = soft.astype(jnp.bfloat16)

    def weigh(r, g, z_ref, l_ref, first):
        late = jnp.dot(l_ref[:, HALF:], tri_s[...], preferred_element_type=jnp.float32)
        early = jnp.dot(l_ref[:, :HALF], tri_s[...], preferred_element_type=jnp.float32)
        late_total = late[:, 0:1]
        early_total = early[:, 0:1]
        if first:
            w_late = jnp.exp2(z_ref[:, HALF:] - late)
            before = late_total
        else:
            carry = carry_s[r][:, 0:1]
            w_late = jnp.exp2(z_ref[:, HALF:] - (late + carry))
            before = carry + late_total
        w_early = jnp.exp2(z_ref[:, :HALF] - (early + before))
        w = jnp.concatenate([w_early.astype(jnp.bfloat16), w_late.astype(jnp.bfloat16)], axis=1)
        out = jnp.dot(w, v_s[g], preferred_element_type=jnp.float32)
        carry_s[r] = jnp.broadcast_to(before + early_total, (HALF, 128))
        if first:
            acc_s[r] = out
        else:
            acc_s[r] = acc_s[r] + out

    scores(0, 0, z0, l0, True)

    def own(n, unused):
        r = 2 * n
        scores(r + 1, r + 1, z1, l1, True)
        weigh(r, r, z0, l0, True)
        after = jnp.minimum(r + 2, BLOCKS - 1)
        scores(after, after, z0, l0, True)
        weigh(r + 1, r + 1, z1, l1, True)
        return unused

    lax.fori_loop(0, BLOCKS // 2, own, 0)

    def advance(state):
        distance, r = state
        over = r == BLOCKS - 1
        distance = jnp.where(over, distance + 1, distance)
        r = jnp.where(over, distance, r + 1)
        fits = r < BLOCKS
        return (jnp.where(fits, distance, BLOCKS - 1), jnp.where(fits, r, BLOCKS - 1))

    start = (jnp.int32(1), jnp.int32(1))
    scores(1, 0, z0, l0, False)

    def earlier_blocks(n, state):
        after = advance(state)
        last = advance(after)
        scores(after[1], after[1] - after[0], z1, l1, False)
        weigh(state[1], state[1] - state[0], z0, l0, False)
        scores(last[1], last[1] - last[0], z0, l0, False)
        weigh(after[1], after[1] - after[0], z1, l1, False)
        return last

    lax.fori_loop(0, BLOCKS * (BLOCKS - 1) // 4, earlier_blocks, start)

    def finish(r, unused):
        o_ref[r] = acc_s[r].T.astype(jnp.bfloat16)
        return unused

    lax.fori_loop(0, BLOCKS, finish, 0)


def attention(half, offset, packed):
    return pl.pallas_call(
        attention_kernel,
        out_shape=jax.ShapeDtypeStruct((BLOCKS, HEAD_DIM, HALF), jnp.bfloat16),
        in_specs=[
            pl.BlockSpec(memory_space=pltpu.SMEM),
            pl.BlockSpec(memory_space=pltpu.SMEM),
            pl.BlockSpec(memory_space=pltpu.VMEM),
        ],
        out_specs=pl.BlockSpec(memory_space=pltpu.VMEM),
        scratch_shapes=[
            pltpu.VMEM((BLOCKS, HALF, 128), jnp.bfloat16),
            pltpu.VMEM((BLOCKS, 128, BLOCK), jnp.bfloat16),
            pltpu.VMEM((BLOCKS, BLOCK, HEAD_DIM), jnp.bfloat16),
            pltpu.VMEM((HALF, HALF), jnp.bfloat16),
            pltpu.VMEM((BLOCKS, HALF, HEAD_DIM), jnp.float32),
            pltpu.VMEM((BLOCKS, HALF, 128), jnp.float32),
            pltpu.VMEM((HALF, BLOCK), jnp.float32),
            pltpu.VMEM((HALF, BLOCK), jnp.float32),
            pltpu.VMEM((HALF, BLOCK), jnp.bfloat16),
            pltpu.VMEM((HALF, BLOCK), jnp.bfloat16),
        ],
        compiler_params=pltpu.CompilerParams(vmem_limit_bytes=48 * 1024 * 1024),
        cost_estimate=pl.CostEstimate(
            flops=40_000_000_000, bytes_accessed=4_000_000, transcendentals=50_000_000
        ),
        name="stick_attention",
    )(half, offset, packed)


def head_norm_t(projected, gain):
    factor = lax.rsqrt(jnp.mean(projected * projected, axis=1, keepdims=True) + EPS)
    return (projected * factor * gain[None, :, None]).astype(jnp.bfloat16)


def pooling(pool_raw, pool_mix, pool_scale):
    row_count, pool_cols = pool_raw.shape
    reach = 16
    pool_in = pool_raw.astype(jnp.bfloat16)
    previous = shifted_2(pool_in[row_count - reach :], "sp", 1)
    extended = jnp.concatenate([previous, pool_in], axis=0).astype(jnp.float32)
    group_ch = POOL // POOL_GROUPS
    local_groups = pool_cols // group_ch
    group_ids = (
        lax.axis_index("tp") * local_groups + jnp.arange(pool_cols, dtype=jnp.int32) // group_ch
    )
    window = jnp.left_shift(jnp.int32(2), group_ids)
    summed = jnp.zeros((row_count, pool_cols), jnp.float32)
    for behind in range(reach):
        shifted = extended[reach - behind : reach - behind + row_count]
        summed = summed + jnp.where(behind < window[None, :], shifted, 0.0)
    sp_index = lax.axis_index("sp")
    position = sp_index * row_count + jnp.arange(row_count, dtype=jnp.int32)
    counted = jnp.minimum(position[:, None] + 1, window[None, :]).astype(jnp.float32)
    centered = (summed / counted - extended[reach:]).astype(jnp.bfloat16)
    pooled = jnp.einsum(
        "tgc,gcd->tgd",
        centered.reshape(row_count, local_groups, group_ch),
        pool_mix,
        preferred_element_type=jnp.float32,
    )
    return (pooled.reshape(row_count, pool_cols) * pool_scale).astype(jnp.bfloat16)


def shards(
    tokens,
    norm_gain,
    w_pool_in,
    w_query,
    w_key,
    w_value,
    query_gain,
    key_gain,
    stick_offset,
    pool_mix,
    pool_scale,
    pool_gain,
    attn_gain,
    w_out_pool,
    w_out_attn,
):
    sp_index = lax.axis_index("sp")
    whole = gathered_copies(tokens, "tp", 2)[0]
    whole_f = whole.astype(jnp.float32)
    normed = (
        whole_f * lax.rsqrt(jnp.mean(whole_f * whole_f, axis=-1, keepdims=True) + EPS) * norm_gain
    ).astype(jnp.bfloat16)
    both = jnp.concatenate((w_query, w_key, w_value, w_pool_in), axis=1)
    weights = lax.all_gather(both, "fs", axis=0, tiled=True)
    pool_raw = jnp.dot(normed, weights[:, 1536:], preferred_element_type=jnp.float32)
    raw = lax.dot_general(
        weights[:, :1536], normed, (((0,), (1,)), ((), ())), preferred_element_type=jnp.float32
    ).reshape(3, 8, HEAD_DIM, BLOCK)
    query = head_norm_t(raw[0], query_gain)
    key = head_norm_t(raw[1], key_gain)
    value = raw[2].astype(jnp.bfloat16)
    key_value = jnp.concatenate(
        [key[:, :, :HALF], value[:, :, :HALF], key[:, :, HALF:], value[:, :, HALF:]], axis=1
    )
    packed = jnp.stack(
        [
            jnp.concatenate([key_value, query[:, :, :HALF]], axis=1),
            jnp.concatenate([key_value, query[:, :, HALF:]], axis=1),
        ],
        axis=1,
    ).reshape(BLOCKS, 5 * HEAD_DIM, HALF)
    packed = lax.all_to_all(packed, "sp", 0, 0, tiled=True)
    offset = lax.dynamic_slice_in_dim(stick_offset, sp_index // 2, 1, 0)
    half = jnp.reshape(sp_index % 2, (1,))
    attended = attention(half, offset, packed)
    attended = lax.all_to_all(attended, "sp", 0, 0, tiled=True)
    attn_out = (
        attended.reshape(8, 2, HEAD_DIM, HALF).transpose(0, 2, 1, 3).reshape(8 * HEAD_DIM, 2, HALF)
    )
    pool_out = pooling(pool_raw, pool_mix, pool_scale)
    w_pool_cols, w_attn_cols = (
        lax.all_gather(w_out_pool, "fs", axis=1, tiled=True),
        lax.all_gather(w_out_attn, "fs", axis=1, tiled=True),
    )
    pool_rows = lax.all_to_all(pool_out, "tp", split_axis=0, concat_axis=1, tiled=True)
    attn_cols = lax.all_to_all(
        jnp.moveaxis(attn_out, 1, 0), "tp", split_axis=0, concat_axis=0, tiled=True
    ).reshape(2 * 8 * HEAD_DIM, HALF)
    w_pool_all, w_attn_all, pool_gain_all, attn_gain_all = (
        lax.all_gather(w_pool_cols, "tp", axis=0, tiled=True),
        lax.all_gather(w_attn_cols, "tp", axis=0, tiled=True),
        lax.all_gather(pool_gain, "tp", axis=0, tiled=True),
        lax.all_gather(attn_gain, "tp", axis=0, tiled=True),
    )
    pool_f = pool_rows.astype(jnp.float32)
    attn_f = attn_cols.astype(jnp.float32)
    pool_normed = branch_norm(pool_rows, jnp.sum(pool_f * pool_f, axis=-1), POOL, pool_gain_all)
    factor = lax.rsqrt(jnp.sum(attn_f * attn_f, axis=0) / (HEADS * HEAD_DIM) + EPS)
    attn_normed = (
        attn_f * factor[None, :] * attn_gain_all.astype(jnp.float32)[:, None]
    ).astype(jnp.bfloat16)
    mixed = jnp.dot(pool_normed, w_pool_all, preferred_element_type=jnp.float32) + lax.dot_general(
        attn_normed, w_attn_all, (((0,), (0,)), ((), ())), preferred_element_type=jnp.float32
    )
    return mixed.astype(jnp.bfloat16)[None]


def solution(mesh):
    in_specs = (
        P("fs", "sp", "tp"),
        P(),
        P("fs", "tp"),
        P("fs", "tp"),
        P("fs", "tp"),
        P("fs", "tp"),
        P(),
        P(),
        P("tp"),
        P("tp", None, None),
        P("tp"),
        P("tp"),
        P("tp"),
        P("tp", "fs"),
        P("tp", "fs"),
    )
    out_specs = P("fs", ("sp", "tp"), None)
    return jax.shard_map(shards, mesh=mesh, in_specs=in_specs, out_specs=out_specs, check_vma=False)
```

```python
import functools
import math

import jax
import jax.numpy as jnp
from jax import lax
from jax.experimental import pallas as pl
from jax.experimental.pallas import tpu as pltpu
from jax.sharding import PartitionSpec as P

HEADS = 16
HEAD_DIM = 64
POOL = 512
POOL_GROUPS = 4
BLOCKS = 16
HALF = 256
BLOCK = 512

EPS = 1e-06
LOG2E = 1.4426950408889634


def shifted_2(value, axis, steps):
    count = lax.axis_size(axis)
    initial, last = (max(0, -steps), min(count, count - steps))
    return lax.ppermute(value, axis, [(source, source + steps) for source in range(initial, last)])


def branch_norm(values_in, squares, width, gain):
    values_f = values_in.astype(jnp.float32)
    factor = lax.rsqrt(squares / width + EPS)
    return (values_f * factor[:, None] * gain.astype(jnp.float32)).astype(jnp.bfloat16)


def split_terms(value):
    high = value.astype(jnp.bfloat16)
    rest = value - high.astype(jnp.float32)
    middle = rest.astype(jnp.bfloat16)
    low = (rest - middle.astype(jnp.float32)).astype(jnp.bfloat16)
    return (high, middle, low)


MESH = pl.DeviceIdType.MESH


def project_kernel(
    tok_ref, gain_ref, wk_ref, wv_ref, wq_ref, wp_ref, kg_ref, qg_ref,
    out_ref, pool_ref,
    buf, pbuf, tok_s, x_s, acc, acc_p, mine, theirs, send, recv,
):
    sp, y, core = lax.axis_index("sp"), lax.axis_index("fs"), lax.axis_index("tp")
    z, x = sp // 4, sp % 4
    y_up, y_down, y_far = (y + 1) % 4, (y + 3) % 4, (y + 2) % 4
    x_up, x_down, x_far = (x + 1) % 4, (x + 3) % 4, (x + 2) % 4
    z_up, z_down, z_far = (z + 1) % 4, (z + 3) % 4, (z + 2) % 4

    def at(z_to, x_to, y_to, core_to):
        return {"sp": z_to * 4 + x_to, "fs": y_to, "tp": core_to}

    partner = at(z, x, y, 1 - core)
    to = {
        "yp": at(z, x, y_up, core), "ym": at(z, x, y_down, core),
        "xp": at(z, x_up, y, core), "xm": at(z, x_down, y, core),
        "zp": at(z_up, x, y, core), "zm": at(z_down, x, y, core),
    }

    barrier = pltpu.get_barrier_semaphore()
    for target in (partner, *to.values()):
        pl.semaphore_signal(barrier, inc=1, device_id=target, device_id_type=MESH)
    pl.semaphore_wait(barrier, 7)

    started = []

    def remote(source, target_ref, index, target):
        return pltpu.make_async_remote_copy(
            src_ref=source, dst_ref=target_ref, send_sem=send.at[index],
            recv_sem=recv.at[index], device_id=target, device_id_type=MESH,
        )

    def go(source, target_ref, index, target):
        copy = remote(source, target_ref, index, target)
        copy.start()
        started.append(copy)

    def got(target_ref, index):
        remote(target_ref, target_ref, index, partner).wait_recv()

    def rows(start, count=64):
        return pl.ds(pl.multiple_of(start, 32), count)

    weights = (wk_ref, wv_ref, wq_ref)
    quarters = (y_down, y_up, y_far)

    def part(a, quarter, start, count=64):
        return buf.at[a, quarter, rows(start, count), :]

    def direct(a):
        base = a * 30
        own_x, own_z = 64 * x, 256 + 64 * z
        w = weights[a]
        go(w.at[rows(own_x), :], part(a, y, own_x), base + 0, to["yp"])
        go(w.at[rows(own_z), :], part(a, y, own_z), base + 1, to["ym"])
        go(w.at[rows(own_x), :], part(a, y, own_x), base + 2, to["ym"])
        go(w.at[rows(own_z), :], part(a, y, own_z), base + 3, to["yp"])

    def ring_base(a, item, ring):
        return a * 30 + 6 + item * 8 + ring * 4

    own_row = (64 * x, 256 + 64 * z)
    down_row = (64 * x_down, 256 + 64 * z_down)
    up_row = (64 * x_up, 256 + 64 * z_up)
    far_row = (64 * x_far, 256 + 64 * z_far)
    ups = ("xp", "zp")
    downs = ("xm", "zm")

    def spread(a, item, ring):
        base = ring_base(a, item, ring)
        piece = part(a, quarters[item], own_row[ring])
        go(piece, piece, base + 0, to[ups[ring]])
        go(piece, piece, base + 1, to[downs[ring]])

    def relay(a, item, ring):
        base = ring_base(a, item, ring)
        q = quarters[item]
        got(part(a, q, down_row[ring]), base + 0)
        piece = part(a, q, down_row[ring], 32)
        go(piece, piece, base + 2, to[ups[ring]])
        got(part(a, q, up_row[ring]), base + 1)
        piece = part(a, q, up_row[ring] + 32, 32)
        go(piece, piece, base + 3, to[downs[ring]])

    def settle(a):
        for item in range(3):
            for ring in range(2):
                base = ring_base(a, item, ring)
                q = quarters[item]
                got(part(a, q, far_row[ring], 32), base + 2)
                got(part(a, q, far_row[ring] + 32, 32), base + 3)

    def first(a):
        base = a * 30
        piece = part(a, y_down, own_row[0])
        got(piece, base + 0)
        go(piece, piece, base + 4, to["yp"])
        spread(a, 0, 0)
        piece = part(a, y_up, own_row[1])
        got(piece, base + 1)
        go(piece, piece, base + 5, to["ym"])
        spread(a, 1, 1)
        got(part(a, y_up, own_row[0]), base + 2)
        spread(a, 1, 0)
        got(part(a, y_down, own_row[1]), base + 3)
        spread(a, 0, 1)

    def second(a):
        relay(a, 0, 0)
        relay(a, 1, 1)

    def third(a):
        base = a * 30
        got(part(a, y_far, own_row[0]), base + 4)
        spread(a, 2, 0)
        got(part(a, y_far, own_row[1]), base + 5)
        spread(a, 2, 1)
        relay(a, 1, 0)
        relay(a, 0, 1)

    def fourth(a):
        relay(a, 2, 0)
        relay(a, 2, 1)

    pool_base = 90

    def pool_direct():
        go(wp_ref, pbuf.at[y], pool_base + 0, to["yp"])
        go(wp_ref, pbuf.at[y], pool_base + 1, to["ym"])

    def pool_relay():
        got(pbuf.at[y_down], pool_base + 0)
        piece = pbuf.at[y_down, 0:256, :]
        go(piece, piece, pool_base + 2, to["yp"])
        got(pbuf.at[y_up], pool_base + 1)
        piece = pbuf.at[y_up, 256:512, :]
        go(piece, piece, pool_base + 3, to["ym"])

    def pool_settle():
        got(pbuf.at[y_far, 0:256, :], pool_base + 2)
        got(pbuf.at[y_far, 256:512, :], pool_base + 3)

    def own(a):
        acc[a] = jnp.dot(x_s[y], weights[a][...], preferred_element_type=jnp.float32)

    def rest(a):
        total = acc[a]
        for q in quarters:
            total = total + jnp.dot(x_s[q], buf[a, q], preferred_element_type=jnp.float32)
        return total

    def deliver(a, total):
        turned = total.T.reshape(8, HEAD_DIM, BLOCK)
        if a != 1:
            factor = lax.rsqrt(jnp.mean(turned * turned, axis=1, keepdims=True) + EPS)
            gain = (kg_ref if a == 0 else qg_ref)[...]
            turned = turned * factor * gain[None]
        turned = turned.astype(jnp.bfloat16)
        is_first = core == 0
        low, high = turned[:, :, :HALF], turned[:, :, HALF:]
        out_ref[pl.ds(8 * core, 8), a * 64 : a * 64 + 64, :] = jnp.where(is_first, low, high)
        theirs[a] = jnp.where(is_first, high, low)
        go(
            theirs.at[a],
            out_ref.at[pl.ds(8 * core, 8), a * 64 : a * 64 + 64, :],
            95 + a,
            partner,
        )

    go(tok_ref, tok_s, 94, partner)
    direct(0)
    direct(1)
    got(tok_s, 94)

    mine_f = tok_ref[...].astype(jnp.float32)
    other_f = tok_s[...].astype(jnp.float32)
    squares = jnp.sum(mine_f * mine_f, axis=1, keepdims=True) + jnp.sum(
        other_f * other_f, axis=1, keepdims=True
    )
    factor = lax.rsqrt(squares / 2048.0 + EPS)
    for j in range(2):
        columns = slice(512 * j, 512 * j + 512)
        at_mine = 2 * core + j
        at_other = 2 * (1 - core) + j
        x_s[at_mine] = (
            tok_ref[:, columns].astype(jnp.float32) * factor * gain_ref[at_mine]
        ).astype(jnp.bfloat16)
        x_s[at_other] = (
            tok_s[:, columns].astype(jnp.float32) * factor * gain_ref[at_other]
        ).astype(jnp.bfloat16)

    first(0)
    direct(2)
    own(0)
    second(0)
    first(1)
    pool_direct()
    own(1)
    third(0)
    second(1)
    first(2)
    own(2)
    fourth(0)
    third(1)
    second(2)
    pool_relay()
    acc_p[...] = jnp.dot(x_s[y], wp_ref[...], preferred_element_type=jnp.float32)
    fourth(1)
    third(2)
    settle(0)
    deliver(0, rest(0))
    fourth(2)
    settle(1)
    deliver(1, rest(1))
    settle(2)
    deliver(2, rest(2))
    pool_settle()
    total = acc_p[...]
    for q in quarters:
        total = total + jnp.dot(x_s[q], pbuf[q], preferred_element_type=jnp.float32)
    pool_ref[...] = total.astype(jnp.bfloat16)
    for a in range(3):
        got(out_ref.at[pl.ds(8 * (1 - core), 8), a * 64 : a * 64 + 64, :], 95 + a)
    for copy in started:
        copy.wait_send()


def project(tokens, norm_gain, wk, wv, wq, wp, key_gain, query_gain):
    vmem = pl.BlockSpec(memory_space=pltpu.VMEM)
    return pl.pallas_call(
        project_kernel,
        out_shape=(
            jax.ShapeDtypeStruct((HEADS, 3 * HEAD_DIM, HALF), jnp.bfloat16),
            jax.ShapeDtypeStruct((BLOCK, 256), jnp.bfloat16),
        ),
        in_specs=[vmem] * 8,
        out_specs=(vmem, vmem),
        scratch_shapes=[
            pltpu.VMEM((3, 4, 512, 512), jnp.bfloat16),
            pltpu.VMEM((4, 512, 256), jnp.bfloat16),
            pltpu.VMEM((512, 1024), jnp.bfloat16),
            pltpu.VMEM((4, 512, 512), jnp.bfloat16),
            pltpu.VMEM((3, 512, 512), jnp.float32),
            pltpu.VMEM((512, 256), jnp.float32),
            pltpu.VMEM((8, 128), jnp.float32),
            pltpu.VMEM((3, 8, HEAD_DIM, HALF), jnp.bfloat16),
            pltpu.SemaphoreType.DMA((98,)),
            pltpu.SemaphoreType.DMA((98,)),
        ],
        compiler_params=pltpu.CompilerParams(
            collective_id=0, has_side_effects=True, vmem_limit_bytes=56 * 1024 * 1024
        ),
        cost_estimate=pl.CostEstimate(
            flops=4_000_000_000, bytes_accessed=6_000_000, transcendentals=10_000
        ),
        name="gather_project",
    )(
        tokens, norm_gain.reshape(4, 1, 512), wk, wv, wq, wp,
        key_gain.reshape(HEAD_DIM, 1), query_gain.reshape(HEAD_DIM, 1),
    )


def attention_kernel(
    offset_ref, x_ref, wp_ref, wa_ref, gains_ref,
    o_ref, wp_all, wa_all, gains_all,
    offset_s, other_s, q_s, k_s, v_s, tri_s, acc_s, carry_s, z0, z1, l0, l1, send, recv,
):
    sp, y, core = lax.axis_index("sp"), lax.axis_index("fs"), lax.axis_index("tp")
    y_up, y_down, y_far = (y + 1) % 4, (y + 3) % 4, (y + 2) % 4
    partner = {"sp": sp, "fs": y, "tp": 1 - core}
    up = {"sp": sp, "fs": y_up, "tp": core}
    down = {"sp": sp, "fs": y_down, "tp": core}
    barrier = pltpu.get_barrier_semaphore()
    for target in (partner, up, down):
        pl.semaphore_signal(barrier, inc=1, device_id=target, device_id_type=MESH)
    pl.semaphore_wait(barrier, 3)
    started = []

    def remote(source, target_ref, index, target):
        return pltpu.make_async_remote_copy(
            src_ref=source, dst_ref=target_ref, send_sem=send.at[index],
            recv_sem=recv.at[index], device_id=target, device_id_type=MESH,
        )

    def go(source, target_ref, index, target):
        copy = remote(source, target_ref, index, target)
        copy.start()
        started.append(copy)

    def got(target_ref, index):
        remote(target_ref, target_ref, index, partner).wait_recv()

    def wa_part(quarter, of_core, start, count):
        return wa_all.at[
            pl.ds(pl.multiple_of(of_core * 512 + start, 128), count),
            pl.ds(pl.multiple_of(quarter * 512, 512), 512),
        ]

    def wp_part(quarter, of_core, start, count):
        return wp_all.at[
            pl.ds(pl.multiple_of(of_core * 256 + start, 128), count),
            pl.ds(pl.multiple_of(quarter * 512, 512), 512),
        ]

    def share(quarter, index):
        go(wa_part(quarter, core, 0, 512), wa_part(quarter, core, 0, 512), index, partner)
        go(wp_part(quarter, core, 0, 256), wp_part(quarter, core, 0, 256), index + 1, partner)

    def shared(quarter, index):
        got(wa_part(quarter, 1 - core, 0, 512), index)
        got(wp_part(quarter, 1 - core, 0, 256), index + 1)

    def weights_start():
        go(wa_ref, wa_part(y, core, 0, 512), 2, up)
        go(wp_ref, wp_part(y, core, 0, 256), 3, up)
        go(wa_ref, wa_part(y, core, 0, 512), 4, down)
        go(wp_ref, wp_part(y, core, 0, 256), 5, down)
        go(wa_ref, wa_part(y, core, 0, 512), 10, partner)
        go(wp_ref, wp_part(y, core, 0, 256), 11, partner)

    def weights_middle():
        got(wa_part(y_down, core, 0, 512), 2)
        got(wp_part(y_down, core, 0, 256), 3)
        go(wa_part(y_down, core, 0, 256), wa_part(y_down, core, 0, 256), 6, up)
        go(wp_part(y_down, core, 0, 128), wp_part(y_down, core, 0, 128), 7, up)
        got(wa_part(y_up, core, 0, 512), 4)
        got(wp_part(y_up, core, 0, 256), 5)
        go(wa_part(y_up, core, 256, 256), wa_part(y_up, core, 256, 256), 8, down)
        go(wp_part(y_up, core, 128, 128), wp_part(y_up, core, 128, 128), 9, down)
        share(y_down, 12)
        share(y_up, 14)

    def weights_late():
        got(wa_part(y_far, core, 0, 256), 6)
        got(wp_part(y_far, core, 0, 128), 7)
        got(wa_part(y_far, core, 256, 256), 8)
        got(wp_part(y_far, core, 128, 128), 9)
        share(y_far, 16)

    def weights_end():
        shared(y, 10)
        shared(y_down, 12)
        shared(y_up, 14)
        shared(y_far, 16)

    go(offset_ref, offset_s, 18, partner)
    keys_values = x_ref.at[:, 0:128, :]
    go(keys_values, other_s, 0, partner)
    go(gains_ref, gains_all.at[pl.ds(pl.multiple_of(16 * core, 16), 16), :], 1, partner)
    weights_start()
    wa_part(y, core, 0, 512)[...] = wa_ref[...]
    wp_part(y, core, 0, 256)[...] = wp_ref[...]
    gains_all[pl.ds(pl.multiple_of(16 * core, 16), 16), :] = gains_ref[...]

    scale = LOG2E / math.sqrt(HEAD_DIM)
    half = core
    got(offset_s, 18)
    of_head = jnp.where(sp // 8 == core, offset_ref[pl.ds(sp % 8, 1), :], offset_s[pl.ds(sp % 8, 1), :])
    offset = of_head[:, 0:1] * math.sqrt(HEAD_DIM)

    row16 = lax.broadcasted_iota(jnp.int32, (64, BLOCK), 0)
    terms = split_terms(jnp.broadcast_to(offset, (64, BLOCK)))
    extra = jnp.where(
        row16 == 0,
        terms[0].astype(jnp.float32),
        jnp.where(
            row16 == 1,
            terms[1].astype(jnp.float32),
            jnp.where(row16 == 2, terms[2].astype(jnp.float32), 0.0),
        ),
    ).astype(jnp.bfloat16)
    lane = lax.broadcasted_iota(jnp.int32, (HALF, 64), 1)
    ones = jnp.where(lane < 3, 1.0, 0.0).astype(jnp.bfloat16)
    tri_s[...] = jnp.where(
        lax.broadcasted_iota(jnp.int32, (HALF, HALF), 0)
        >= lax.broadcasted_iota(jnp.int32, (HALF, HALF), 1),
        1.0,
        0.0,
    ).astype(jnp.bfloat16)

    mine_at = pl.ds(pl.multiple_of(core * HALF, HALF), HALF)
    other_at = pl.ds(pl.multiple_of((1 - core) * HALF, HALF), HALF)

    def turned(block):
        return block.astype(jnp.float32).T.astype(jnp.bfloat16)

    def prepare(r, unused):
        k_s[r, 0:64, mine_at] = x_ref[r, 0:64, :]
        k_s[r, 64:128, :] = extra
        v_s[r, mine_at, :] = turned(x_ref[r, 64:128, :])
        q_s[r, :, 0:64] = turned(x_ref[r, 128:192, :])
        q_s[r, :, 64:128] = ones
        return unused

    lax.fori_loop(0, BLOCKS, prepare, 0)
    got(other_s, 0)

    def complete(r, unused):
        k_s[r, 0:64, other_at] = other_s[r, 0:64, :]
        v_s[r, other_at, :] = turned(other_s[r, 64:128, :])
        return unused

    lax.fori_loop(0, BLOCKS, complete, 0)

    def scores(r, g, z_ref, l_ref, masked):
        z = (
            jnp.dot(q_s[r], k_s[g], preferred_element_type=jnp.float32) * scale
        )
        soft = jnp.log2(1.0 + jnp.exp2(z))
        if masked:
            earlier = (
                lax.broadcasted_iota(jnp.int32, (HALF, BLOCK), 1)
                < lax.broadcasted_iota(jnp.int32, (HALF, BLOCK), 0) + half * HALF
            )
            soft = jnp.where(earlier, soft, 0.0)
            z = jnp.where(earlier, z, -1e30)
        z_ref[...] = z
        l_ref[...] = soft.astype(jnp.bfloat16)

    def weigh(r, g, z_ref, l_ref, first):
        late = jnp.dot(l_ref[:, HALF:], tri_s[...], preferred_element_type=jnp.float32)
        early = jnp.dot(l_ref[:, :HALF], tri_s[...], preferred_element_type=jnp.float32)
        late_total = late[:, 0:1]
        early_total = early[:, 0:1]
        if first:
            w_late = jnp.exp2(z_ref[:, HALF:] - late)
            before = late_total
        else:
            carry = carry_s[r][:, 0:1]
            w_late = jnp.exp2(z_ref[:, HALF:] - (late + carry))
            before = carry + late_total
        w_early = jnp.exp2(z_ref[:, :HALF] - (early + before))
        w = jnp.concatenate([w_early.astype(jnp.bfloat16), w_late.astype(jnp.bfloat16)], axis=1)
        out = jnp.dot(w, v_s[g], preferred_element_type=jnp.float32)
        carry_s[r] = jnp.broadcast_to(before + early_total, (HALF, 128))
        if first:
            acc_s[r] = out
        else:
            acc_s[r] = acc_s[r] + out

    scores(0, 0, z0, l0, True)

    def own(n, unused):
        r = 2 * n
        scores(r + 1, r + 1, z1, l1, True)
        weigh(r, r, z0, l0, True)
        after = jnp.minimum(r + 2, BLOCKS - 1)
        scores(after, after, z0, l0, True)
        weigh(r + 1, r + 1, z1, l1, True)
        return unused

    lax.fori_loop(0, BLOCKS // 2, own, 0)

    def advance(state):
        distance, r = state
        over = r == BLOCKS - 1
        distance = jnp.where(over, distance + 1, distance)
        r = jnp.where(over, distance, r + 1)
        fits = r < BLOCKS
        return (jnp.where(fits, distance, BLOCKS - 1), jnp.where(fits, r, BLOCKS - 1))

    start = (jnp.int32(1), jnp.int32(1))
    scores(1, 0, z0, l0, False)

    def earlier_blocks(n, state):
        after = advance(state)
        last = advance(after)
        scores(after[1], after[1] - after[0], z1, l1, False)
        weigh(state[1], state[1] - state[0], z0, l0, False)
        scores(last[1], last[1] - last[0], z0, l0, False)
        weigh(after[1], after[1] - after[0], z1, l1, False)
        return last

    state = lax.fori_loop(0, 28, earlier_blocks, start)
    weights_middle()
    state = lax.fori_loop(28, 46, earlier_blocks, state)
    weights_late()
    lax.fori_loop(46, BLOCKS * (BLOCKS - 1) // 4, earlier_blocks, state)

    def finish(r, unused):
        o_ref[r] = acc_s[r].T.astype(jnp.bfloat16)
        return unused

    lax.fori_loop(0, BLOCKS, finish, 0)
    weights_end()
    got(gains_all.at[pl.ds(pl.multiple_of(16 * (1 - core), 16), 16), :], 1)
    for copy in started:
        copy.wait_send()


def attention(offset, packed, w_pool, w_attn, gains):
    vmem = pl.BlockSpec(memory_space=pltpu.VMEM)
    return pl.pallas_call(
        attention_kernel,
        out_shape=(
            jax.ShapeDtypeStruct((BLOCKS, HEAD_DIM, HALF), jnp.bfloat16),
            jax.ShapeDtypeStruct((512, 2048), jnp.bfloat16),
            jax.ShapeDtypeStruct((1024, 2048), jnp.bfloat16),
            jax.ShapeDtypeStruct((32, 768), jnp.bfloat16),
        ),
        in_specs=[vmem] * 5,
        out_specs=(vmem, vmem, vmem, vmem),
        scratch_shapes=[
            pltpu.VMEM((8, 128), jnp.float32),
            pltpu.VMEM((BLOCKS, 128, HALF), jnp.bfloat16),
            pltpu.VMEM((BLOCKS, HALF, 128), jnp.bfloat16),
            pltpu.VMEM((BLOCKS, 128, BLOCK), jnp.bfloat16),
            pltpu.VMEM((BLOCKS, BLOCK, HEAD_DIM), jnp.bfloat16),
            pltpu.VMEM((HALF, HALF), jnp.bfloat16),
            pltpu.VMEM((BLOCKS, HALF, HEAD_DIM), jnp.float32),
            pltpu.VMEM((BLOCKS, HALF, 128), jnp.float32),
            pltpu.VMEM((HALF, BLOCK), jnp.float32),
            pltpu.VMEM((HALF, BLOCK), jnp.float32),
            pltpu.VMEM((HALF, BLOCK), jnp.bfloat16),
            pltpu.VMEM((HALF, BLOCK), jnp.bfloat16),
            pltpu.SemaphoreType.DMA((19,)),
            pltpu.SemaphoreType.DMA((19,)),
        ],
        compiler_params=pltpu.CompilerParams(
            collective_id=1, has_side_effects=True, vmem_limit_bytes=56 * 1024 * 1024
        ),
        cost_estimate=pl.CostEstimate(
            flops=40_000_000_000, bytes_accessed=4_000_000, transcendentals=50_000_000
        ),
        name="stick_attention",
    )(offset, packed, w_pool, w_attn, gains)


def pooling(pool_in, pool_mix, pool_scale):
    row_count, pool_cols = pool_in.shape
    reach = 16
    previous = shifted_2(pool_in[row_count - reach :], "sp", 1)
    extended = jnp.concatenate([previous, pool_in], axis=0).astype(jnp.float32)
    group_ch = POOL // POOL_GROUPS
    local_groups = pool_cols // group_ch
    group_ids = (
        lax.axis_index("tp") * local_groups + jnp.arange(pool_cols, dtype=jnp.int32) // group_ch
    )
    window = jnp.left_shift(jnp.int32(2), group_ids)
    summed = jnp.zeros((row_count, pool_cols), jnp.float32)
    for behind in range(reach):
        shifted = extended[reach - behind : reach - behind + row_count]
        summed = summed + jnp.where(behind < window[None, :], shifted, 0.0)
    sp_index = lax.axis_index("sp")
    position = sp_index * row_count + jnp.arange(row_count, dtype=jnp.int32)
    counted = jnp.minimum(position[:, None] + 1, window[None, :]).astype(jnp.float32)
    centered = (summed / counted - extended[reach:]).astype(jnp.bfloat16)
    pooled = jnp.einsum(
        "tgc,gcd->tgd",
        centered.reshape(row_count, local_groups, group_ch),
        pool_mix,
        preferred_element_type=jnp.float32,
    )
    return (pooled.reshape(row_count, pool_cols) * pool_scale).astype(jnp.bfloat16)


def shards(
    tokens,
    norm_gain,
    w_pool_in,
    w_query,
    w_key,
    w_value,
    query_gain,
    key_gain,
    stick_offset,
    pool_mix,
    pool_scale,
    pool_gain,
    attn_gain,
    w_out_pool,
    w_out_attn,
):
    packed, pool_in = project(
        tokens[0], norm_gain, w_key, w_value, w_query, w_pool_in, key_gain, query_gain
    )
    packed = lax.all_to_all(packed, "sp", 0, 0, tiled=True)
    offset = jnp.broadcast_to(stick_offset[:, None], (8, 128))
    gains = jnp.broadcast_to(jnp.concatenate([pool_gain, attn_gain])[None], (16, 768))
    attended, w_pool_all, w_attn_all, gains_all = attention(
        offset, packed, w_out_pool, w_out_attn, gains
    )
    attended = lax.all_to_all(attended, "sp", 0, 0, tiled=True).reshape(HEADS * HEAD_DIM, HALF)
    pool_out = pooling(pool_in, pool_mix, pool_scale)
    pool_rows = lax.all_to_all(pool_out, "tp", split_axis=0, concat_axis=1, tiled=True)
    pool_gain_all = jnp.concatenate([gains_all[0, :256], gains_all[16, :256]])
    attn_gain_all = jnp.concatenate([gains_all[0, 256:], gains_all[16, 256:]])
    pool_f = pool_rows.astype(jnp.float32)
    attn_f = attended.astype(jnp.float32)
    pool_normed = branch_norm(pool_rows, jnp.sum(pool_f * pool_f, axis=-1), POOL, pool_gain_all)
    factor = lax.rsqrt(jnp.sum(attn_f * attn_f, axis=0) / (HEADS * HEAD_DIM) + EPS)
    attn_normed = (
        attn_f * factor[None, :] * attn_gain_all.astype(jnp.float32)[:, None]
    ).astype(jnp.bfloat16)
    mixed = jnp.dot(pool_normed, w_pool_all, preferred_element_type=jnp.float32) + lax.dot_general(
        attn_normed, w_attn_all, (((0,), (0,)), ((), ())), preferred_element_type=jnp.float32
    )
    return mixed.astype(jnp.bfloat16)[None]


def solution(mesh):
    in_specs = (
        P("fs", "sp", "tp"),
        P(),
        P("fs", "tp"),
        P("fs", "tp"),
        P("fs", "tp"),
        P("fs", "tp"),
        P(),
        P(),
        P("tp"),
        P("tp", None, None),
        P("tp"),
        P("tp"),
        P("tp"),
        P("tp", "fs"),
        P("tp", "fs"),
    )
    out_specs = P("fs", ("sp", "tp"), None)
    return jax.shard_map(shards, mesh=mesh, in_specs=in_specs, out_specs=out_specs, check_vma=False)
```

```python
import functools
import math

import jax
import jax.numpy as jnp
from jax import lax
from jax.experimental import pallas as pl
from jax.experimental.pallas import tpu as pltpu
from jax.sharding import PartitionSpec as P

HEADS = 16
HEAD_DIM = 64
POOL = 512
POOL_GROUPS = 4
BLOCKS = 16
HALF = 256
BLOCK = 512

EPS = 1e-06
LOG2E = 1.4426950408889634


def shifted_2(value, axis, steps):
    count = lax.axis_size(axis)
    initial, last = (max(0, -steps), min(count, count - steps))
    return lax.ppermute(value, axis, [(source, source + steps) for source in range(initial, last)])


def branch_norm(values_in, squares, width, gain):
    values_f = values_in.astype(jnp.float32)
    factor = lax.rsqrt(squares / width + EPS)
    return (values_f * factor[:, None] * gain.astype(jnp.float32)).astype(jnp.bfloat16)


def split_terms(value):
    high = value.astype(jnp.bfloat16)
    rest = value - high.astype(jnp.float32)
    middle = rest.astype(jnp.bfloat16)
    low = (rest - middle.astype(jnp.float32)).astype(jnp.bfloat16)
    return (high, middle, low)


MESH = pl.DeviceIdType.MESH


def project_kernel(
    tok_ref, gain_ref, wk_ref, wv_ref, wq_ref, wp_ref, kg_ref, qg_ref,
    out_ref, pool_ref,
    buf, pbuf, tok_s, x_s, acc, acc_p, mine, theirs, send, recv,
):
    sp, y, core = lax.axis_index("sp"), lax.axis_index("fs"), lax.axis_index("tp")
    z, x = sp // 4, sp % 4
    y_up, y_down, y_far = (y + 1) % 4, (y + 3) % 4, (y + 2) % 4
    x_up, x_down, x_far = (x + 1) % 4, (x + 3) % 4, (x + 2) % 4
    z_up, z_down, z_far = (z + 1) % 4, (z + 3) % 4, (z + 2) % 4

    def at(z_to, x_to, y_to, core_to):
        return {"sp": z_to * 4 + x_to, "fs": y_to, "tp": core_to}

    partner = at(z, x, y, 1 - core)
    to = {
        "yp": at(z, x, y_up, core), "ym": at(z, x, y_down, core),
        "xp": at(z, x_up, y, core), "xm": at(z, x_down, y, core),
        "zp": at(z_up, x, y, core), "zm": at(z_down, x, y, core),
    }

    barrier = pltpu.get_barrier_semaphore()
    for target in (partner, *to.values()):
        pl.semaphore_signal(barrier, inc=1, device_id=target, device_id_type=MESH)
    pl.semaphore_wait(barrier, 7)

    started = []

    def remote(source, target_ref, index, target):
        return pltpu.make_async_remote_copy(
            src_ref=source, dst_ref=target_ref, send_sem=send.at[index],
            recv_sem=recv.at[index], device_id=target, device_id_type=MESH,
        )

    def go(source, target_ref, index, target):
        copy = remote(source, target_ref, index, target)
        copy.start()
        started.append(copy)

    def got(target_ref, index):
        remote(target_ref, target_ref, index, partner).wait_recv()

    def rows(start, count=64):
        return pl.ds(pl.multiple_of(start, 32), count)

    weights = (wk_ref, wv_ref, wq_ref)
    quarters = (y_down, y_up, y_far)

    def part(a, quarter, start, count=64):
        return buf.at[a, quarter, rows(start, count), :]

    def direct(a):
        base = a * 30
        own_x, own_z = 64 * x, 256 + 64 * z
        w = weights[a]
        go(w.at[rows(own_x), :], part(a, y, own_x), base + 0, to["yp"])
        go(w.at[rows(own_z), :], part(a, y, own_z), base + 1, to["ym"])
        go(w.at[rows(own_x), :], part(a, y, own_x), base + 2, to["ym"])
        go(w.at[rows(own_z), :], part(a, y, own_z), base + 3, to["yp"])

    def ring_base(a, item, ring):
        return a * 30 + 6 + item * 8 + ring * 4

    own_row = (64 * x, 256 + 64 * z)
    down_row = (64 * x_down, 256 + 64 * z_down)
    up_row = (64 * x_up, 256 + 64 * z_up)
    far_row = (64 * x_far, 256 + 64 * z_far)
    ups = ("xp", "zp")
    downs = ("xm", "zm")

    def spread(a, item, ring):
        base = ring_base(a, item, ring)
        piece = part(a, quarters[item], own_row[ring])
        go(piece, piece, base + 0, to[ups[ring]])
        go(piece, piece, base + 1, to[downs[ring]])

    def relay(a, item, ring):
        base = ring_base(a, item, ring)
        q = quarters[item]
        got(part(a, q, down_row[ring]), base + 0)
        piece = part(a, q, down_row[ring], 32)
        go(piece, piece, base + 2, to[ups[ring]])
        got(part(a, q, up_row[ring]), base + 1)
        piece = part(a, q, up_row[ring] + 32, 32)
        go(piece, piece, base + 3, to[downs[ring]])

    def settle(a):
        for item in range(3):
            for ring in range(2):
                base = ring_base(a, item, ring)
                q = quarters[item]
                got(part(a, q, far_row[ring], 32), base + 2)
                got(part(a, q, far_row[ring] + 32, 32), base + 3)

    def first(a):
        base = a * 30
        piece = part(a, y_down, own_row[0])
        got(piece, base + 0)
        go(piece, piece, base + 4, to["yp"])
        spread(a, 0, 0)
        piece = part(a, y_up, own_row[1])
        got(piece, base + 1)
        go(piece, piece, base + 5, to["ym"])
        spread(a, 1, 1)
        got(part(a, y_up, own_row[0]), base + 2)
        spread(a, 1, 0)
        got(part(a, y_down, own_row[1]), base + 3)
        spread(a, 0, 1)

    def second(a):
        relay(a, 0, 0)
        relay(a, 1, 1)

    def third(a):
        base = a * 30
        got(part(a, y_far, own_row[0]), base + 4)
        spread(a, 2, 0)
        got(part(a, y_far, own_row[1]), base + 5)
        spread(a, 2, 1)
        relay(a, 1, 0)
        relay(a, 0, 1)

    def fourth(a):
        relay(a, 2, 0)
        relay(a, 2, 1)

    pool_base = 90

    def pool_direct():
        go(wp_ref, pbuf.at[y], pool_base + 0, to["yp"])
        go(wp_ref, pbuf.at[y], pool_base + 1, to["ym"])

    def pool_relay():
        got(pbuf.at[y_down], pool_base + 0)
        piece = pbuf.at[y_down, 0:256, :]
        go(piece, piece, pool_base + 2, to["yp"])
        got(pbuf.at[y_up], pool_base + 1)
        piece = pbuf.at[y_up, 256:512, :]
        go(piece, piece, pool_base + 3, to["ym"])

    def pool_settle():
        got(pbuf.at[y_far, 0:256, :], pool_base + 2)
        got(pbuf.at[y_far, 256:512, :], pool_base + 3)

    def own(a):
        acc[a] = jnp.dot(x_s[y], weights[a][...], preferred_element_type=jnp.float32)

    def rest(a):
        total = acc[a]
        for q in quarters:
            total = total + jnp.dot(x_s[q], buf[a, q], preferred_element_type=jnp.float32)
        return total

    def deliver(a, total):
        turned = total.T.reshape(8, HEAD_DIM, BLOCK)
        if a != 1:
            factor = lax.rsqrt(jnp.mean(turned * turned, axis=1, keepdims=True) + EPS)
            gain = (kg_ref if a == 0 else qg_ref)[...]
            turned = turned * factor * gain[None]
        turned = turned.astype(jnp.bfloat16)
        is_first = core == 0
        low, high = turned[:, :, :HALF], turned[:, :, HALF:]
        out_ref[pl.ds(8 * core, 8), a * 64 : a * 64 + 64, :] = jnp.where(is_first, low, high)
        theirs[a] = jnp.where(is_first, high, low)
        go(
            theirs.at[a],
            out_ref.at[pl.ds(8 * core, 8), a * 64 : a * 64 + 64, :],
            95 + a,
            partner,
        )

    go(tok_ref, tok_s, 94, partner)
    direct(0)
    direct(1)
    got(tok_s, 94)

    mine_f = tok_ref[...].astype(jnp.float32)
    other_f = tok_s[...].astype(jnp.float32)
    squares = jnp.sum(mine_f * mine_f, axis=1, keepdims=True) + jnp.sum(
        other_f * other_f, axis=1, keepdims=True
    )
    factor = lax.rsqrt(squares / 2048.0 + EPS)
    for j in range(2):
        columns = slice(512 * j, 512 * j + 512)
        at_mine = 2 * core + j
        at_other = 2 * (1 - core) + j
        x_s[at_mine] = (
            tok_ref[:, columns].astype(jnp.float32) * factor * gain_ref[at_mine]
        ).astype(jnp.bfloat16)
        x_s[at_other] = (
            tok_s[:, columns].astype(jnp.float32) * factor * gain_ref[at_other]
        ).astype(jnp.bfloat16)

    first(0)
    direct(2)
    own(0)
    second(0)
    first(1)
    pool_direct()
    own(1)
    third(0)
    second(1)
    first(2)
    own(2)
    fourth(0)
    third(1)
    second(2)
    pool_relay()
    acc_p[...] = jnp.dot(x_s[y], wp_ref[...], preferred_element_type=jnp.float32)
    fourth(1)
    third(2)
    settle(0)
    deliver(0, rest(0))
    fourth(2)
    settle(1)
    deliver(1, rest(1))
    settle(2)
    deliver(2, rest(2))
    pool_settle()
    total = acc_p[...]
    for q in quarters:
        total = total + jnp.dot(x_s[q], pbuf[q], preferred_element_type=jnp.float32)
    pool_ref[...] = total.astype(jnp.bfloat16)
    for a in range(3):
        got(out_ref.at[pl.ds(8 * (1 - core), 8), a * 64 : a * 64 + 64, :], 95 + a)
    for copy in started:
        copy.wait_send()


def project(tokens, norm_gain, wk, wv, wq, wp, key_gain, query_gain):
    vmem = pl.BlockSpec(memory_space=pltpu.VMEM)
    return pl.pallas_call(
        project_kernel,
        out_shape=(
            jax.ShapeDtypeStruct((HEADS, 3 * HEAD_DIM, HALF), jnp.bfloat16),
            jax.ShapeDtypeStruct((BLOCK, 256), jnp.bfloat16),
        ),
        in_specs=[vmem] * 8,
        out_specs=(vmem, vmem),
        scratch_shapes=[
            pltpu.VMEM((3, 4, 512, 512), jnp.bfloat16),
            pltpu.VMEM((4, 512, 256), jnp.bfloat16),
            pltpu.VMEM((512, 1024), jnp.bfloat16),
            pltpu.VMEM((4, 512, 512), jnp.bfloat16),
            pltpu.VMEM((3, 512, 512), jnp.float32),
            pltpu.VMEM((512, 256), jnp.float32),
            pltpu.VMEM((8, 128), jnp.float32),
            pltpu.VMEM((3, 8, HEAD_DIM, HALF), jnp.bfloat16),
            pltpu.SemaphoreType.DMA((98,)),
            pltpu.SemaphoreType.DMA((98,)),
        ],
        compiler_params=pltpu.CompilerParams(
            collective_id=0, has_side_effects=True, vmem_limit_bytes=56 * 1024 * 1024
        ),
        cost_estimate=pl.CostEstimate(
            flops=4_000_000_000, bytes_accessed=6_000_000, transcendentals=10_000
        ),
        name="gather_project",
    )(
        tokens, norm_gain.reshape(4, 1, 512), wk, wv, wq, wp,
        key_gain.reshape(HEAD_DIM, 1), query_gain.reshape(HEAD_DIM, 1),
    )


def attention_kernel(
    offset_ref, x_ref, wp_ref, wa_ref, gains_ref,
    o_ref, wp_all, wa_all, gains_all,
    offset_s, other_s, q_s, k_s, v_s, tri_s, mask_s, acc_s, carry_s, done_s,
    z0, z1, z2, l0, l1, l2, w0, w1, w2, send, recv,
):
    sp, y, core = lax.axis_index("sp"), lax.axis_index("fs"), lax.axis_index("tp")
    y_up, y_down, y_far = (y + 1) % 4, (y + 3) % 4, (y + 2) % 4
    partner = {"sp": sp, "fs": y, "tp": 1 - core}
    up = {"sp": sp, "fs": y_up, "tp": core}
    down = {"sp": sp, "fs": y_down, "tp": core}

    def owner(block):
        return {"sp": block, "fs": y, "tp": core}

    barrier = pltpu.get_barrier_semaphore()
    for target in (partner, up, down):
        pl.semaphore_signal(barrier, inc=1, device_id=target, device_id_type=MESH)

    def greet(i, unused):
        pl.semaphore_signal(
            barrier, inc=1, device_id=owner((sp + i) % BLOCKS), device_id_type=MESH
        )
        return unused

    lax.fori_loop(1, BLOCKS, greet, 0)
    pl.semaphore_wait(barrier, 18)
    started = []

    def remote(source, target_ref, index, target):
        return pltpu.make_async_remote_copy(
            src_ref=source, dst_ref=target_ref, send_sem=send.at[index],
            recv_sem=recv.at[index], device_id=target, device_id_type=MESH,
        )

    def go(source, target_ref, index, target):
        copy = remote(source, target_ref, index, target)
        copy.start()
        started.append(copy)

    def got(target_ref, index):
        remote(target_ref, target_ref, index, partner).wait_recv()

    def wa_part(quarter, of_core, start, count):
        return wa_all.at[
            pl.ds(pl.multiple_of(of_core * 512 + start, 128), count),
            pl.ds(pl.multiple_of(quarter * 512, 512), 512),
        ]

    def wp_part(quarter, of_core, start, count):
        return wp_all.at[
            pl.ds(pl.multiple_of(of_core * 256 + start, 128), count),
            pl.ds(pl.multiple_of(quarter * 512, 512), 512),
        ]

    def share(quarter, index):
        go(wa_part(quarter, core, 0, 512), wa_part(quarter, core, 0, 512), index, partner)
        go(wp_part(quarter, core, 0, 256), wp_part(quarter, core, 0, 256), index + 1, partner)

    def shared(quarter, index):
        got(wa_part(quarter, 1 - core, 0, 512), index)
        got(wp_part(quarter, 1 - core, 0, 256), index + 1)

    def weights_start():
        go(wa_ref, wa_part(y, core, 0, 512), 2, up)
        go(wp_ref, wp_part(y, core, 0, 256), 3, up)
        go(wa_ref, wa_part(y, core, 0, 512), 4, down)
        go(wp_ref, wp_part(y, core, 0, 256), 5, down)
        go(wa_ref, wa_part(y, core, 0, 512), 10, partner)
        go(wp_ref, wp_part(y, core, 0, 256), 11, partner)

    def weights_middle():
        got(wa_part(y_down, core, 0, 512), 2)
        got(wp_part(y_down, core, 0, 256), 3)
        go(wa_part(y_down, core, 0, 256), wa_part(y_down, core, 0, 256), 6, up)
        go(wp_part(y_down, core, 0, 128), wp_part(y_down, core, 0, 128), 7, up)
        got(wa_part(y_up, core, 0, 512), 4)
        got(wp_part(y_up, core, 0, 256), 5)
        go(wa_part(y_up, core, 256, 256), wa_part(y_up, core, 256, 256), 8, down)
        go(wp_part(y_up, core, 128, 128), wp_part(y_up, core, 128, 128), 9, down)
        share(y_down, 12)
        share(y_up, 14)

    def weights_late():
        got(wa_part(y_far, core, 0, 256), 6)
        got(wp_part(y_far, core, 0, 128), 7)
        got(wa_part(y_far, core, 256, 256), 8)
        got(wp_part(y_far, core, 128, 128), 9)
        share(y_far, 16)

    def weights_end():
        shared(y, 10)
        shared(y_down, 12)
        shared(y_up, 14)
        shared(y_far, 16)

    go(offset_ref, offset_s, 18, partner)
    keys_values = x_ref.at[:, 0:128, :]
    go(keys_values, other_s, 0, partner)
    go(gains_ref, gains_all.at[pl.ds(pl.multiple_of(16 * core, 16), 16), :], 1, partner)
    weights_start()
    wa_part(y, core, 0, 512)[...] = wa_ref[...]
    wp_part(y, core, 0, 256)[...] = wp_ref[...]
    gains_all[pl.ds(pl.multiple_of(16 * core, 16), 16), :] = gains_ref[...]

    scale = LOG2E / math.sqrt(HEAD_DIM)
    half = core
    got(offset_s, 18)
    of_head = jnp.where(sp // 8 == core, offset_ref[pl.ds(sp % 8, 1), :], offset_s[pl.ds(sp % 8, 1), :])
    offset = of_head[:, 0:1] * math.sqrt(HEAD_DIM)

    column = lax.broadcasted_iota(jnp.int32, (BLOCK, 64), 1)
    terms = split_terms(jnp.broadcast_to(offset, (BLOCK, 64)))
    extra = jnp.where(
        column == 0,
        terms[0].astype(jnp.float32),
        jnp.where(
            column == 1,
            terms[1].astype(jnp.float32),
            jnp.where(column == 2, terms[2].astype(jnp.float32), 0.0),
        ),
    ).astype(jnp.bfloat16)
    row = lax.broadcasted_iota(jnp.int32, (64, HALF), 0)
    ones = jnp.where(row < 3, 1.0, 0.0).astype(jnp.bfloat16)
    tri_s[...] = jnp.where(
        lax.broadcasted_iota(jnp.int32, (HALF, HALF), 0)
        <= lax.broadcasted_iota(jnp.int32, (HALF, HALF), 1),
        1.0,
        0.0,
    ).astype(jnp.bfloat16)
    mask_s[...] = jnp.where(
        lax.broadcasted_iota(jnp.int32, (BLOCK, HALF), 0)
        < lax.broadcasted_iota(jnp.int32, (BLOCK, HALF), 1) + half * HALF,
        0.0,
        -1e30,
    )
    acc_s[...] = jnp.zeros_like(acc_s)
    carry_s[...] = jnp.zeros_like(carry_s)

    mine_at = pl.ds(pl.multiple_of(core * HALF, HALF), HALF)
    other_at = pl.ds(pl.multiple_of((1 - core) * HALF, HALF), HALF)

    def turned(block):
        return block.astype(jnp.float32).T.astype(jnp.bfloat16)

    mine_rows = pl.ds(pl.multiple_of(core * HALF, HALF), HALF)
    other_rows = pl.ds(pl.multiple_of((1 - core) * HALF, HALF), HALF)

    def prepare(n, unused):
        for r in (2 * n, 2 * n + 1):
            k_s[r, mine_rows, 0:64] = turned(x_ref[r, 0:64, :])
            k_s[r, :, 64:128] = extra
            v_s[r, :, mine_at] = x_ref[r, 64:128, :]
            q_s[r, 0:64, :] = x_ref[r, 128:192, :]
            q_s[r, 64:128, :] = ones
        return unused

    lax.fori_loop(0, BLOCKS // 2, prepare, 0)
    got(other_s, 0)

    def complete(n, unused):
        for r in (2 * n, 2 * n + 1):
            k_s[r, other_rows, 0:64] = turned(other_s[r, 0:64, :])
            v_s[r, :, other_at] = other_s[r, 64:128, :]
        return unused

    lax.fori_loop(0, BLOCKS // 2, complete, 0)

    zs, ls, ws = (z0, z1, z2), (l0, l1, l2), (w0, w1, w2)

    def places(state):
        distance, r = state
        r_in = jnp.clip(r, 0, BLOCKS - 1)
        row_at = jnp.where((r < 0) | (r >= BLOCKS), BLOCKS, r)
        return (row_at, r_in, jnp.clip(r_in - distance, 0, BLOCKS - 1))

    def advance(state):
        distance, r = state
        over = r == BLOCKS - 1
        distance = jnp.where(over, distance + 1, distance)
        return (distance, jnp.where(over, distance, r + 1))

    def scores(state, b, masked):
        unused_row, r, g = places(state)
        z = jnp.dot(k_s[g], q_s[r], preferred_element_type=jnp.float32) * scale
        if masked:
            z = z + mask_s[...]
        zs[b][...] = z

    def soften(b):
        ls[b][...] = jnp.log2(1.0 + jnp.exp2(zs[b][...])).astype(jnp.bfloat16)

    def weigh(state, b):
        row_at = places(state)[0]
        late = jnp.dot(tri_s[...], ls[b][HALF:, :], preferred_element_type=jnp.float32)
        early = jnp.dot(tri_s[...], ls[b][:HALF, :], preferred_element_type=jnp.float32)
        carry = carry_s[row_at][0:1]
        before = carry + late[0:1]
        ws[b][HALF:, :] = jnp.exp2(zs[b][HALF:, :] - (late + carry)).astype(jnp.bfloat16)
        ws[b][:HALF, :] = jnp.exp2(zs[b][:HALF, :] - (early + before)).astype(jnp.bfloat16)
        carry_s[row_at] = jnp.broadcast_to(before + early[0:1], (8, HALF))

    def gather_values(state, b):
        row_at, unused_row, g = places(state)
        acc_s[row_at] = acc_s[row_at] + jnp.dot(
            v_s[g], ws[b][...], preferred_element_type=jnp.float32
        )

    def steps(masked):
        def body(n, states):
            states = list(states)
            for unused_step in range(6):
                states.append(advance(states[-1]))
            for u in range(6):
                gather_values(states[u], (u + 2) % 3)
                weigh(states[u + 1], u % 3)
                soften((u + 1) % 3)
                scores(states[u + 3], (u + 2) % 3, masked)
            return tuple(states[6:])

        return body

    def return_rows(low, high):
        def send_row(r, unused):
            done_s[r] = acc_s[r].astype(jnp.bfloat16)

            @pl.when(r != sp)
            def _():
                pltpu.make_async_remote_copy(
                    src_ref=done_s.at[r], dst_ref=o_ref.at[sp], send_sem=send.at[19 + r],
                    recv_sem=recv.at[19 + sp], device_id=owner(r), device_id_type=MESH,
                ).start()

            return unused

        lax.fori_loop(low, high, send_row, 0)

    first = tuple((jnp.int32(0), jnp.int32(r)) for r in (-5, -4, -3, -2))
    states = lax.fori_loop(0, 3, steps(True), first)
    states = lax.fori_loop(0, 8, steps(False), states)
    weights_middle()
    states = lax.fori_loop(8, 14, steps(False), states)
    weights_late()
    return_rows(0, 8)
    states = lax.fori_loop(14, 19, steps(False), states)
    return_rows(8, 13)
    states = lax.fori_loop(19, 21, steps(False), states)
    return_rows(13, 16)
    o_ref[sp] = done_s[sp]
    weights_end()
    got(gains_all.at[pl.ds(pl.multiple_of(16 * (1 - core), 16), 16), :], 1)
    for copy in started:
        copy.wait_send()

    def settle_row(i, unused):
        r = (sp + i) % BLOCKS
        copy = pltpu.make_async_remote_copy(
            src_ref=done_s.at[r], dst_ref=o_ref.at[r], send_sem=send.at[19 + r],
            recv_sem=recv.at[19 + r], device_id=owner(r), device_id_type=MESH,
        )
        copy.wait_send()
        copy.wait_recv()
        return unused

    lax.fori_loop(1, BLOCKS, settle_row, 0)


def attention(offset, packed, w_pool, w_attn, gains):
    vmem = pl.BlockSpec(memory_space=pltpu.VMEM)
    return pl.pallas_call(
        attention_kernel,
        out_shape=(
            jax.ShapeDtypeStruct((BLOCKS, HEAD_DIM, HALF), jnp.bfloat16),
            jax.ShapeDtypeStruct((512, 2048), jnp.bfloat16),
            jax.ShapeDtypeStruct((1024, 2048), jnp.bfloat16),
            jax.ShapeDtypeStruct((32, 768), jnp.bfloat16),
        ),
        in_specs=[vmem] * 5,
        out_specs=(vmem, vmem, vmem, vmem),
        scratch_shapes=[
            pltpu.VMEM((8, 128), jnp.float32),
            pltpu.VMEM((BLOCKS, 128, HALF), jnp.bfloat16),
            pltpu.VMEM((BLOCKS, 128, HALF), jnp.bfloat16),
            pltpu.VMEM((BLOCKS, BLOCK, 128), jnp.bfloat16),
            pltpu.VMEM((BLOCKS, HEAD_DIM, BLOCK), jnp.bfloat16),
            pltpu.VMEM((HALF, HALF), jnp.bfloat16),
            pltpu.VMEM((BLOCK, HALF), jnp.float32),
            pltpu.VMEM((BLOCKS + 1, HEAD_DIM, HALF), jnp.float32),
            pltpu.VMEM((BLOCKS + 1, 8, HALF), jnp.float32),
            pltpu.VMEM((BLOCKS, HEAD_DIM, HALF), jnp.bfloat16),
            *[pltpu.VMEM((BLOCK, HALF), jnp.float32)] * 3,
            *[pltpu.VMEM((BLOCK, HALF), jnp.bfloat16)] * 6,
            pltpu.SemaphoreType.DMA((35,)),
            pltpu.SemaphoreType.DMA((35,)),
        ],
        compiler_params=pltpu.CompilerParams(
            collective_id=1, has_side_effects=True, vmem_limit_bytes=56 * 1024 * 1024
        ),
        cost_estimate=pl.CostEstimate(
            flops=40_000_000_000, bytes_accessed=4_000_000, transcendentals=50_000_000
        ),
        name="stick_attention",
    )(offset, packed, w_pool, w_attn, gains)


def pooling(pool_in, pool_mix, pool_scale):
    row_count, pool_cols = pool_in.shape
    reach = 16
    previous = shifted_2(pool_in[row_count - reach :], "sp", 1)
    extended = jnp.concatenate([previous, pool_in], axis=0).astype(jnp.float32)
    group_ch = POOL // POOL_GROUPS
    local_groups = pool_cols // group_ch
    group_ids = (
        lax.axis_index("tp") * local_groups + jnp.arange(pool_cols, dtype=jnp.int32) // group_ch
    )
    window = jnp.left_shift(jnp.int32(2), group_ids)
    summed = jnp.zeros((row_count, pool_cols), jnp.float32)
    for behind in range(reach):
        shifted = extended[reach - behind : reach - behind + row_count]
        summed = summed + jnp.where(behind < window[None, :], shifted, 0.0)
    sp_index = lax.axis_index("sp")
    position = sp_index * row_count + jnp.arange(row_count, dtype=jnp.int32)
    counted = jnp.minimum(position[:, None] + 1, window[None, :]).astype(jnp.float32)
    centered = (summed / counted - extended[reach:]).astype(jnp.bfloat16)
    pooled = jnp.einsum(
        "tgc,gcd->tgd",
        centered.reshape(row_count, local_groups, group_ch),
        pool_mix,
        preferred_element_type=jnp.float32,
    )
    return (pooled.reshape(row_count, pool_cols) * pool_scale).astype(jnp.bfloat16)


def shards(
    tokens,
    norm_gain,
    w_pool_in,
    w_query,
    w_key,
    w_value,
    query_gain,
    key_gain,
    stick_offset,
    pool_mix,
    pool_scale,
    pool_gain,
    attn_gain,
    w_out_pool,
    w_out_attn,
):
    packed, pool_in = project(
        tokens[0], norm_gain, w_key, w_value, w_query, w_pool_in, key_gain, query_gain
    )
    packed = lax.all_to_all(packed, "sp", 0, 0, tiled=True)
    offset = jnp.broadcast_to(stick_offset[:, None], (8, 128))
    gains = jnp.broadcast_to(jnp.concatenate([pool_gain, attn_gain])[None], (16, 768))
    attended, w_pool_all, w_attn_all, gains_all = attention(
        offset, packed, w_out_pool, w_out_attn, gains
    )
    attended = attended.reshape(HEADS * HEAD_DIM, HALF)
    pool_out = pooling(pool_in, pool_mix, pool_scale)
    pool_rows = lax.all_to_all(pool_out, "tp", split_axis=0, concat_axis=1, tiled=True)
    pool_gain_all = jnp.concatenate([gains_all[0, :256], gains_all[16, :256]])
    attn_gain_all = jnp.concatenate([gains_all[0, 256:], gains_all[16, 256:]])
    pool_f = pool_rows.astype(jnp.float32)
    attn_f = attended.astype(jnp.float32)
    pool_normed = branch_norm(pool_rows, jnp.sum(pool_f * pool_f, axis=-1), POOL, pool_gain_all)
    factor = lax.rsqrt(jnp.sum(attn_f * attn_f, axis=0) / (HEADS * HEAD_DIM) + EPS)
    attn_normed = (
        attn_f * factor[None, :] * attn_gain_all.astype(jnp.float32)[:, None]
    ).astype(jnp.bfloat16)
    mixed = jnp.dot(pool_normed, w_pool_all, preferred_element_type=jnp.float32) + lax.dot_general(
        attn_normed, w_attn_all, (((0,), (0,)), ((), ())), preferred_element_type=jnp.float32
    )
    return mixed.astype(jnp.bfloat16)[None]


def solution(mesh):
    in_specs = (
        P("fs", "sp", "tp"),
        P(),
        P("fs", "tp"),
        P("fs", "tp"),
        P("fs", "tp"),
        P("fs", "tp"),
        P(),
        P(),
        P("tp"),
        P("tp", None, None),
        P("tp"),
        P("tp"),
        P("tp"),
        P("tp", "fs"),
        P("tp", "fs"),
    )
    out_specs = P("fs", ("sp", "tp"), None)
    return jax.shard_map(shards, mesh=mesh, in_specs=in_specs, out_specs=out_specs, check_vma=False)
```

```python
import math

import jax
import jax.numpy as jnp
from jax import lax
from jax.experimental import pallas as pl
from jax.experimental.pallas import tpu as pltpu
from jax.sharding import PartitionSpec as P

HEADS = 16
HEAD_DIM = 64
POOL = 512
POOL_GROUPS = 4
BLOCKS = 16
HALF = 256
BLOCK = 512

EPS = 1e-06
LOG2E = 1.4426950408889634


def branch_norm(values_in, squares, width, gain):
    values_f = values_in.astype(jnp.float32)
    factor = lax.rsqrt(squares / width + EPS)
    return (values_f * factor[:, None] * gain.astype(jnp.float32)).astype(jnp.bfloat16)


def split_terms(value):
    high = value.astype(jnp.bfloat16)
    rest = value - high.astype(jnp.float32)
    middle = rest.astype(jnp.bfloat16)
    low = (rest - middle.astype(jnp.float32)).astype(jnp.bfloat16)
    return (high, middle, low)


MESH = pl.DeviceIdType.MESH


def project_kernel(
    tok_ref, gain_ref, wk_ref, wv_ref, wq_ref, wp_ref, kg_ref, qg_ref, mix_ref, scale_ref,
    out_ref, pool_ref,
    buf, pbuf, tok_s, x_s, acc, acc_p, heads_s, pool_in, before_s, pooled_s, send, recv,
):
    sp, y, core = lax.axis_index("sp"), lax.axis_index("fs"), lax.axis_index("tp")
    z, x = sp // 4, sp % 4
    y_up, y_down, y_far = (y + 1) % 4, (y + 3) % 4, (y + 2) % 4
    x_up, x_down, x_far = (x + 1) % 4, (x + 3) % 4, (x + 2) % 4
    z_up, z_down, z_far = (z + 1) % 4, (z + 3) % 4, (z + 2) % 4

    def at(z_to, x_to, y_to, core_to):
        return {"sp": z_to * 4 + x_to, "fs": y_to, "tp": core_to}

    partner = at(z, x, y, 1 - core)
    to = {
        "yp": at(z, x, y_up, core), "ym": at(z, x, y_down, core),
        "xp": at(z, x_up, y, core), "xm": at(z, x_down, y, core),
        "zp": at(z_up, x, y, core), "zm": at(z_down, x, y, core),
    }

    barrier = pltpu.get_barrier_semaphore()
    for target in (partner, to["yp"], to["ym"]):
        pl.semaphore_signal(barrier, inc=1, device_id=target, device_id_type=MESH)

    def greet(i, unused):
        for of_core in range(2):
            pl.semaphore_signal(
                barrier, inc=1, device_id={"sp": (sp + i) % BLOCKS, "fs": y, "tp": of_core},
                device_id_type=MESH,
            )
        return unused

    lax.fori_loop(1, BLOCKS, greet, 0)
    pl.semaphore_wait(barrier, 33)

    started = []

    def remote(source, target_ref, index, target):
        return pltpu.make_async_remote_copy(
            src_ref=source, dst_ref=target_ref, send_sem=send.at[index],
            recv_sem=recv.at[index], device_id=target, device_id_type=MESH,
        )

    def go(source, target_ref, index, target):
        copy = remote(source, target_ref, index, target)
        copy.start()
        started.append(copy)

    def got(target_ref, index):
        remote(target_ref, target_ref, index, partner).wait_recv()

    def rows(start, count=64):
        return pl.ds(pl.multiple_of(start, 32), count)

    weights = (wk_ref, wv_ref, wq_ref)
    quarters = (y_down, y_up, y_far)

    def part(a, quarter, start, count=64):
        return buf.at[a, quarter, rows(start, count), :]

    def direct(a):
        base = a * 30
        own_x, own_z = 64 * x, 256 + 64 * z
        w = weights[a]
        go(w.at[rows(own_x), :], part(a, y, own_x), base + 0, to["yp"])
        go(w.at[rows(own_z), :], part(a, y, own_z), base + 1, to["ym"])
        go(w.at[rows(own_x), :], part(a, y, own_x), base + 2, to["ym"])
        go(w.at[rows(own_z), :], part(a, y, own_z), base + 3, to["yp"])

    def ring_base(a, item, ring):
        return a * 30 + 6 + item * 8 + ring * 4

    own_row = (64 * x, 256 + 64 * z)
    down_row = (64 * x_down, 256 + 64 * z_down)
    up_row = (64 * x_up, 256 + 64 * z_up)
    far_row = (64 * x_far, 256 + 64 * z_far)
    ups = ("xp", "zp")
    downs = ("xm", "zm")

    def spread(a, item, ring):
        base = ring_base(a, item, ring)
        piece = part(a, quarters[item], own_row[ring])
        go(piece, piece, base + 0, to[ups[ring]])
        go(piece, piece, base + 1, to[downs[ring]])

    def relay(a, item, ring):
        base = ring_base(a, item, ring)
        q = quarters[item]
        got(part(a, q, down_row[ring]), base + 0)
        piece = part(a, q, down_row[ring], 32)
        go(piece, piece, base + 2, to[ups[ring]])
        got(part(a, q, up_row[ring]), base + 1)
        piece = part(a, q, up_row[ring] + 32, 32)
        go(piece, piece, base + 3, to[downs[ring]])

    def settle(a):
        for item in range(3):
            for ring in range(2):
                base = ring_base(a, item, ring)
                q = quarters[item]
                got(part(a, q, far_row[ring], 32), base + 2)
                got(part(a, q, far_row[ring] + 32, 32), base + 3)

    def first(a):
        base = a * 30
        piece = part(a, y_down, own_row[0])
        got(piece, base + 0)
        go(piece, piece, base + 4, to["yp"])
        spread(a, 0, 0)
        piece = part(a, y_up, own_row[1])
        got(piece, base + 1)
        go(piece, piece, base + 5, to["ym"])
        spread(a, 1, 1)
        got(part(a, y_up, own_row[0]), base + 2)
        spread(a, 1, 0)
        got(part(a, y_down, own_row[1]), base + 3)
        spread(a, 0, 1)

    def second(a):
        relay(a, 0, 0)
        relay(a, 1, 1)

    def third(a):
        base = a * 30
        got(part(a, y_far, own_row[0]), base + 4)
        spread(a, 2, 0)
        got(part(a, y_far, own_row[1]), base + 5)
        spread(a, 2, 1)
        relay(a, 1, 0)
        relay(a, 0, 1)

    def fourth(a):
        relay(a, 2, 0)
        relay(a, 2, 1)

    pool_base = 90

    def pool_direct():
        go(wp_ref, pbuf.at[y], pool_base + 0, to["yp"])
        go(wp_ref, pbuf.at[y], pool_base + 1, to["ym"])

    def pool_relay():
        got(pbuf.at[y_down], pool_base + 0)
        piece = pbuf.at[y_down, 0:256, :]
        go(piece, piece, pool_base + 2, to["yp"])
        got(pbuf.at[y_up], pool_base + 1)
        piece = pbuf.at[y_up, 256:512, :]
        go(piece, piece, pool_base + 3, to["ym"])

    def pool_settle():
        got(pbuf.at[y_far, 0:256, :], pool_base + 2)
        got(pbuf.at[y_far, 256:512, :], pool_base + 3)

    def own(a):
        acc[a] = jnp.dot(x_s[y], weights[a][...], preferred_element_type=jnp.float32)

    def rest(a):
        total = acc[a]
        for q in quarters:
            total = total + jnp.dot(x_s[q], buf[a, q], preferred_element_type=jnp.float32)
        return total

    def head_copy(a, i, source):
        h, of_core = (sp + i // 2) % 8, i % 2
        return pltpu.make_async_remote_copy(
            src_ref=heads_s.at[a, h, of_core],
            dst_ref=out_ref.at[source, a * 64 : a * 64 + 64, :],
            send_sem=send.at[97 + a * 16 + i], recv_sem=recv.at[97 + a * 16 + source],
            device_id={"sp": 8 * core + h, "fs": y, "tp": of_core}, device_id_type=MESH,
        )

    stays = sp // 8 == core

    def deliver(a, total):
        turned = total.T.reshape(8, HEAD_DIM, BLOCK)
        if a != 1:
            factor = lax.rsqrt(jnp.mean(turned * turned, axis=1, keepdims=True) + EPS)
            gain_row = (kg_ref if a == 0 else qg_ref)[...]
            gain = jnp.broadcast_to(gain_row, (HEAD_DIM, HEAD_DIM)).T[:, 0:1]
            turned = turned * factor * gain[None]
        turned = turned.astype(jnp.bfloat16)
        heads_s[a, :, 0] = turned[:, :, :HALF]
        heads_s[a, :, 1] = turned[:, :, HALF:]

        def send_head(i, unused):
            @pl.when(jnp.logical_not(stays & (i == core)))
            def _():
                head_copy(a, i, sp).start()

            return unused

        lax.fori_loop(0, 16, send_head, 0)

        @pl.when(stays)
        def _():
            out_ref[sp, a * 64 : a * 64 + 64, :] = heads_s[a, sp % 8, core]

    def delivered(a):
        def wait_head(i, unused):
            @pl.when(jnp.logical_not(stays & (i == core)))
            def _():
                head_copy(a, i, sp).wait_send()

            @pl.when(jnp.logical_not(stays & (i == sp)))
            def _():
                head_copy(a, 0, i).wait_recv()

            return unused

        lax.fori_loop(0, 16, wait_head, 0)

    go(tok_ref, tok_s, 94, partner)
    direct(0)
    direct(1)
    got(tok_s, 94)

    mine_f = tok_ref[...].astype(jnp.float32)
    other_f = tok_s[...].astype(jnp.float32)
    squares = jnp.sum(mine_f * mine_f, axis=1, keepdims=True) + jnp.sum(
        other_f * other_f, axis=1, keepdims=True
    )
    factor = lax.rsqrt(squares / 2048.0 + EPS)
    for j in range(2):
        columns = slice(512 * j, 512 * j + 512)
        at_mine = 2 * core + j
        at_other = 2 * (1 - core) + j
        x_s[at_mine] = (
            tok_ref[:, columns].astype(jnp.float32) * factor * gain_ref[at_mine]
        ).astype(jnp.bfloat16)
        x_s[at_other] = (
            tok_s[:, columns].astype(jnp.float32) * factor * gain_ref[at_other]
        ).astype(jnp.bfloat16)

    first(0)
    direct(2)
    own(0)
    second(0)
    first(1)
    pool_direct()
    own(1)
    third(0)
    second(1)
    first(2)
    own(2)
    fourth(0)
    third(1)
    second(2)
    pool_relay()
    acc_p[...] = jnp.dot(x_s[y], wp_ref[...], preferred_element_type=jnp.float32)
    fourth(1)
    third(2)
    settle(0)
    deliver(0, rest(0))
    fourth(2)
    settle(1)
    deliver(1, rest(1))
    settle(2)
    deliver(2, rest(2))
    pool_settle()
    total = acc_p[...]
    for q in quarters:
        total = total + jnp.dot(x_s[q], pbuf[q], preferred_element_type=jnp.float32)
    pool_in[...] = total.astype(jnp.bfloat16)
    tail = pool_in.at[BLOCK - 16 : BLOCK, :]
    go(tail, before_s, 95, {"sp": (sp + 1) % BLOCKS, "fs": y, "tp": core})
    current = pool_in[...].astype(jnp.float32)
    got(before_s, 95)
    before = jnp.where(sp == 0, 0.0, before_s[...].astype(jnp.float32))

    def behind(values, count):
        return jnp.concatenate([jnp.zeros((count, values.shape[1]), jnp.float32), values[:-count]], axis=0)

    extended = jnp.concatenate([before, current], axis=0)
    sum_2 = extended + behind(extended, 1)
    sum_4 = sum_2 + behind(sum_2, 2)
    sum_8 = sum_4 + behind(sum_4, 4)
    sum_16 = sum_8 + behind(sum_8, 8)
    position = lax.broadcasted_iota(jnp.int32, (BLOCK, 128), 0) + (sp * BLOCK + 1)
    for group in range(2):
        columns = slice(128 * group, 128 * group + 128)
        low, high = ((sum_2, sum_8), (sum_4, sum_16))[group]
        window = jnp.where(core == 0, 2 << group, 8 << group)
        summed = jnp.where(core == 0, low[16:, columns], high[16:, columns])
        counted = jnp.minimum(position, window).astype(jnp.float32)
        centered = (summed / counted - current[:, columns]).astype(jnp.bfloat16)
        mixed = jnp.dot(centered, mix_ref[group], preferred_element_type=jnp.float32)
        pooled_s[:, columns] = (mixed * scale_ref[:, columns]).astype(jnp.bfloat16)
    mine_rows = pl.ds(pl.multiple_of(core * HALF, HALF), HALF)
    other_rows = pl.ds(pl.multiple_of((1 - core) * HALF, HALF), HALF)
    go(pooled_s.at[other_rows, :], pool_ref.at[core], 96, partner)
    pool_ref[core] = pooled_s[mine_rows, :]
    got(pool_ref.at[1 - core], 96)
    for a in range(3):
        delivered(a)
    for copy in started:
        copy.wait_send()


def project(tokens, norm_gain, wk, wv, wq, wp, key_gain, query_gain, pool_mix, pool_scale):
    vmem = pl.BlockSpec(memory_space=pltpu.VMEM)
    return pl.pallas_call(
        project_kernel,
        out_shape=(
            jax.ShapeDtypeStruct((HEADS, 3 * HEAD_DIM, HALF), jnp.bfloat16),
            jax.ShapeDtypeStruct((2, HALF, 256), jnp.bfloat16),
        ),
        in_specs=[vmem] * 10,
        out_specs=(vmem, vmem),
        scratch_shapes=[
            pltpu.VMEM((3, 4, 512, 512), jnp.bfloat16),
            pltpu.VMEM((4, 512, 256), jnp.bfloat16),
            pltpu.VMEM((512, 1024), jnp.bfloat16),
            pltpu.VMEM((4, 512, 512), jnp.bfloat16),
            pltpu.VMEM((3, 512, 512), jnp.float32),
            pltpu.VMEM((512, 256), jnp.float32),
            pltpu.VMEM((3, 8, 2, HEAD_DIM, HALF), jnp.bfloat16),
            pltpu.VMEM((512, 256), jnp.bfloat16),
            pltpu.VMEM((16, 256), jnp.bfloat16),
            pltpu.VMEM((512, 256), jnp.bfloat16),
            pltpu.SemaphoreType.DMA((145,)),
            pltpu.SemaphoreType.DMA((145,)),
        ],
        compiler_params=pltpu.CompilerParams(
            collective_id=0, has_side_effects=True, vmem_limit_bytes=56 * 1024 * 1024
        ),
        cost_estimate=pl.CostEstimate(
            flops=4_000_000_000, bytes_accessed=6_000_000, transcendentals=10_000
        ),
        name="gather_project",
    )(
        tokens, norm_gain.reshape(4, 1, 512), wk, wv, wq, wp,
        key_gain.reshape(1, HEAD_DIM), query_gain.reshape(1, HEAD_DIM), pool_mix,
        pool_scale.reshape(1, 256),
    )


def attention_kernel(
    offset_ref, x_ref, wp_ref, wa_ref, pg_ref, ag_ref,
    o_ref, wp_all, wa_all, gains_all,
    offset_s, offset_m, gains_m, other_s, q_s, k_s, v_s, tri_s, mask_s, acc_s, carry_s, done_s,
    z0, z1, z2, l0, l1, l2, w0, w1, w2, send, recv,
):
    sp, y, core = lax.axis_index("sp"), lax.axis_index("fs"), lax.axis_index("tp")
    y_up, y_down, y_far = (y + 1) % 4, (y + 3) % 4, (y + 2) % 4
    partner = {"sp": sp, "fs": y, "tp": 1 - core}
    up = {"sp": sp, "fs": y_up, "tp": core}
    down = {"sp": sp, "fs": y_down, "tp": core}

    def owner(block):
        return {"sp": block, "fs": y, "tp": core}

    barrier = pltpu.get_barrier_semaphore()
    for target in (partner, up, down):
        pl.semaphore_signal(barrier, inc=1, device_id=target, device_id_type=MESH)

    def greet(i, unused):
        pl.semaphore_signal(
            barrier, inc=1, device_id=owner((sp + i) % BLOCKS), device_id_type=MESH
        )
        return unused

    lax.fori_loop(1, BLOCKS, greet, 0)
    pl.semaphore_wait(barrier, 18)
    started = []

    def remote(source, target_ref, index, target):
        return pltpu.make_async_remote_copy(
            src_ref=source, dst_ref=target_ref, send_sem=send.at[index],
            recv_sem=recv.at[index], device_id=target, device_id_type=MESH,
        )

    def go(source, target_ref, index, target):
        copy = remote(source, target_ref, index, target)
        copy.start()
        started.append(copy)

    def got(target_ref, index):
        remote(target_ref, target_ref, index, partner).wait_recv()

    def wa_part(quarter, of_core, start, count):
        return wa_all.at[
            pl.ds(pl.multiple_of(of_core * 512 + start, 128), count),
            pl.ds(pl.multiple_of(quarter * 512, 512), 512),
        ]

    def wp_part(quarter, of_core, start, count):
        return wp_all.at[
            pl.ds(pl.multiple_of(of_core * 256 + start, 128), count),
            pl.ds(pl.multiple_of(quarter * 512, 512), 512),
        ]

    def share(quarter, index):
        go(wa_part(quarter, core, 0, 512), wa_part(quarter, core, 0, 512), index, partner)
        go(wp_part(quarter, core, 0, 256), wp_part(quarter, core, 0, 256), index + 1, partner)

    def shared(quarter, index):
        got(wa_part(quarter, 1 - core, 0, 512), index)
        got(wp_part(quarter, 1 - core, 0, 256), index + 1)

    def weights_start():
        go(wa_ref, wa_part(y, core, 0, 512), 2, up)
        go(wp_ref, wp_part(y, core, 0, 256), 3, up)
        go(wa_ref, wa_part(y, core, 0, 512), 4, down)
        go(wp_ref, wp_part(y, core, 0, 256), 5, down)
        go(wa_ref, wa_part(y, core, 0, 512), 10, partner)
        go(wp_ref, wp_part(y, core, 0, 256), 11, partner)

    def weights_middle():
        got(wa_part(y_down, core, 0, 512), 2)
        got(wp_part(y_down, core, 0, 256), 3)
        go(wa_part(y_down, core, 0, 256), wa_part(y_down, core, 0, 256), 6, up)
        go(wp_part(y_down, core, 0, 128), wp_part(y_down, core, 0, 128), 7, up)
        got(wa_part(y_up, core, 0, 512), 4)
        got(wp_part(y_up, core, 0, 256), 5)
        go(wa_part(y_up, core, 256, 256), wa_part(y_up, core, 256, 256), 8, down)
        go(wp_part(y_up, core, 128, 128), wp_part(y_up, core, 128, 128), 9, down)
        share(y_down, 12)
        share(y_up, 14)

    def weights_late():
        got(wa_part(y_far, core, 0, 256), 6)
        got(wp_part(y_far, core, 0, 128), 7)
        got(wa_part(y_far, core, 256, 256), 8)
        got(wp_part(y_far, core, 128, 128), 9)
        share(y_far, 16)

    def weights_end():
        shared(y, 10)
        shared(y_down, 12)
        shared(y_up, 14)
        shared(y_far, 16)

    offset_m[...] = jnp.zeros_like(offset_m)
    offset_m[:, 0:8] = jnp.broadcast_to(offset_ref[...], (8, 8))
    gains_m[:, 0:256] = jnp.broadcast_to(pg_ref[...], (16, 256))
    gains_m[:, 256:768] = jnp.broadcast_to(ag_ref[...], (16, 512))
    keys_values = x_ref.at[:, 0:128, :]
    go(keys_values, other_s, 0, partner)
    weights_start()
    go(offset_m, offset_s, 18, partner)
    go(gains_m, gains_all.at[pl.ds(pl.multiple_of(16 * core, 16), 16), :], 1, partner)
    wa_part(y, core, 0, 512)[...] = wa_ref[...]
    wp_part(y, core, 0, 256)[...] = wp_ref[...]
    gains_all[pl.ds(pl.multiple_of(16 * core, 16), 16), :] = gains_m[...]

    scale = LOG2E / math.sqrt(HEAD_DIM)
    half = core
    got(offset_s, 18)
    of_core = jnp.where(sp // 8 == core, offset_m[0:1, :], offset_s[0:1, :])
    chosen = lax.broadcasted_iota(jnp.int32, (1, 128), 1) == sp % 8
    offset = jnp.sum(jnp.where(chosen, of_core, 0.0), axis=1, keepdims=True) * math.sqrt(HEAD_DIM)

    column = lax.broadcasted_iota(jnp.int32, (BLOCK, 64), 1)
    terms = split_terms(jnp.broadcast_to(offset, (BLOCK, 64)))
    extra = jnp.where(
        column == 0,
        terms[0].astype(jnp.float32),
        jnp.where(
            column == 1,
            terms[1].astype(jnp.float32),
            jnp.where(column == 2, terms[2].astype(jnp.float32), 0.0),
        ),
    ).astype(jnp.bfloat16)
    row = lax.broadcasted_iota(jnp.int32, (64, HALF), 0)
    ones = jnp.where(row < 3, 1.0, 0.0).astype(jnp.bfloat16)
    tri_s[...] = jnp.where(
        lax.broadcasted_iota(jnp.int32, (HALF, HALF), 0)
        <= lax.broadcasted_iota(jnp.int32, (HALF, HALF), 1),
        1.0,
        0.0,
    ).astype(jnp.bfloat16)
    mask_s[...] = jnp.where(
        lax.broadcasted_iota(jnp.int32, (BLOCK, HALF), 0)
        < lax.broadcasted_iota(jnp.int32, (BLOCK, HALF), 1) + half * HALF,
        0.0,
        -1e30,
    )
    acc_s[...] = jnp.zeros_like(acc_s)
    carry_s[...] = jnp.zeros_like(carry_s)

    mine_at = pl.ds(pl.multiple_of(core * HALF, HALF), HALF)
    other_at = pl.ds(pl.multiple_of((1 - core) * HALF, HALF), HALF)

    def turned(block):
        return block.astype(jnp.float32).T.astype(jnp.bfloat16)

    mine_rows = pl.ds(pl.multiple_of(core * HALF, HALF), HALF)
    other_rows = pl.ds(pl.multiple_of((1 - core) * HALF, HALF), HALF)

    def prepare(n, unused):
        for r in (2 * n, 2 * n + 1):
            k_s[r, mine_rows, 0:64] = turned(x_ref[r, 0:64, :])
            k_s[r, :, 64:128] = extra
            v_s[r, :, mine_at] = x_ref[r, 64:128, :]
            q_s[r, 0:64, :] = x_ref[r, 128:192, :]
            q_s[r, 64:128, :] = ones
        return unused

    lax.fori_loop(0, BLOCKS // 2, prepare, 0)
    got(other_s, 0)

    def complete(n, unused):
        for r in (2 * n, 2 * n + 1):
            k_s[r, other_rows, 0:64] = turned(other_s[r, 0:64, :])
            v_s[r, :, other_at] = other_s[r, 64:128, :]
        return unused

    lax.fori_loop(0, BLOCKS // 2, complete, 0)

    zs, ls, ws = (z0, z1, z2), (l0, l1, l2), (w0, w1, w2)

    first_row = jnp.where(sp == BLOCKS - 1, 1, sp + 1)

    def places(state):
        step, r, distance = state
        row_at = jnp.where((step < 0) | (step >= 136), BLOCKS, r)
        return (row_at, r, jnp.maximum(r - distance, 0))

    def advance(state):
        step, r, distance = state
        diagonal = step < BLOCKS - 1
        turn = step == BLOCKS - 1
        done = distance >= r
        next_row = jnp.where(r == BLOCKS - 1, 1, r + 1)
        r_after = jnp.where(
            diagonal,
            jnp.maximum(step + 1, 0),
            jnp.where(turn, first_row, jnp.where(done, next_row, r)),
        )
        after = jnp.where(diagonal, 0, jnp.where(turn | done, 1, distance + 1))
        return (step + 1, r_after, after)

    def scores(state, b, masked):
        unused_row, r, g = places(state)
        z = jnp.dot(k_s[g], q_s[r], preferred_element_type=jnp.float32) * scale
        if masked:
            z = z + mask_s[...]
        zs[b][...] = z

    def soften(b):
        ls[b][...] = jnp.log2(1.0 + jnp.exp2(zs[b][...])).astype(jnp.bfloat16)

    def weigh(state, b):
        row_at = places(state)[0]
        late = jnp.dot(tri_s[...], ls[b][HALF:, :], preferred_element_type=jnp.float32)
        early = jnp.dot(tri_s[...], ls[b][:HALF, :], preferred_element_type=jnp.float32)
        carry = carry_s[row_at][0:1]
        before = carry + late[0:1]
        ws[b][HALF:, :] = jnp.exp2(zs[b][HALF:, :] - (late + carry)).astype(jnp.bfloat16)
        ws[b][:HALF, :] = jnp.exp2(zs[b][:HALF, :] - (early + before)).astype(jnp.bfloat16)
        carry_s[row_at] = jnp.broadcast_to(before + early[0:1], (8, HALF))

    def gather_values(state, b):
        row_at, unused_row, g = places(state)
        acc_s[row_at] = acc_s[row_at] + jnp.dot(
            v_s[g], ws[b][...], preferred_element_type=jnp.float32
        )

    def return_row(state):
        step, r, distance = state

        @pl.when((distance == r) & (step >= 0) & (step < 136))
        def _():
            done_s[r] = acc_s[r].astype(jnp.bfloat16)

            @pl.when(r != sp)
            def _():
                pltpu.make_async_remote_copy(
                    src_ref=done_s.at[r], dst_ref=o_ref.at[sp], send_sem=send.at[19 + r],
                    recv_sem=recv.at[19 + sp], device_id=owner(r), device_id_type=MESH,
                ).start()

    def steps(masked):
        def body(n, states):
            states = list(states)
            for unused_step in range(6):
                states.append(advance(states[-1]))
            for u in range(6):
                gather_values(states[u], (u + 2) % 3)
                weigh(states[u + 1], u % 3)
                soften((u + 1) % 3)
                scores(states[u + 3], (u + 2) % 3, masked)
            for u in range(6):
                return_row(states[u])
            return tuple(states[6:])

        return body

    first = tuple((jnp.int32(step), jnp.int32(0), jnp.int32(0)) for step in (-5, -4, -3, -2))
    states = lax.fori_loop(0, 3, steps(True), first)
    states = lax.fori_loop(0, 8, steps(False), states)
    weights_middle()
    states = lax.fori_loop(8, 14, steps(False), states)
    weights_late()
    lax.fori_loop(14, 21, steps(False), states)
    o_ref[sp] = done_s[sp]
    weights_end()
    got(gains_all.at[pl.ds(pl.multiple_of(16 * (1 - core), 16), 16), :], 1)
    for copy in started:
        copy.wait_send()

    def settle_row(i, unused):
        r = (sp + i) % BLOCKS
        copy = pltpu.make_async_remote_copy(
            src_ref=done_s.at[r], dst_ref=o_ref.at[r], send_sem=send.at[19 + r],
            recv_sem=recv.at[19 + r], device_id=owner(r), device_id_type=MESH,
        )
        copy.wait_send()
        copy.wait_recv()
        return unused

    lax.fori_loop(1, BLOCKS, settle_row, 0)


def attention(offset, packed, w_pool, w_attn, pool_gain, attn_gain):
    vmem = pl.BlockSpec(memory_space=pltpu.VMEM)
    return pl.pallas_call(
        attention_kernel,
        out_shape=(
            jax.ShapeDtypeStruct((BLOCKS, HEAD_DIM, HALF), jnp.bfloat16),
            jax.ShapeDtypeStruct((512, 2048), jnp.bfloat16),
            jax.ShapeDtypeStruct((1024, 2048), jnp.bfloat16),
            jax.ShapeDtypeStruct((32, 768), jnp.bfloat16),
        ),
        in_specs=[vmem] * 6,
        out_specs=(vmem, vmem, vmem, vmem),
        scratch_shapes=[
            pltpu.VMEM((8, 128), jnp.float32),
            pltpu.VMEM((8, 128), jnp.float32),
            pltpu.VMEM((16, 768), jnp.bfloat16),
            pltpu.VMEM((BLOCKS, 128, HALF), jnp.bfloat16),
            pltpu.VMEM((BLOCKS, 128, HALF), jnp.bfloat16),
            pltpu.VMEM((BLOCKS, BLOCK, 128), jnp.bfloat16),
            pltpu.VMEM((BLOCKS, HEAD_DIM, BLOCK), jnp.bfloat16),
            pltpu.VMEM((HALF, HALF), jnp.bfloat16),
            pltpu.VMEM((BLOCK, HALF), jnp.float32),
            pltpu.VMEM((BLOCKS + 1, HEAD_DIM, HALF), jnp.float32),
            pltpu.VMEM((BLOCKS + 1, 8, HALF), jnp.float32),
            pltpu.VMEM((BLOCKS, HEAD_DIM, HALF), jnp.bfloat16),
            *[pltpu.VMEM((BLOCK, HALF), jnp.float32)] * 3,
            *[pltpu.VMEM((BLOCK, HALF), jnp.bfloat16)] * 6,
            pltpu.SemaphoreType.DMA((35,)),
            pltpu.SemaphoreType.DMA((35,)),
        ],
        compiler_params=pltpu.CompilerParams(
            collective_id=1, has_side_effects=True, vmem_limit_bytes=56 * 1024 * 1024
        ),
        cost_estimate=pl.CostEstimate(
            flops=40_000_000_000, bytes_accessed=4_000_000, transcendentals=50_000_000
        ),
        name="stick_attention",
    )(offset, packed, w_pool, w_attn, pool_gain, attn_gain)


def shards(
    tokens,
    norm_gain,
    w_pool_in,
    w_query,
    w_key,
    w_value,
    query_gain,
    key_gain,
    stick_offset,
    pool_mix,
    pool_scale,
    pool_gain,
    attn_gain,
    w_out_pool,
    w_out_attn,
):
    packed, pool_parts = project(
        tokens[0], norm_gain, w_key, w_value, w_query, w_pool_in, key_gain, query_gain,
        pool_mix, pool_scale,
    )
    attended, w_pool_all, w_attn_all, gains_all = attention(
        stick_offset.reshape(1, 8), packed, w_out_pool, w_out_attn,
        pool_gain.reshape(1, 256), attn_gain.reshape(1, 512),
    )
    attended = attended.reshape(HEADS * HEAD_DIM, HALF)
    pool_rows = jnp.concatenate([pool_parts[0], pool_parts[1]], axis=1)
    pool_gain_all = jnp.concatenate([gains_all[0, :256], gains_all[16, :256]])
    attn_gain_all = jnp.concatenate([gains_all[0, 256:], gains_all[16, 256:]])
    pool_f = pool_rows.astype(jnp.float32)
    attn_f = attended.astype(jnp.float32)
    pool_normed = branch_norm(pool_rows, jnp.sum(pool_f * pool_f, axis=-1), POOL, pool_gain_all)
    factor = lax.rsqrt(jnp.sum(attn_f * attn_f, axis=0) / (HEADS * HEAD_DIM) + EPS)
    attn_normed = (
        attn_f * factor[None, :] * attn_gain_all.astype(jnp.float32)[:, None]
    ).astype(jnp.bfloat16)
    mixed = jnp.dot(pool_normed, w_pool_all, preferred_element_type=jnp.float32) + lax.dot_general(
        attn_normed, w_attn_all, (((0,), (0,)), ((), ())), preferred_element_type=jnp.float32
    )
    return mixed.astype(jnp.bfloat16)[None]


def solution(mesh):
    in_specs = (
        P("fs", "sp", "tp"),
        P(),
        P("fs", "tp"),
        P("fs", "tp"),
        P("fs", "tp"),
        P("fs", "tp"),
        P(),
        P(),
        P("tp"),
        P("tp", None, None),
        P("tp"),
        P("tp"),
        P("tp"),
        P("tp", "fs"),
        P("tp", "fs"),
    )
    out_specs = P("fs", ("sp", "tp"), None)
    return jax.shard_map(shards, mesh=mesh, in_specs=in_specs, out_specs=out_specs, check_vma=False)
```

```python
import math

import jax
import jax.numpy as jnp
from jax import lax
from jax.experimental import pallas as pl
from jax.experimental.pallas import tpu as pltpu
from jax.sharding import PartitionSpec as P

HEADS = 16
HEAD_DIM = 64
POOL = 512
POOL_GROUPS = 4
BLOCKS = 16
HALF = 256
BLOCK = 512

EPS = 1e-06
LOG2E = 1.4426950408889634


def split_terms(value):
    high = value.astype(jnp.bfloat16)
    rest = value - high.astype(jnp.float32)
    middle = rest.astype(jnp.bfloat16)
    low = (rest - middle.astype(jnp.float32)).astype(jnp.bfloat16)
    return (high, middle, low)


MESH = pl.DeviceIdType.MESH


def mixer_kernel(
    tok_ref, gain_ref, wk_ref, wv_ref, wq_ref, wp_ref, kg_ref, qg_ref, mix_ref, scale_ref,
    offset_ref, wpo_ref, wao_ref, pg_ref, ag_ref,
    mixed_ref,
    buf, pbuf, tok_s, x_s, acc, acc_p, heads_s, pool_in, before_s, pooled_s, pool_rows,
    recv_s, other_s, o_ref, wp_all, wa_all, gains_m, gains_o, offset_m, offset_s,
    q_s, k_s, v_s, tri_s, mask_s, acc_s, carry_s, done_s,
    z0, z1, z2, l0, l1, l2, w0, w1, w2, send, recv,
):
    sp, y, core = lax.axis_index("sp"), lax.axis_index("fs"), lax.axis_index("tp")
    z, x = sp // 4, sp % 4
    y_up, y_down, y_far = (y + 1) % 4, (y + 3) % 4, (y + 2) % 4
    x_up, x_down, x_far = (x + 1) % 4, (x + 3) % 4, (x + 2) % 4
    z_up, z_down, z_far = (z + 1) % 4, (z + 3) % 4, (z + 2) % 4

    def at(z_to, x_to, y_to, core_to):
        return {"sp": z_to * 4 + x_to, "fs": y_to, "tp": core_to}

    partner = at(z, x, y, 1 - core)
    to = {
        "yp": at(z, x, y_up, core), "ym": at(z, x, y_down, core),
        "xp": at(z, x_up, y, core), "xm": at(z, x_down, y, core),
        "zp": at(z_up, x, y, core), "zm": at(z_down, x, y, core),
    }

    barrier = pltpu.get_barrier_semaphore()
    for target in (partner, to["yp"], to["ym"]):
        pl.semaphore_signal(barrier, inc=1, device_id=target, device_id_type=MESH)

    def greet(i, unused):
        for of_core in range(2):
            pl.semaphore_signal(
                barrier, inc=1, device_id={"sp": (sp + i) % BLOCKS, "fs": y, "tp": of_core},
                device_id_type=MESH,
            )
        return unused

    lax.fori_loop(1, BLOCKS, greet, 0)
    pl.semaphore_wait(barrier, 33)

    started = []

    def remote(source, target_ref, index, target):
        return pltpu.make_async_remote_copy(
            src_ref=source, dst_ref=target_ref, send_sem=send.at[index],
            recv_sem=recv.at[index], device_id=target, device_id_type=MESH,
        )

    def go(source, target_ref, index, target):
        copy = remote(source, target_ref, index, target)
        copy.start()
        started.append(copy)

    def got(target_ref, index):
        remote(target_ref, target_ref, index, partner).wait_recv()

    def rows(start, count=64):
        return pl.ds(pl.multiple_of(start, 32), count)

    weights = (wk_ref, wv_ref, wq_ref)
    quarters = (y_down, y_up, y_far)

    def part(a, quarter, start, count=64):
        return buf.at[a, quarter, rows(start, count), :]

    def direct(a):
        base = a * 30
        own_x, own_z = 64 * x, 256 + 64 * z
        w = weights[a]
        go(w.at[rows(own_x), :], part(a, y, own_x), base + 0, to["yp"])
        go(w.at[rows(own_z), :], part(a, y, own_z), base + 1, to["ym"])
        go(w.at[rows(own_x), :], part(a, y, own_x), base + 2, to["ym"])
        go(w.at[rows(own_z), :], part(a, y, own_z), base + 3, to["yp"])

    def ring_base(a, item, ring):
        return a * 30 + 6 + item * 8 + ring * 4

    own_row = (64 * x, 256 + 64 * z)
    down_row = (64 * x_down, 256 + 64 * z_down)
    up_row = (64 * x_up, 256 + 64 * z_up)
    far_row = (64 * x_far, 256 + 64 * z_far)
    ups = ("xp", "zp")
    downs = ("xm", "zm")

    def spread(a, item, ring):
        base = ring_base(a, item, ring)
        piece = part(a, quarters[item], own_row[ring])
        go(piece, piece, base + 0, to[ups[ring]])
        go(piece, piece, base + 1, to[downs[ring]])

    def relay(a, item, ring):
        base = ring_base(a, item, ring)
        q = quarters[item]
        got(part(a, q, down_row[ring]), base + 0)
        piece = part(a, q, down_row[ring], 32)
        go(piece, piece, base + 2, to[ups[ring]])
        got(part(a, q, up_row[ring]), base + 1)
        piece = part(a, q, up_row[ring] + 32, 32)
        go(piece, piece, base + 3, to[downs[ring]])

    def settle(a):
        for item in range(3):
            for ring in range(2):
                base = ring_base(a, item, ring)
                q = quarters[item]
                got(part(a, q, far_row[ring], 32), base + 2)
                got(part(a, q, far_row[ring] + 32, 32), base + 3)

    def first(a):
        base = a * 30
        piece = part(a, y_down, own_row[0])
        got(piece, base + 0)
        go(piece, piece, base + 4, to["yp"])
        spread(a, 0, 0)
        piece = part(a, y_up, own_row[1])
        got(piece, base + 1)
        go(piece, piece, base + 5, to["ym"])
        spread(a, 1, 1)
        got(part(a, y_up, own_row[0]), base + 2)
        spread(a, 1, 0)
        got(part(a, y_down, own_row[1]), base + 3)
        spread(a, 0, 1)

    def second(a):
        relay(a, 0, 0)
        relay(a, 1, 1)

    def third(a):
        base = a * 30
        got(part(a, y_far, own_row[0]), base + 4)
        spread(a, 2, 0)
        got(part(a, y_far, own_row[1]), base + 5)
        spread(a, 2, 1)
        relay(a, 1, 0)
        relay(a, 0, 1)

    def fourth(a):
        relay(a, 2, 0)
        relay(a, 2, 1)

    def query_direct():
        go(wq_ref, buf.at[2, y], 60, to["yp"])
        go(wq_ref, buf.at[2, y], 61, to["ym"])

    def query_relay():
        got(buf.at[2, y_down], 60)
        piece = buf.at[2, y_down, 0:256, :]
        go(piece, piece, 62, to["yp"])
        got(buf.at[2, y_up], 61)
        piece = buf.at[2, y_up, 256:512, :]
        go(piece, piece, 63, to["ym"])

    def query_settle():
        got(buf.at[2, y_far, 0:256, :], 62)
        got(buf.at[2, y_far, 256:512, :], 63)

    pool_base = 90

    def pool_direct():
        go(wp_ref, pbuf.at[y], pool_base + 0, to["yp"])
        go(wp_ref, pbuf.at[y], pool_base + 1, to["ym"])

    def pool_relay():
        got(pbuf.at[y_down], pool_base + 0)
        piece = pbuf.at[y_down, 0:256, :]
        go(piece, piece, pool_base + 2, to["yp"])
        got(pbuf.at[y_up], pool_base + 1)
        piece = pbuf.at[y_up, 256:512, :]
        go(piece, piece, pool_base + 3, to["ym"])

    def pool_settle():
        got(pbuf.at[y_far, 0:256, :], pool_base + 2)
        got(pbuf.at[y_far, 256:512, :], pool_base + 3)

    def own(a):
        acc[a] = jnp.dot(x_s[y], weights[a][...], preferred_element_type=jnp.float32)

    def rest(a):
        total = acc[a]
        for q in quarters:
            total = total + jnp.dot(x_s[q], buf[a, q], preferred_element_type=jnp.float32)
        return total

    def head_copy(a, i, source):
        h, of_core = (sp + i // 2) % 8, i % 2
        return pltpu.make_async_remote_copy(
            src_ref=heads_s.at[a, h, of_core],
            dst_ref=recv_s.at[source, a * 64 : a * 64 + 64, :],
            send_sem=send.at[97 + a * 16 + i], recv_sem=recv.at[97 + a * 16 + source],
            device_id={"sp": 8 * core + h, "fs": y, "tp": of_core}, device_id_type=MESH,
        )

    stays = sp // 8 == core

    def deliver(a, total):
        turned = total.T.reshape(8, HEAD_DIM, BLOCK)
        if a != 1:
            factor = lax.rsqrt(jnp.mean(turned * turned, axis=1, keepdims=True) + EPS)
            gain_row = (kg_ref if a == 0 else qg_ref)[...]
            gain = jnp.broadcast_to(gain_row, (HEAD_DIM, HEAD_DIM)).T[:, 0:1]
            turned = turned * factor * gain[None]
        turned = turned.astype(jnp.bfloat16)
        heads_s[a, :, 0] = turned[:, :, :HALF]
        heads_s[a, :, 1] = turned[:, :, HALF:]

        def send_head(i, unused):
            @pl.when(jnp.logical_not(stays & (i == core)))
            def _():
                head_copy(a, i, sp).start()

            return unused

        lax.fori_loop(0, 16, send_head, 0)

        @pl.when(stays)
        def _():
            recv_s[sp, a * 64 : a * 64 + 64, :] = heads_s[a, sp % 8, core]

    def wa_part(quarter, of_core, start, count):
        return wa_all.at[
            pl.ds(pl.multiple_of(of_core * 512 + start, 128), count),
            pl.ds(pl.multiple_of(quarter * 512, 512), 512),
        ]

    def wp_part(quarter, of_core, start, count):
        return wp_all.at[
            pl.ds(pl.multiple_of(of_core * 256 + start, 128), count),
            pl.ds(pl.multiple_of(quarter * 512, 512), 512),
        ]

    def share(quarter, index):
        go(wa_part(quarter, core, 0, 512), wa_part(quarter, core, 0, 512), index, partner)
        go(wp_part(quarter, core, 0, 256), wp_part(quarter, core, 0, 256), index + 1, partner)

    def shared(quarter, index):
        got(wa_part(quarter, 1 - core, 0, 512), index)
        got(wp_part(quarter, 1 - core, 0, 256), index + 1)

    def weights_start():
        go(wao_ref, wa_part(y, core, 0, 512), 147, to["yp"])
        go(wpo_ref, wp_part(y, core, 0, 256), 148, to["yp"])
        go(wao_ref, wa_part(y, core, 0, 512), 149, to["ym"])
        go(wpo_ref, wp_part(y, core, 0, 256), 150, to["ym"])
        go(wao_ref, wa_part(y, core, 0, 512), 155, partner)
        go(wpo_ref, wp_part(y, core, 0, 256), 156, partner)

    def weights_middle():
        got(wa_part(y_down, core, 0, 512), 147)
        got(wp_part(y_down, core, 0, 256), 148)
        go(wa_part(y_down, core, 0, 256), wa_part(y_down, core, 0, 256), 151, to["yp"])
        go(wp_part(y_down, core, 0, 128), wp_part(y_down, core, 0, 128), 152, to["yp"])
        got(wa_part(y_up, core, 0, 512), 149)
        got(wp_part(y_up, core, 0, 256), 150)
        go(wa_part(y_up, core, 256, 256), wa_part(y_up, core, 256, 256), 153, to["ym"])
        go(wp_part(y_up, core, 128, 128), wp_part(y_up, core, 128, 128), 154, to["ym"])
        share(y_down, 157)
        share(y_up, 159)

    def weights_late():
        got(wa_part(y_far, core, 0, 256), 151)
        got(wp_part(y_far, core, 0, 128), 152)
        got(wa_part(y_far, core, 256, 256), 153)
        got(wp_part(y_far, core, 128, 128), 154)
        share(y_far, 161)

    def weights_end():
        shared(y, 155)
        shared(y_down, 157)
        shared(y_up, 159)
        shared(y_far, 161)

    mine_at = pl.ds(pl.multiple_of(core * HALF, HALF), HALF)
    other_at = pl.ds(pl.multiple_of((1 - core) * HALF, HALF), HALF)

    def turned(block):
        return block.astype(jnp.float32).T.astype(jnp.bfloat16)

    def forward(a, r):
        return pltpu.make_async_remote_copy(
            src_ref=recv_s.at[r, a * 64 : a * 64 + 64, :],
            dst_ref=other_s.at[r, a * 64 : a * 64 + 64, :],
            send_sem=send.at[200 + a * 16 + r], recv_sem=recv.at[200 + a * 16 + r],
            device_id=partner, device_id_type=MESH,
        )

    def place(a, r, block, at):
        if a == 0:
            k_s[r, at, 0:64] = turned(block)
        elif a == 1:
            v_s[r, :, at] = block
        else:
            q_s[r, 0:64, :] = block

    def take(a):
        def pair(n, unused):
            places_now = [(sp + 2 * n) % BLOCKS, (sp + 2 * n + 1) % BLOCKS]
            for r in places_now:
                @pl.when(jnp.logical_not(stays & (r == sp)))
                def _():
                    head_copy(a, 0, r).wait_recv()

                if a < 2:
                    forward(a, r).start()
            for r in places_now:
                place(a, r, recv_s[r, a * 64 : a * 64 + 64, :], mine_at)
            return unused

        lax.fori_loop(0, BLOCKS // 2, pair, 0)

    def take_other(a):
        def pair(n, unused):
            places_now = [(sp + 2 * n) % BLOCKS, (sp + 2 * n + 1) % BLOCKS]
            for r in places_now:
                forward(a, r).wait_recv()
            for r in places_now:
                place(a, r, other_s[r, a * 64 : a * 64 + 64, :], other_at)
            return unused

        lax.fori_loop(0, BLOCKS // 2, pair, 0)

    scale = LOG2E / math.sqrt(HEAD_DIM)
    half = core
    go(tok_ref, tok_s, 94, partner)
    direct(0)
    direct(1)
    offset_m[...] = jnp.zeros_like(offset_m)
    offset_m[:, 0:8] = jnp.broadcast_to(offset_ref[...], (8, 8))
    gains_m[:, 0:256] = jnp.broadcast_to(pg_ref[...], (16, 256))
    gains_m[:, 256:768] = jnp.broadcast_to(ag_ref[...], (16, 512))
    tri_s[...] = jnp.where(
        lax.broadcasted_iota(jnp.int32, (HALF, HALF), 0)
        <= lax.broadcasted_iota(jnp.int32, (HALF, HALF), 1),
        1.0,
        0.0,
    ).astype(jnp.bfloat16)
    go(offset_m, offset_s, 163, partner)
    go(gains_m, gains_o, 146, partner)
    got(tok_s, 94)

    mine_f = tok_ref[...].astype(jnp.float32)
    other_f = tok_s[...].astype(jnp.float32)
    squares = jnp.sum(mine_f * mine_f, axis=1, keepdims=True) + jnp.sum(
        other_f * other_f, axis=1, keepdims=True
    )
    factor = lax.rsqrt(squares / 2048.0 + EPS)
    for j in range(2):
        columns = slice(512 * j, 512 * j + 512)
        at_mine = 2 * core + j
        at_other = 2 * (1 - core) + j
        x_s[at_mine] = (
            tok_ref[:, columns].astype(jnp.float32) * factor * gain_ref[at_mine]
        ).astype(jnp.bfloat16)
        x_s[at_other] = (
            tok_s[:, columns].astype(jnp.float32) * factor * gain_ref[at_other]
        ).astype(jnp.bfloat16)

    first(0)
    own(0)
    own(1)
    first(1)
    query_direct()
    own(2)
    second(0)
    acc_p[...] = jnp.dot(x_s[y], wp_ref[...], preferred_element_type=jnp.float32)
    third(0)
    second(1)
    fourth(0)
    third(1)
    settle(0)
    deliver(0, rest(0))
    fourth(1)
    settle(1)
    deliver(1, rest(1))
    query_relay()
    pool_direct()
    got(offset_s, 163)
    of_core = jnp.where(sp // 8 == core, offset_m[0:1, :], offset_s[0:1, :])
    chosen = lax.broadcasted_iota(jnp.int32, (1, 128), 1) == sp % 8
    offset = jnp.sum(jnp.where(chosen, of_core, 0.0), axis=1, keepdims=True) * math.sqrt(HEAD_DIM)
    column = lax.broadcasted_iota(jnp.int32, (BLOCK, 64), 1)
    terms = split_terms(jnp.broadcast_to(offset, (BLOCK, 64)))
    extra = jnp.where(
        column == 0,
        terms[0].astype(jnp.float32),
        jnp.where(
            column == 1,
            terms[1].astype(jnp.float32),
            jnp.where(column == 2, terms[2].astype(jnp.float32), 0.0),
        ),
    ).astype(jnp.bfloat16)
    row = lax.broadcasted_iota(jnp.int32, (64, HALF), 0)
    ones = jnp.where(row < 3, 1.0, 0.0).astype(jnp.bfloat16)
    mask_s[...] = jnp.where(
        lax.broadcasted_iota(jnp.int32, (BLOCK, HALF), 0)
        < lax.broadcasted_iota(jnp.int32, (BLOCK, HALF), 1) + half * HALF,
        0.0,
        -1e30,
    )
    acc_s[...] = jnp.zeros_like(acc_s)
    carry_s[...] = jnp.zeros_like(carry_s)


    def fill(r, unused):
        k_s[r, :, 64:128] = extra
        q_s[r, 64:128, :] = ones
        return unused

    lax.fori_loop(0, BLOCKS, fill, 0)
    mine_half = pl.ds(pl.multiple_of(core * HALF, HALF), HALF)
    other_half = pl.ds(pl.multiple_of((1 - core) * HALF, HALF), HALF)
    take(0)
    query_settle()
    deliver(2, rest(2))
    pool_relay()
    weights_start()
    take(1)
    take_other(0)
    wa_part(y, core, 0, 512)[...] = wao_ref[...]
    wp_part(y, core, 0, 256)[...] = wpo_ref[...]
    pool_settle()
    total = acc_p[...]
    for q in quarters:
        total = total + jnp.dot(x_s[q], pbuf[q], preferred_element_type=jnp.float32)
    pool_in[...] = total.astype(jnp.bfloat16)
    tail = pool_in.at[BLOCK - 16 : BLOCK, :]
    go(tail, before_s, 95, {"sp": (sp + 1) % BLOCKS, "fs": y, "tp": core})
    current = pool_in[...].astype(jnp.float32)
    got(before_s, 95)
    before = jnp.where(sp == 0, 0.0, before_s[...].astype(jnp.float32))

    def behind(values, count):
        return jnp.concatenate([jnp.zeros((count, values.shape[1]), jnp.float32), values[:-count]], axis=0)

    extended = jnp.concatenate([before, current], axis=0)
    sum_2 = extended + behind(extended, 1)
    sum_4 = sum_2 + behind(sum_2, 2)
    sum_8 = sum_4 + behind(sum_4, 4)
    sum_16 = sum_8 + behind(sum_8, 8)
    position = lax.broadcasted_iota(jnp.int32, (BLOCK, 128), 0) + (sp * BLOCK + 1)
    for group in range(2):
        columns = slice(128 * group, 128 * group + 128)
        low, high = ((sum_2, sum_8), (sum_4, sum_16))[group]
        window = jnp.where(core == 0, 2 << group, 8 << group)
        summed = jnp.where(core == 0, low[16:, columns], high[16:, columns])
        counted = jnp.minimum(position, window).astype(jnp.float32)
        centered = (summed / counted - current[:, columns]).astype(jnp.bfloat16)
        mixed = jnp.dot(centered, mix_ref[group], preferred_element_type=jnp.float32)
        pooled_s[:, columns] = (mixed * scale_ref[:, columns]).astype(jnp.bfloat16)
    mine_rows = pl.ds(pl.multiple_of(core * HALF, HALF), HALF)
    other_rows = pl.ds(pl.multiple_of((1 - core) * HALF, HALF), HALF)
    go(pooled_s.at[other_rows, :], pool_rows.at[core], 96, partner)
    pool_rows[core] = pooled_s[mine_rows, :]
    take_other(1)
    take(2)

    zs, ls, ws = (z0, z1, z2), (l0, l1, l2), (w0, w1, w2)

    first_row = jnp.where(sp == BLOCKS - 1, 1, sp + 1)

    def places(state):
        step, r, distance = state
        row_at = jnp.where((step < 0) | (step >= 136), BLOCKS, r)
        return (row_at, r, jnp.maximum(r - distance, 0))

    def advance(state):
        step, r, distance = state
        diagonal = step < BLOCKS - 1
        turn = step == BLOCKS - 1
        done = distance >= r
        next_row = jnp.where(r == BLOCKS - 1, 1, r + 1)
        r_after = jnp.where(
            diagonal,
            jnp.maximum(step + 1, 0),
            jnp.where(turn, first_row, jnp.where(done, next_row, r)),
        )
        after = jnp.where(diagonal, 0, jnp.where(turn | done, 1, distance + 1))
        return (step + 1, r_after, after)

    def scores(state, b, masked):
        unused_row, r, g = places(state)
        z = jnp.dot(k_s[g], q_s[r], preferred_element_type=jnp.float32) * scale
        if masked:
            z = z + mask_s[...]
        zs[b][...] = z

    def soften(b):
        ls[b][...] = jnp.log2(1.0 + jnp.exp2(zs[b][...])).astype(jnp.bfloat16)

    def weigh(state, b):
        row_at = places(state)[0]
        late = jnp.dot(tri_s[...], ls[b][HALF:, :], preferred_element_type=jnp.float32)
        early = jnp.dot(tri_s[...], ls[b][:HALF, :], preferred_element_type=jnp.float32)
        carry = carry_s[row_at][0:1]
        before = carry + late[0:1]
        ws[b][HALF:, :] = jnp.exp2(zs[b][HALF:, :] - (late + carry)).astype(jnp.bfloat16)
        ws[b][:HALF, :] = jnp.exp2(zs[b][:HALF, :] - (early + before)).astype(jnp.bfloat16)
        carry_s[row_at] = jnp.broadcast_to(before + early[0:1], (8, HALF))

    def gather_values(state, b):
        row_at, unused_row, g = places(state)
        acc_s[row_at] = acc_s[row_at] + jnp.dot(
            v_s[g], ws[b][...], preferred_element_type=jnp.float32
        )

    def return_row(state):
        step, r, distance = state

        @pl.when((distance == r) & (step >= 0) & (step < 136))
        def _():
            done_s[r] = acc_s[r].astype(jnp.bfloat16)

            @pl.when(r != sp)
            def _():
                pltpu.make_async_remote_copy(
                    src_ref=done_s.at[r], dst_ref=o_ref.at[sp], send_sem=send.at[180 + r],
                    recv_sem=recv.at[180 + sp], device_id={"sp": r, "fs": y, "tp": core}, device_id_type=MESH,
                ).start()

    def steps(masked):
        def body(n, states):
            states = list(states)
            for unused_step in range(6):
                states.append(advance(states[-1]))
            for u in range(6):
                gather_values(states[u], (u + 2) % 3)
                weigh(states[u + 1], u % 3)
                soften((u + 1) % 3)
                scores(states[u + 3], (u + 2) % 3, masked)
            for u in range(6):
                return_row(states[u])
            return tuple(states[6:])

        return body

    first_states = tuple(
        (jnp.int32(step), jnp.int32(0), jnp.int32(0)) for step in (-5, -4, -3, -2)
    )
    states = lax.fori_loop(0, 3, steps(True), first_states)
    states = lax.fori_loop(0, 8, steps(False), states)
    weights_middle()
    states = lax.fori_loop(8, 14, steps(False), states)
    weights_late()
    lax.fori_loop(14, 21, steps(False), states)
    o_ref[sp] = done_s[sp]
    weights_end()
    got(gains_o, 146)
    got(pool_rows.at[1 - core], 96)

    def settle_row(i, unused):
        r = (sp + i) % BLOCKS
        copy = pltpu.make_async_remote_copy(
            src_ref=done_s.at[r], dst_ref=o_ref.at[r], send_sem=send.at[180 + r],
            recv_sem=recv.at[180 + r], device_id={"sp": r, "fs": y, "tp": core},
            device_id_type=MESH,
        )
        copy.wait_send()
        copy.wait_recv()
        return unused

    lax.fori_loop(1, BLOCKS, settle_row, 0)

    def gain_rows(columns):
        mine_gain = gains_m[0:1, columns].astype(jnp.float32)
        other_gain = gains_o[0:1, columns].astype(jnp.float32)
        low = jnp.where(core == 0, mine_gain, other_gain)
        high = jnp.where(core == 0, other_gain, mine_gain)
        return jnp.concatenate([low, high], axis=1)

    attended = o_ref[...].reshape(HEADS * HEAD_DIM, HALF).astype(jnp.float32).T
    factor = lax.rsqrt(jnp.mean(attended * attended, axis=1, keepdims=True) + EPS)
    attn_normed = (attended * factor * gain_rows(slice(256, 768))).astype(jnp.bfloat16)
    pooled = jnp.concatenate([pool_rows[0], pool_rows[1]], axis=1).astype(jnp.float32)
    factor = lax.rsqrt(jnp.mean(pooled * pooled, axis=1, keepdims=True) + EPS)
    pool_normed = (pooled * factor * gain_rows(slice(0, 256))).astype(jnp.bfloat16)
    for j in range(4):
        columns = slice(512 * j, 512 * j + 512)
        mixed_ref[:, columns] = (
            jnp.dot(pool_normed, wp_all[:, columns], preferred_element_type=jnp.float32)
            + jnp.dot(attn_normed, wa_all[:, columns], preferred_element_type=jnp.float32)
        ).astype(jnp.bfloat16)

    for copy in started:
        copy.wait_send()

    def settle_heads(i, unused):
        for a in range(3):
            @pl.when(jnp.logical_not(stays & (i == core)))
            def _():
                head_copy(a, i, sp).wait_send()

        for a in range(2):
            forward(a, i).wait_send()
        return unused

    lax.fori_loop(0, BLOCKS, settle_heads, 0)


def mixer(*operands):
    vmem = pl.BlockSpec(memory_space=pltpu.VMEM)
    return pl.pallas_call(
        mixer_kernel,
        out_shape=jax.ShapeDtypeStruct((HALF, 2048), jnp.bfloat16),
        in_specs=[vmem] * 15,
        out_specs=vmem,
        scratch_shapes=[
            pltpu.VMEM((3, 4, 512, 512), jnp.bfloat16),
            pltpu.VMEM((4, 512, 256), jnp.bfloat16),
            pltpu.VMEM((512, 1024), jnp.bfloat16),
            pltpu.VMEM((4, 512, 512), jnp.bfloat16),
            pltpu.VMEM((3, 512, 512), jnp.float32),
            pltpu.VMEM((512, 256), jnp.float32),
            pltpu.VMEM((3, 8, 2, HEAD_DIM, HALF), jnp.bfloat16),
            pltpu.VMEM((512, 256), jnp.bfloat16),
            pltpu.VMEM((16, 256), jnp.bfloat16),
            pltpu.VMEM((512, 256), jnp.bfloat16),
            pltpu.VMEM((2, HALF, 256), jnp.bfloat16),
            pltpu.VMEM((BLOCKS, 3 * HEAD_DIM, HALF), jnp.bfloat16),
            pltpu.VMEM((BLOCKS, 2 * HEAD_DIM, HALF), jnp.bfloat16),
            pltpu.VMEM((BLOCKS, HEAD_DIM, HALF), jnp.bfloat16),
            pltpu.VMEM((512, 2048), jnp.bfloat16),
            pltpu.VMEM((1024, 2048), jnp.bfloat16),
            pltpu.VMEM((16, 768), jnp.bfloat16),
            pltpu.VMEM((16, 768), jnp.bfloat16),
            pltpu.VMEM((8, 128), jnp.float32),
            pltpu.VMEM((8, 128), jnp.float32),
            pltpu.VMEM((BLOCKS, 128, HALF), jnp.bfloat16),
            pltpu.VMEM((BLOCKS, BLOCK, 128), jnp.bfloat16),
            pltpu.VMEM((BLOCKS, HEAD_DIM, BLOCK), jnp.bfloat16),
            pltpu.VMEM((HALF, HALF), jnp.bfloat16),
            pltpu.VMEM((BLOCK, HALF), jnp.float32),
            pltpu.VMEM((BLOCKS + 1, HEAD_DIM, HALF), jnp.float32),
            pltpu.VMEM((BLOCKS + 1, 8, HALF), jnp.float32),
            pltpu.VMEM((BLOCKS, HEAD_DIM, HALF), jnp.bfloat16),
            *[pltpu.VMEM((BLOCK, HALF), jnp.float32)] * 3,
            *[pltpu.VMEM((BLOCK, HALF), jnp.bfloat16)] * 6,
            pltpu.SemaphoreType.DMA((232,)),
            pltpu.SemaphoreType.DMA((232,)),
        ],
        compiler_params=pltpu.CompilerParams(
            collective_id=0, has_side_effects=True, vmem_limit_bytes=62 * 1024 * 1024
        ),
        cost_estimate=pl.CostEstimate(
            flops=45_000_000_000, bytes_accessed=8_000_000, transcendentals=50_000_000
        ),
        name="token_mixer",
    )(*operands)


def shards(
    tokens,
    norm_gain,
    w_pool_in,
    w_query,
    w_key,
    w_value,
    query_gain,
    key_gain,
    stick_offset,
    pool_mix,
    pool_scale,
    pool_gain,
    attn_gain,
    w_out_pool,
    w_out_attn,
):
    mixed = mixer(
        tokens[0], norm_gain.reshape(4, 1, 512), w_key, w_value, w_query, w_pool_in,
        key_gain.reshape(1, HEAD_DIM), query_gain.reshape(1, HEAD_DIM), pool_mix,
        pool_scale.reshape(1, 256), stick_offset.reshape(1, 8), w_out_pool, w_out_attn,
        pool_gain.reshape(1, 256), attn_gain.reshape(1, 512),
    )
    return mixed[None]


def solution(mesh):
    in_specs = (
        P("fs", "sp", "tp"),
        P(),
        P("fs", "tp"),
        P("fs", "tp"),
        P("fs", "tp"),
        P("fs", "tp"),
        P(),
        P(),
        P("tp"),
        P("tp", None, None),
        P("tp"),
        P("tp"),
        P("tp"),
        P("tp", "fs"),
        P("tp", "fs"),
    )
    out_specs = P("fs", ("sp", "tp"), None)
    return jax.shard_map(shards, mesh=mesh, in_specs=in_specs, out_specs=out_specs, check_vma=False)
```

```python
import functools
import math

import jax
import jax.numpy as jnp
from jax import lax
from jax.experimental import pallas as pl
from jax.experimental.pallas import tpu as pltpu
from jax.sharding import PartitionSpec as P

HEADS = 16
HEAD_DIM = 64
POOL = 512
POOL_GROUPS = 4
BLOCKS = 16
HALF = 256
BLOCK = 512

EPS = 1e-06
LOG2E = 1.4426950408889634


def split_terms(value):
    high = value.astype(jnp.bfloat16)
    rest = value - high.astype(jnp.float32)
    middle = rest.astype(jnp.bfloat16)
    low = (rest - middle.astype(jnp.float32)).astype(jnp.bfloat16)
    return (high, middle, low)


MESH = pl.DeviceIdType.MESH


def mixer_kernel(
    tok_hbm, gain_ref, wk_hbm, wv_hbm, wq_hbm, wp_hbm, kg_ref, qg_ref, mix_ref, scale_ref,
    offset_ref, wpo_ref, wao_ref, pg_ref, ag_ref,
    left_ref, right_ref,
    tok_ref, wk_ref, wv_ref, wq_ref, wp_ref,
    buf, pbuf, tok_s, x_s, acc, acc_p, heads_s, pool_in, before_s, pooled_s, pool_rows,
    recv_s, other_s, o_ref, wp_all, wa_all, gains_m, gains_o, offset_m, offset_s,
    q_s, k_s, v_s, tri_s, mask_s, acc_s, carry_s, done_s,
    z0, z1, z2, l0, l1, l2, w0, w1, w2, send, recv, local,
):
    sp, y, core = lax.axis_index("sp"), lax.axis_index("fs"), lax.axis_index("tp")
    z, x = sp // 4, sp % 4
    y_up, y_down, y_far = (y + 1) % 4, (y + 3) % 4, (y + 2) % 4
    x_up, x_down, x_far = (x + 1) % 4, (x + 3) % 4, (x + 2) % 4
    z_up, z_down, z_far = (z + 1) % 4, (z + 3) % 4, (z + 2) % 4

    def at(z_to, x_to, y_to, core_to):
        return {"sp": z_to * 4 + x_to, "fs": y_to, "tp": core_to}

    partner = at(z, x, y, 1 - core)
    to = {
        "yp": at(z, x, y_up, core), "ym": at(z, x, y_down, core),
        "xp": at(z, x_up, y, core), "xm": at(z, x_down, y, core),
        "zp": at(z_up, x, y, core), "zm": at(z_down, x, y, core),
    }

    barrier = pltpu.get_barrier_semaphore()
    for target in (partner, to["yp"], to["ym"]):
        pl.semaphore_signal(barrier, inc=1, device_id=target, device_id_type=MESH)

    def greet(i, unused):
        for of_core in range(2):
            pl.semaphore_signal(
                barrier, inc=1, device_id={"sp": (sp + i) % BLOCKS, "fs": y, "tp": of_core},
                device_id_type=MESH,
            )
        return unused

    lax.fori_loop(1, BLOCKS, greet, 0)
    loads = [
        pltpu.make_async_copy(source, target, local.at[i])
        for i, (source, target) in enumerate(
            (
                (tok_hbm, tok_ref), (wk_hbm, wk_ref), (wv_hbm, wv_ref), (wq_hbm, wq_ref),
                (wp_hbm, wp_ref),
            )
        )
    ]
    for load in loads:
        load.start()

    started = []

    def remote(source, target_ref, index, target):
        return pltpu.make_async_remote_copy(
            src_ref=source, dst_ref=target_ref, send_sem=send.at[index],
            recv_sem=recv.at[index], device_id=target, device_id_type=MESH,
        )

    mode = ["start"]

    def go(source, target_ref, index, target):
        copy = remote(source, target_ref, index, target)
        if mode[0] == "wait":
            copy.wait_send()
            return
        copy.start()
        if mode[0] == "start":
            started.append(copy)

    def got(target_ref, index):
        if mode[0] != "wait":
            remote(target_ref, target_ref, index, partner).wait_recv()

    def rows(start, count=64):
        return pl.ds(pl.multiple_of(start, 32), count)

    weights = (wk_ref, wv_ref, wq_ref)
    quarters = (y_down, y_up, y_far)

    widths = (512, 512, 256)

    def part(a, quarter, start, count=64):
        return buf.at[a, quarter, rows(start, count), 0 : widths[a]]

    def direct(a):
        base = a * 30
        own_x, own_z = 64 * x, 256 + 64 * z
        w = weights[a]
        go(w.at[rows(own_x), 0 : widths[a]], part(a, y, own_x), base + 0, to["yp"])
        go(w.at[rows(own_z), 0 : widths[a]], part(a, y, own_z), base + 1, to["ym"])
        go(w.at[rows(own_x), 0 : widths[a]], part(a, y, own_x), base + 2, to["ym"])
        go(w.at[rows(own_z), 0 : widths[a]], part(a, y, own_z), base + 3, to["yp"])

    def ring_base(a, item, ring):
        return a * 30 + 6 + item * 8 + ring * 4

    own_row = (64 * x, 256 + 64 * z)
    down_row = (64 * x_down, 256 + 64 * z_down)
    up_row = (64 * x_up, 256 + 64 * z_up)
    far_row = (64 * x_far, 256 + 64 * z_far)
    ups = ("xp", "zp")
    downs = ("xm", "zm")

    def spread(a, item, ring):
        base = ring_base(a, item, ring)
        piece = part(a, quarters[item], own_row[ring])
        go(piece, piece, base + 0, to[ups[ring]])
        go(piece, piece, base + 1, to[downs[ring]])

    def relay(a, item, ring):
        base = ring_base(a, item, ring)
        q = quarters[item]
        got(part(a, q, down_row[ring]), base + 0)
        piece = part(a, q, down_row[ring], 32)
        go(piece, piece, base + 2, to[ups[ring]])
        got(part(a, q, up_row[ring]), base + 1)
        piece = part(a, q, up_row[ring] + 32, 32)
        go(piece, piece, base + 3, to[downs[ring]])

    def settle(a):
        for item in range(3):
            for ring in range(2):
                base = ring_base(a, item, ring)
                q = quarters[item]
                got(part(a, q, far_row[ring], 32), base + 2)
                got(part(a, q, far_row[ring] + 32, 32), base + 3)

    def first(a):
        base = a * 30
        piece = part(a, y_down, own_row[0])
        got(piece, base + 0)
        go(piece, piece, base + 4, to["yp"])
        spread(a, 0, 0)
        piece = part(a, y_up, own_row[1])
        got(piece, base + 1)
        go(piece, piece, base + 5, to["ym"])
        spread(a, 1, 1)
        got(part(a, y_up, own_row[0]), base + 2)
        spread(a, 1, 0)
        got(part(a, y_down, own_row[1]), base + 3)
        spread(a, 0, 1)

    def second(a):
        relay(a, 0, 0)
        relay(a, 1, 1)

    def third(a):
        base = a * 30
        got(part(a, y_far, own_row[0]), base + 4)
        spread(a, 2, 0)
        got(part(a, y_far, own_row[1]), base + 5)
        spread(a, 2, 1)
        relay(a, 1, 0)
        relay(a, 0, 1)

    def fourth(a):
        relay(a, 2, 0)
        relay(a, 2, 1)

    def query_part(quarter, start, count):
        return buf.at[2, quarter, start : start + count, 256:512]

    def query_direct():
        go(wq_ref.at[:, 256:512], query_part(y, 0, 512), 232, to["yp"])
        go(wq_ref.at[:, 256:512], query_part(y, 0, 512), 233, to["ym"])

    def query_relay():
        got(query_part(y_down, 0, 512), 232)
        go(query_part(y_down, 0, 256), query_part(y_down, 0, 256), 234, to["yp"])
        got(query_part(y_up, 0, 512), 233)
        go(query_part(y_up, 256, 256), query_part(y_up, 256, 256), 235, to["ym"])

    def query_settle():
        got(query_part(y_far, 0, 256), 234)
        got(query_part(y_far, 256, 256), 235)

    pool_base = 90

    def pool_direct():
        go(wp_ref, pbuf.at[y], pool_base + 0, to["yp"])
        go(wp_ref, pbuf.at[y], pool_base + 1, to["ym"])

    def pool_relay():
        got(pbuf.at[y_down], pool_base + 0)
        piece = pbuf.at[y_down, 0:256, :]
        go(piece, piece, pool_base + 2, to["yp"])
        got(pbuf.at[y_up], pool_base + 1)
        piece = pbuf.at[y_up, 256:512, :]
        go(piece, piece, pool_base + 3, to["ym"])

    def pool_settle():
        got(pbuf.at[y_far, 0:256, :], pool_base + 2)
        got(pbuf.at[y_far, 256:512, :], pool_base + 3)

    def own(a):
        acc[a] = jnp.dot(x_s[y], weights[a][...], preferred_element_type=jnp.float32)

    def rest(a, low=0, high=512):
        total = acc[a][:, low:high]
        for q in quarters:
            total = total + jnp.dot(
                x_s[q], buf[a, q, :, low:high], preferred_element_type=jnp.float32
            )
        return total

    stays = sp // 8 == core

    def head_copy(a, h, of_core, source):
        return pltpu.make_async_remote_copy(
            src_ref=heads_s.at[a, h, of_core],
            dst_ref=recv_s.at[source, a * 64 : a * 64 + 64, :],
            send_sem=send.at[97 + a * 16 + h * 2 + of_core],
            recv_sem=recv.at[97 + a * 16 + source],
            device_id={"sp": 8 * core + h, "fs": y, "tp": of_core}, device_id_type=MESH,
        )

    def leaves(h, of_core):
        return jnp.logical_not(stays & (h == sp % 8) & (of_core == core))

    def deliver(a, total, low=0):
        count = total.shape[1] // HEAD_DIM
        turned = total.T.reshape(count, HEAD_DIM, BLOCK)
        if a != 1:
            factor = lax.rsqrt(jnp.mean(turned * turned, axis=1, keepdims=True) + EPS)
            gain_row = (kg_ref if a == 0 else qg_ref)[...]
            gain = jnp.broadcast_to(gain_row, (HEAD_DIM, HEAD_DIM)).T[:, 0:1]
            turned = turned * factor * gain[None]
        turned = turned.astype(jnp.bfloat16)
        heads_s[a, low : low + count, 0] = turned[:, :, :HALF]
        heads_s[a, low : low + count, 1] = turned[:, :, HALF:]

        def send_head(i, unused):
            h, of_core = low + (sp + i // 2) % count, i % 2

            @pl.when(leaves(h, of_core))
            def _():
                head_copy(a, h, of_core, sp).start()

            return unused

        lax.fori_loop(0, 2 * count, send_head, 0)

        @pl.when(stays & (sp % 8 >= low) & (sp % 8 < low + count))
        def _():
            recv_s[sp, a * 64 : a * 64 + 64, :] = heads_s[a, sp % 8, core]

    def wa_part(quarter, of_core, start, count):
        return wa_all.at[
            pl.ds(pl.multiple_of(of_core * 512 + start, 128), count),
            pl.ds(pl.multiple_of(quarter * 512, 512), 512),
        ]

    def wp_part(quarter, of_core, start, count):
        return wp_all.at[
            pl.ds(pl.multiple_of(of_core * 256 + start, 128), count),
            pl.ds(pl.multiple_of(quarter * 512, 512), 512),
        ]

    def share(quarter, index):
        go(wa_part(quarter, core, 0, 512), wa_part(quarter, core, 0, 512), index, partner)
        go(wp_part(quarter, core, 0, 256), wp_part(quarter, core, 0, 256), index + 1, partner)

    def shared(quarter, index):
        got(wa_part(quarter, 1 - core, 0, 512), index)
        got(wp_part(quarter, 1 - core, 0, 256), index + 1)

    def weights_start():
        go(wao_ref, wa_part(y, core, 0, 512), 147, to["yp"])
        go(wpo_ref, wp_part(y, core, 0, 256), 148, to["yp"])
        go(wao_ref, wa_part(y, core, 0, 512), 149, to["ym"])
        go(wpo_ref, wp_part(y, core, 0, 256), 150, to["ym"])
        go(wao_ref, wa_part(y, core, 0, 512), 155, partner)
        go(wpo_ref, wp_part(y, core, 0, 256), 156, partner)

    def weights_middle():
        got(wa_part(y_down, core, 0, 512), 147)
        got(wp_part(y_down, core, 0, 256), 148)
        go(wa_part(y_down, core, 0, 256), wa_part(y_down, core, 0, 256), 151, to["yp"])
        go(wp_part(y_down, core, 0, 128), wp_part(y_down, core, 0, 128), 152, to["yp"])
        got(wa_part(y_up, core, 0, 512), 149)
        got(wp_part(y_up, core, 0, 256), 150)
        go(wa_part(y_up, core, 256, 256), wa_part(y_up, core, 256, 256), 153, to["ym"])
        go(wp_part(y_up, core, 128, 128), wp_part(y_up, core, 128, 128), 154, to["ym"])
        share(y_down, 157)
        share(y_up, 159)

    def weights_late():
        got(wa_part(y_far, core, 0, 256), 151)
        got(wp_part(y_far, core, 0, 128), 152)
        got(wa_part(y_far, core, 256, 256), 153)
        got(wp_part(y_far, core, 128, 128), 154)
        share(y_far, 161)

    def weights_end():
        shared(y, 155)
        shared(y_down, 157)
        shared(y_up, 159)
        shared(y_far, 161)

    mine_at = pl.ds(pl.multiple_of(core * HALF, HALF), HALF)
    other_at = pl.ds(pl.multiple_of((1 - core) * HALF, HALF), HALF)

    def turned(block):
        return block.astype(jnp.float32).T.astype(jnp.bfloat16)

    def forward(a, r):
        return pltpu.make_async_remote_copy(
            src_ref=recv_s.at[r, a * 64 : a * 64 + 64, :],
            dst_ref=other_s.at[r, a * 64 : a * 64 + 64, :],
            send_sem=send.at[200 + a * 16 + r], recv_sem=recv.at[200 + a * 16 + r],
            device_id=partner, device_id_type=MESH,
        )

    def place(a, r, block, at):
        if a == 0:
            k_s[r, at, 0:64] = turned(block)
        elif a == 1:
            v_s[r, :, at] = block
        else:
            q_s[r, 0:64, :] = block

    def take(a):
        def pair(n, unused):
            places_now = [(sp + 2 * n) % BLOCKS, (sp + 2 * n + 1) % BLOCKS]
            for r in places_now:
                @pl.when(jnp.logical_not(stays & (r == sp)))
                def _():
                    head_copy(a, 0, 0, r).wait_recv()

                if a < 2:
                    forward(a, r).start()
            for r in places_now:
                place(a, r, recv_s[r, a * 64 : a * 64 + 64, :], mine_at)
            return unused

        lax.fori_loop(0, BLOCKS // 2, pair, 0)

    def take_other(a):
        def pair(n, unused):
            places_now = [(sp + 2 * n) % BLOCKS, (sp + 2 * n + 1) % BLOCKS]
            for r in places_now:
                forward(a, r).wait_recv()
            for r in places_now:
                place(a, r, other_s[r, a * 64 : a * 64 + 64, :], other_at)
            return unused

        lax.fori_loop(0, BLOCKS // 2, pair, 0)

    scale = LOG2E / math.sqrt(HEAD_DIM)
    half = core
    offset_m[...] = jnp.zeros_like(offset_m)
    offset_m[:, 0:8] = jnp.broadcast_to(offset_ref[...], (8, 8))
    gains_m[:, 0:256] = jnp.broadcast_to(pg_ref[...].reshape(1, 256), (16, 256))
    gains_m[:, 256:768] = jnp.broadcast_to(ag_ref[...].reshape(1, 512), (16, 512))
    tri_s[...] = jnp.where(
        lax.broadcasted_iota(jnp.int32, (HALF, HALF), 0)
        <= lax.broadcasted_iota(jnp.int32, (HALF, HALF), 1),
        1.0,
        0.0,
    ).astype(jnp.bfloat16)
    for load in loads:
        load.wait()
    pl.semaphore_wait(barrier, 33)
    direct(0)
    go(tok_ref, tok_s, 94, partner)
    direct(1)
    go(offset_m, offset_s, 163, partner)
    go(gains_m, gains_o, 146, partner)
    got(tok_s, 94)

    mine_f = tok_ref[...].astype(jnp.float32)
    other_f = tok_s[...].astype(jnp.float32)
    squares = jnp.sum(mine_f * mine_f, axis=1, keepdims=True) + jnp.sum(
        other_f * other_f, axis=1, keepdims=True
    )
    factor = lax.rsqrt(squares / 2048.0 + EPS)
    for j in range(2):
        columns = slice(512 * j, 512 * j + 512)
        at_mine = 2 * core + j
        at_other = 2 * (1 - core) + j
        x_s[at_mine] = (
            tok_ref[:, columns].astype(jnp.float32) * factor * gain_ref[at_mine]
        ).astype(jnp.bfloat16)
        x_s[at_other] = (
            tok_s[:, columns].astype(jnp.float32) * factor * gain_ref[at_other]
        ).astype(jnp.bfloat16)

    first(0)
    own(0)
    own(1)
    first(1)
    direct(2)
    second(0)
    own(2)
    third(0)
    second(1)
    first(2)
    query_direct()
    acc_p[...] = jnp.dot(x_s[y], wp_ref[...], preferred_element_type=jnp.float32)
    fourth(0)
    third(1)
    settle(0)
    deliver(0, rest(0))
    fourth(1)
    second(2)
    settle(1)
    deliver(1, rest(1))
    third(2)
    query_relay()
    pool_direct()
    got(offset_s, 163)
    of_core = jnp.where(sp // 8 == core, offset_m[0:1, :], offset_s[0:1, :])
    chosen = lax.broadcasted_iota(jnp.int32, (1, 128), 1) == sp % 8
    offset = jnp.sum(jnp.where(chosen, of_core, 0.0), axis=1, keepdims=True) * math.sqrt(HEAD_DIM)
    column = lax.broadcasted_iota(jnp.int32, (BLOCK, 64), 1)
    terms = split_terms(jnp.broadcast_to(offset, (BLOCK, 64)))
    extra = jnp.where(
        column == 0,
        terms[0].astype(jnp.float32),
        jnp.where(
            column == 1,
            terms[1].astype(jnp.float32),
            jnp.where(column == 2, terms[2].astype(jnp.float32), 0.0),
        ),
    ).astype(jnp.bfloat16)
    row = lax.broadcasted_iota(jnp.int32, (64, HALF), 0)
    ones = jnp.where(row < 3, 1.0, 0.0).astype(jnp.bfloat16)
    mask_s[...] = jnp.where(
        lax.broadcasted_iota(jnp.int32, (BLOCK, HALF), 0)
        < lax.broadcasted_iota(jnp.int32, (BLOCK, HALF), 1) + half * HALF,
        0.0,
        -1e30,
    )
    acc_s[...] = jnp.zeros_like(acc_s)
    carry_s[...] = jnp.zeros_like(carry_s)


    def fill(r, unused):
        k_s[r, :, 64:128] = extra
        q_s[r, 64:128, :] = ones
        return unused

    lax.fori_loop(0, BLOCKS, fill, 0)
    mine_half = pl.ds(pl.multiple_of(core * HALF, HALF), HALF)
    other_half = pl.ds(pl.multiple_of((1 - core) * HALF, HALF), HALF)
    fourth(2)
    take(0)
    settle(2)
    deliver(2, rest(2, 0, 256))
    query_settle()
    deliver(2, rest(2, 256, 512), 4)
    take(1)
    take_other(0)
    pool_relay()
    take_other(1)
    take(2)
    weights_start()
    stores = [
        pltpu.make_async_copy(wao_ref, wa_part(y, core, 0, 512), local.at[5]),
        pltpu.make_async_copy(wpo_ref, wp_part(y, core, 0, 256), local.at[6]),
    ]
    for store in stores:
        store.start()

    def pool_tail():
        tail = pool_in.at[BLOCK - 16 : BLOCK, :]
        go(tail, before_s, 95, {"sp": (sp + 1) % BLOCKS, "fs": y, "tp": core})

    def pool_swap():
        go(pooled_s.at[other_at, :], pool_rows.at[core], 96, partner)

    def pool_project():
        pool_settle()
        total = acc_p[...]
        for q in quarters:
            total = total + jnp.dot(x_s[q], pbuf[q], preferred_element_type=jnp.float32)
        pool_in[...] = total.astype(jnp.bfloat16)
        pool_tail()

    def pool_windows():
        got(before_s, 95)
        current = pool_in[...].astype(jnp.float32)
        before = jnp.where(sp == 0, 0.0, before_s[...].astype(jnp.float32))

        def behind(values, count):
            return jnp.concatenate([jnp.zeros((count, values.shape[1]), jnp.float32), values[:-count]], axis=0)

        extended = jnp.concatenate([before, current], axis=0)
        sum_2 = extended + behind(extended, 1)
        sum_4 = sum_2 + behind(sum_2, 2)
        sum_8 = sum_4 + behind(sum_4, 4)
        sum_16 = sum_8 + behind(sum_8, 8)
        position = lax.broadcasted_iota(jnp.int32, (BLOCK, 128), 0) + (sp * BLOCK + 1)
        for group in range(2):
            columns = slice(128 * group, 128 * group + 128)
            low, high = ((sum_2, sum_8), (sum_4, sum_16))[group]
            window = jnp.where(core == 0, 2 << group, 8 << group)
            summed = jnp.where(core == 0, low[16:, columns], high[16:, columns])
            counted = jnp.minimum(position, window).astype(jnp.float32)
            centered = (summed / counted - current[:, columns]).astype(jnp.bfloat16)
            mixed = jnp.dot(centered, mix_ref[group], preferred_element_type=jnp.float32)
            pooled_s[:, columns] = (mixed * scale_ref[:, columns]).astype(jnp.bfloat16)
        pool_swap()
        pool_rows[core] = pooled_s[mine_at, :]

    zs, ls, ws = (z0, z1, z2), (l0, l1, l2), (w0, w1, w2)

    first_row = jnp.where(sp == BLOCKS - 1, 1, sp + 1)

    def places(state):
        step, r, distance = state
        row_at = jnp.where((step < 0) | (step >= 136), BLOCKS, r)
        return (row_at, r, jnp.maximum(r - distance, 0))

    def advance(state):
        step, r, distance = state
        diagonal = step < BLOCKS - 1
        turn = step == BLOCKS - 1
        done = distance >= r
        next_row = jnp.where(r == BLOCKS - 1, 1, r + 1)
        r_after = jnp.where(
            diagonal,
            jnp.maximum(step + 1, 0),
            jnp.where(turn, first_row, jnp.where(done, next_row, r)),
        )
        after = jnp.where(diagonal, 0, jnp.where(turn | done, 1, distance + 1))
        return (step + 1, r_after, after)

    def scores(state, b, masked):
        unused_row, r, g = places(state)
        z = jnp.dot(k_s[g], q_s[r], preferred_element_type=jnp.float32) * scale
        if masked:
            z = z + mask_s[...]
        zs[b][...] = z

    def soften(b):
        ls[b][...] = jnp.log2(1.0 + jnp.exp2(zs[b][...])).astype(jnp.bfloat16)

    def weigh(state, b):
        row_at = places(state)[0]
        late = jnp.dot(tri_s[...], ls[b][HALF:, :], preferred_element_type=jnp.float32)
        early = jnp.dot(tri_s[...], ls[b][:HALF, :], preferred_element_type=jnp.float32)
        carry = carry_s[row_at][0:1]
        before = carry + late[0:1]
        ws[b][HALF:, :] = jnp.exp2(zs[b][HALF:, :] - (late + carry)).astype(jnp.bfloat16)
        ws[b][:HALF, :] = jnp.exp2(zs[b][:HALF, :] - (early + before)).astype(jnp.bfloat16)
        carry_s[row_at] = jnp.broadcast_to(before + early[0:1], (8, HALF))

    def gather_values(state, b):
        row_at, unused_row, g = places(state)
        acc_s[row_at] = acc_s[row_at] + jnp.dot(
            v_s[g], ws[b][...], preferred_element_type=jnp.float32
        )

    def return_row(state):
        step, r, distance = state

        @pl.when((distance == r) & (step >= 0) & (step < 136))
        def _():
            done_s[r] = acc_s[r].astype(jnp.bfloat16)

            @pl.when(r != sp)
            def _():
                pltpu.make_async_remote_copy(
                    src_ref=done_s.at[r], dst_ref=o_ref.at[sp], send_sem=send.at[180 + r],
                    recv_sem=recv.at[180 + sp], device_id={"sp": r, "fs": y, "tp": core}, device_id_type=MESH,
                ).start()

    hooks = ((1, pool_project), (3, pool_windows), (6, weights_middle), (11, weights_late))

    def steps(masked):
        def body(n, states):
            if not masked:
                for turn, hook in hooks:
                    pl.when(n == turn)(hook)
            states = list(states)
            for unused_step in range(9):
                states.append(advance(states[-1]))
            for u in range(9):
                gather_values(states[u], (u + 2) % 3)
                weigh(states[u + 1], u % 3)
                soften((u + 1) % 3)
                scores(states[u + 3], (u + 2) % 3, masked)
            finished = functools.reduce(
                jnp.logical_or, [distance == r for unused_step, r, distance in states[:9]]
            )

            @pl.when(finished)
            def _():
                for u in range(9):
                    return_row(states[u])

            return tuple(states[9:])

        return body

    first_states = tuple(
        (jnp.int32(step), jnp.int32(0), jnp.int32(0)) for step in (-5, -4, -3, -2)
    )
    states = lax.fori_loop(0, 2, steps(True), first_states)
    mode[0] = "hook"
    lax.fori_loop(0, 14, steps(False), states)
    mode[0] = "start"
    for store in stores:
        store.wait()
    o_ref[sp] = done_s[sp]
    weights_end()
    got(gains_o, 146)
    got(pool_rows.at[1 - core], 96)

    def settle_row(i, unused):
        r = (sp + i) % BLOCKS
        copy = pltpu.make_async_remote_copy(
            src_ref=done_s.at[r], dst_ref=o_ref.at[r], send_sem=send.at[180 + r],
            recv_sem=recv.at[180 + r], device_id={"sp": r, "fs": y, "tp": core},
            device_id_type=MESH,
        )
        copy.wait_send()
        copy.wait_recv()
        return unused

    lax.fori_loop(1, BLOCKS, settle_row, 0)

    def gain_rows(columns):
        mine_gain = gains_m[0:1, columns].astype(jnp.float32)
        other_gain = gains_o[0:1, columns].astype(jnp.float32)
        low = jnp.where(core == 0, mine_gain, other_gain)
        high = jnp.where(core == 0, other_gain, mine_gain)
        return jnp.concatenate([low, high], axis=1)

    attended = o_ref[...].reshape(HEADS * HEAD_DIM, HALF).astype(jnp.float32).T
    factor = lax.rsqrt(jnp.mean(attended * attended, axis=1, keepdims=True) + EPS)
    attn_normed = (attended * factor * gain_rows(slice(256, 768))).astype(jnp.bfloat16)
    pooled = jnp.concatenate([pool_rows[0], pool_rows[1]], axis=1).astype(jnp.float32)
    factor = lax.rsqrt(jnp.mean(pooled * pooled, axis=1, keepdims=True) + EPS)
    pool_normed = (pooled * factor * gain_rows(slice(0, 256))).astype(jnp.bfloat16)
    for j in range(4):
        columns = slice(512 * j, 512 * j + 512)
        side = (left_ref, right_ref)[j // 2]
        side[:, 512 * (j % 2) : 512 * (j % 2) + 512] = (
            jnp.dot(pool_normed, wp_all[:, columns], preferred_element_type=jnp.float32)
            + jnp.dot(attn_normed, wa_all[:, columns], preferred_element_type=jnp.float32)
        ).astype(jnp.bfloat16)

    for copy in started:
        copy.wait_send()
    mode[0] = "wait"
    for resend in (pool_tail, pool_swap, weights_middle, weights_late):
        resend()

    def settle_heads(i, unused):
        for a in range(3):
            @pl.when(leaves(i // 2, i % 2))
            def _():
                head_copy(a, i // 2, i % 2, sp).wait_send()

        for a in range(2):
            forward(a, i).wait_send()
        return unused

    lax.fori_loop(0, BLOCKS, settle_heads, 0)


def mixer(*operands):
    vmem = pl.BlockSpec(memory_space=pltpu.VMEM)
    here = pl.BlockSpec(memory_space=pl.ANY)
    return pl.pallas_call(
        mixer_kernel,
        out_shape=(jax.ShapeDtypeStruct((HALF, 1024), jnp.bfloat16),) * 2,
        in_specs=[here, vmem, here, here, here, here, *[vmem] * 5, here, here, vmem, vmem],
        out_specs=(vmem, vmem),
        scratch_shapes=[
            pltpu.VMEM((512, 1024), jnp.bfloat16),
            *[pltpu.VMEM((512, 512), jnp.bfloat16)] * 3,
            pltpu.VMEM((512, 256), jnp.bfloat16),
            pltpu.VMEM((3, 4, 512, 512), jnp.bfloat16),
            pltpu.VMEM((4, 512, 256), jnp.bfloat16),
            pltpu.VMEM((512, 1024), jnp.bfloat16),
            pltpu.VMEM((4, 512, 512), jnp.bfloat16),
            pltpu.VMEM((3, 512, 512), jnp.float32),
            pltpu.VMEM((512, 256), jnp.float32),
            pltpu.VMEM((3, 8, 2, HEAD_DIM, HALF), jnp.bfloat16),
            pltpu.VMEM((512, 256), jnp.bfloat16),
            pltpu.VMEM((16, 256), jnp.bfloat16),
            pltpu.VMEM((512, 256), jnp.bfloat16),
            pltpu.VMEM((2, HALF, 256), jnp.bfloat16),
            pltpu.VMEM((BLOCKS, 3 * HEAD_DIM, HALF), jnp.bfloat16),
            pltpu.VMEM((BLOCKS, 2 * HEAD_DIM, HALF), jnp.bfloat16),
            pltpu.VMEM((BLOCKS, HEAD_DIM, HALF), jnp.bfloat16),
            pltpu.VMEM((512, 2048), jnp.bfloat16),
            pltpu.VMEM((1024, 2048), jnp.bfloat16),
            pltpu.VMEM((16, 768), jnp.bfloat16),
            pltpu.VMEM((16, 768), jnp.bfloat16),
            pltpu.VMEM((8, 128), jnp.float32),
            pltpu.VMEM((8, 128), jnp.float32),
            pltpu.VMEM((BLOCKS, 128, HALF), jnp.bfloat16),
            pltpu.VMEM((BLOCKS, BLOCK, 128), jnp.bfloat16),
            pltpu.VMEM((BLOCKS, HEAD_DIM, BLOCK), jnp.bfloat16),
            pltpu.VMEM((HALF, HALF), jnp.bfloat16),
            pltpu.VMEM((BLOCK, HALF), jnp.float32),
            pltpu.VMEM((BLOCKS + 1, HEAD_DIM, HALF), jnp.float32),
            pltpu.VMEM((BLOCKS + 1, 8, HALF), jnp.float32),
            pltpu.VMEM((BLOCKS, HEAD_DIM, HALF), jnp.bfloat16),
            *[pltpu.VMEM((BLOCK, HALF), jnp.float32)] * 3,
            *[pltpu.VMEM((BLOCK, HALF), jnp.bfloat16)] * 6,
            pltpu.SemaphoreType.DMA((236,)),
            pltpu.SemaphoreType.DMA((236,)),
            pltpu.SemaphoreType.DMA((7,)),
        ],
        compiler_params=pltpu.CompilerParams(
            collective_id=0, has_side_effects=True, vmem_limit_bytes=62 * 1024 * 1024,
        ),
        cost_estimate=pl.CostEstimate(
            flops=45_000_000_000, bytes_accessed=8_000_000, transcendentals=50_000_000
        ),
        name="token_mixer",
    )(*operands)


def join_kernel(left_ref, right_ref, joined_ref):
    joined_ref[:, :1024] = left_ref[...]
    joined_ref[:, 1024:] = right_ref[...]


def join(left, right):
    side = pl.BlockSpec((HALF // 2, 1024), lambda i: (i, 0))
    return pl.pallas_call(
        join_kernel,
        grid=(2,),
        out_shape=jax.ShapeDtypeStruct((HALF, 2048), jnp.bfloat16),
        in_specs=[side, side],
        out_specs=pl.BlockSpec((HALF // 2, 2048), lambda i: (i, 0)),
        name="join_sides",
    )(left, right)


def shards(
    tokens,
    norm_gain,
    w_pool_in,
    w_query,
    w_key,
    w_value,
    query_gain,
    key_gain,
    stick_offset,
    pool_mix,
    pool_scale,
    pool_gain,
    attn_gain,
    w_out_pool,
    w_out_attn,
):
    left, right = mixer(
        tokens[0], norm_gain.reshape(4, 1, 512), w_key, w_value, w_query, w_pool_in,
        key_gain.reshape(1, HEAD_DIM), query_gain.reshape(1, HEAD_DIM), pool_mix,
        pool_scale.reshape(1, 256), stick_offset.reshape(1, 8), w_out_pool, w_out_attn,
        pool_gain, attn_gain,
    )
    return join(left, right)[None]


def solution(mesh):
    in_specs = (
        P("fs", "sp", "tp"),
        P(),
        P("fs", "tp"),
        P("fs", "tp"),
        P("fs", "tp"),
        P("fs", "tp"),
        P(),
        P(),
        P("tp"),
        P("tp", None, None),
        P("tp"),
        P("tp"),
        P("tp"),
        P("tp", "fs"),
        P("tp", "fs"),
    )
    out_specs = P("fs", ("sp", "tp"), None)
    return jax.shard_map(shards, mesh=mesh, in_specs=in_specs, out_specs=out_specs, check_vma=False)
```

```python
import functools
import math

import jax
import jax.numpy as jnp
from jax import lax
from jax.experimental import pallas as pl
from jax.experimental.pallas import tpu as pltpu
from jax.sharding import PartitionSpec as P

HEADS = 16
HEAD_DIM = 64
POOL = 512
POOL_GROUPS = 4
BLOCKS = 16
HALF = 256
BLOCK = 512

EPS = 1e-06
LOG2E = 1.4426950408889634


def split_terms(value):
    high = value.astype(jnp.bfloat16)
    rest = value - high.astype(jnp.float32)
    middle = rest.astype(jnp.bfloat16)
    low = (rest - middle.astype(jnp.float32)).astype(jnp.bfloat16)
    return (high, middle, low)


MESH = pl.DeviceIdType.MESH


def mixer_kernel(
    tok_hbm, gain_ref, wk_hbm, wv_hbm, wq_hbm, wp_hbm, kg_ref, qg_ref, mix_ref, scale_ref,
    offset_ref, wpo_ref, wao_ref, pg_ref, ag_ref,
    left_ref, right_ref,
    tok_ref, wk_ref, wv_ref, wq_ref, wp_ref,
    buf, pbuf, tok_s, x_s, acc, acc_p, heads_s, pool_in, before_s, pooled_s, pool_rows,
    recv_s, other_s, o_ref, wp_all, wa_all, gains_m, gains_o, offset_m, offset_s,
    q_s, k_s, v_s, tri_s, mask_s, acc_s, carry_s, done_s,
    z0, z1, z2, l0, l1, l2, w0, w1, w2, send, recv, local, known,
):
    sp, y, core = lax.axis_index("sp"), lax.axis_index("fs"), lax.axis_index("tp")
    z, x = sp // 4, sp % 4
    y_up, y_down, y_far = (y + 1) % 4, (y + 3) % 4, (y + 2) % 4
    x_up, x_down, x_far = (x + 1) % 4, (x + 3) % 4, (x + 2) % 4
    z_up, z_down, z_far = (z + 1) % 4, (z + 3) % 4, (z + 2) % 4

    def at(z_to, x_to, y_to, core_to):
        return {"sp": z_to * 4 + x_to, "fs": y_to, "tp": core_to}

    partner = at(z, x, y, 1 - core)
    to = {
        "yp": at(z, x, y_up, core), "ym": at(z, x, y_down, core),
        "xp": at(z, x_up, y, core), "xm": at(z, x_down, y, core),
        "zp": at(z_up, x, y, core), "zm": at(z_down, x, y, core),
    }

    barrier = pltpu.get_barrier_semaphore()
    for target in (partner, *to.values()):
        pl.semaphore_signal(barrier, inc=1, device_id=target, device_id_type=MESH)
    loads = [
        pltpu.make_async_copy(source, target, local.at[i])
        for i, (source, target) in enumerate(
            (
                (tok_hbm, tok_ref), (wk_hbm, wk_ref), (wv_hbm, wv_ref), (wq_hbm, wq_ref),
                (wp_hbm, wp_ref),
            )
        )
    ]
    for load in loads:
        load.start()

    started = []

    def remote(source, target_ref, index, target):
        return pltpu.make_async_remote_copy(
            src_ref=source, dst_ref=target_ref, send_sem=send.at[index],
            recv_sem=recv.at[index], device_id=target, device_id_type=MESH,
        )

    mode = ["start"]

    def go(source, target_ref, index, target):
        copy = remote(source, target_ref, index, target)
        if mode[0] == "wait":
            copy.wait_send()
            return
        copy.start()
        if mode[0] == "start":
            started.append(copy)

    def got(target_ref, index):
        if mode[0] != "wait":
            remote(target_ref, target_ref, index, partner).wait_recv()

    def rows(start, count=64):
        return pl.ds(pl.multiple_of(start, 32), count)

    weights = (wk_ref, wv_ref, wq_ref)
    quarters = (y_down, y_up, y_far)

    widths = (512, 512, 256)

    def part(a, quarter, start, count=64):
        return buf.at[a, quarter, rows(start, count), 0 : widths[a]]

    def direct(a):
        base = a * 30
        own_x, own_z = 64 * x, 256 + 64 * z
        w = weights[a]
        go(w.at[rows(own_x), 0 : widths[a]], part(a, y, own_x), base + 0, to["yp"])
        go(w.at[rows(own_z), 0 : widths[a]], part(a, y, own_z), base + 1, to["ym"])
        go(w.at[rows(own_x), 0 : widths[a]], part(a, y, own_x), base + 2, to["ym"])
        go(w.at[rows(own_z), 0 : widths[a]], part(a, y, own_z), base + 3, to["yp"])

    def ring_base(a, item, ring):
        return a * 30 + 6 + item * 8 + ring * 4

    own_row = (64 * x, 256 + 64 * z)
    down_row = (64 * x_down, 256 + 64 * z_down)
    up_row = (64 * x_up, 256 + 64 * z_up)
    far_row = (64 * x_far, 256 + 64 * z_far)
    ups = ("xp", "zp")
    downs = ("xm", "zm")

    def spread(a, item, ring):
        base = ring_base(a, item, ring)
        piece = part(a, quarters[item], own_row[ring])
        go(piece, piece, base + 0, to[ups[ring]])
        go(piece, piece, base + 1, to[downs[ring]])

    def relay(a, item, ring):
        base = ring_base(a, item, ring)
        q = quarters[item]
        got(part(a, q, down_row[ring]), base + 0)
        piece = part(a, q, down_row[ring], 32)
        go(piece, piece, base + 2, to[ups[ring]])
        got(part(a, q, up_row[ring]), base + 1)
        piece = part(a, q, up_row[ring] + 32, 32)
        go(piece, piece, base + 3, to[downs[ring]])

    def settle(a):
        for item in range(3):
            for ring in range(2):
                base = ring_base(a, item, ring)
                q = quarters[item]
                got(part(a, q, far_row[ring], 32), base + 2)
                got(part(a, q, far_row[ring] + 32, 32), base + 3)

    def first(a):
        base = a * 30
        piece = part(a, y_down, own_row[0])
        got(piece, base + 0)
        go(piece, piece, base + 4, to["yp"])
        spread(a, 0, 0)
        piece = part(a, y_up, own_row[1])
        got(piece, base + 1)
        go(piece, piece, base + 5, to["ym"])
        spread(a, 1, 1)
        got(part(a, y_up, own_row[0]), base + 2)
        spread(a, 1, 0)
        got(part(a, y_down, own_row[1]), base + 3)
        spread(a, 0, 1)

    def second(a):
        relay(a, 0, 0)
        relay(a, 1, 1)

    def third(a):
        base = a * 30
        got(part(a, y_far, own_row[0]), base + 4)
        spread(a, 2, 0)
        got(part(a, y_far, own_row[1]), base + 5)
        spread(a, 2, 1)
        relay(a, 1, 0)
        relay(a, 0, 1)

    def fourth(a):
        relay(a, 2, 0)
        relay(a, 2, 1)

    def query_part(quarter, start, count):
        return buf.at[2, quarter, start : start + count, 256:512]

    def query_direct():
        go(wq_ref.at[:, 256:512], query_part(y, 0, 512), 232, to["yp"])
        go(wq_ref.at[:, 256:512], query_part(y, 0, 512), 233, to["ym"])

    def query_relay():
        got(query_part(y_down, 0, 512), 232)
        go(query_part(y_down, 0, 256), query_part(y_down, 0, 256), 234, to["yp"])
        got(query_part(y_up, 0, 512), 233)
        go(query_part(y_up, 256, 256), query_part(y_up, 256, 256), 235, to["ym"])

    def query_settle():
        got(query_part(y_far, 0, 256), 234)
        got(query_part(y_far, 256, 256), 235)

    pool_base = 90

    def pool_direct():
        go(wp_ref, pbuf.at[y], pool_base + 0, to["yp"])
        go(wp_ref, pbuf.at[y], pool_base + 1, to["ym"])

    def pool_relay():
        got(pbuf.at[y_down], pool_base + 0)
        piece = pbuf.at[y_down, 0:256, :]
        go(piece, piece, pool_base + 2, to["yp"])
        got(pbuf.at[y_up], pool_base + 1)
        piece = pbuf.at[y_up, 256:512, :]
        go(piece, piece, pool_base + 3, to["ym"])

    def pool_settle():
        got(pbuf.at[y_far, 0:256, :], pool_base + 2)
        got(pbuf.at[y_far, 256:512, :], pool_base + 3)

    def own(a):
        acc[a] = jnp.dot(x_s[y], weights[a][...], preferred_element_type=jnp.float32)

    def rest(a, low=0, high=512):
        total = acc[a][:, low:high]
        for q in quarters:
            total = total + jnp.dot(
                x_s[q], buf[a, q, :, low:high], preferred_element_type=jnp.float32
            )
        return total

    stays = sp // 8 == core

    def head_copy(a, h, of_core, source):
        return pltpu.make_async_remote_copy(
            src_ref=heads_s.at[a, h, of_core],
            dst_ref=recv_s.at[source, a * 64 : a * 64 + 64, :],
            send_sem=send.at[97 + a * 16 + h * 2 + of_core],
            recv_sem=recv.at[97 + a * 16 + source],
            device_id={"sp": 8 * core + h, "fs": y, "tp": of_core}, device_id_type=MESH,
        )

    def leaves(h, of_core):
        return jnp.logical_not(stays & (h == sp % 8) & (of_core == core))

    def deliver(a, total, low=0):
        count = total.shape[1] // HEAD_DIM
        turned = total.T.reshape(count, HEAD_DIM, BLOCK)
        if a != 1:
            factor = lax.rsqrt(jnp.mean(turned * turned, axis=1, keepdims=True) + EPS)
            gain_row = (kg_ref if a == 0 else qg_ref)[...]
            gain = jnp.broadcast_to(gain_row, (HEAD_DIM, HEAD_DIM)).T[:, 0:1]
            turned = turned * factor * gain[None]
        turned = turned.astype(jnp.bfloat16)
        heads_s[a, low : low + count, 0] = turned[:, :, :HALF]
        heads_s[a, low : low + count, 1] = turned[:, :, HALF:]

        def send_head(i, unused):
            h, of_core = low + (sp + i // 2) % count, i % 2

            @pl.when(leaves(h, of_core))
            def _():
                head_copy(a, h, of_core, sp).start()

            return unused

        lax.fori_loop(0, 2 * count, send_head, 0)

        @pl.when(stays & (sp % 8 >= low) & (sp % 8 < low + count))
        def _():
            recv_s[sp, a * 64 : a * 64 + 64, :] = heads_s[a, sp % 8, core]

    def wa_part(quarter, of_core, start, count):
        return wa_all.at[
            pl.ds(pl.multiple_of(of_core * 512 + start, 128), count),
            pl.ds(pl.multiple_of(quarter * 512, 512), 512),
        ]

    def wp_part(quarter, of_core, start, count):
        return wp_all.at[
            pl.ds(pl.multiple_of(of_core * 256 + start, 128), count),
            pl.ds(pl.multiple_of(quarter * 512, 512), 512),
        ]

    def share(quarter, index):
        go(wa_part(quarter, core, 0, 512), wa_part(quarter, core, 0, 512), index, partner)
        go(wp_part(quarter, core, 0, 256), wp_part(quarter, core, 0, 256), index + 1, partner)

    def shared(quarter, index):
        got(wa_part(quarter, 1 - core, 0, 512), index)
        got(wp_part(quarter, 1 - core, 0, 256), index + 1)

    def weights_start():
        go(wao_ref, wa_part(y, core, 0, 512), 147, to["yp"])
        go(wpo_ref, wp_part(y, core, 0, 256), 148, to["yp"])
        go(wao_ref, wa_part(y, core, 0, 512), 149, to["ym"])
        go(wpo_ref, wp_part(y, core, 0, 256), 150, to["ym"])
        go(wao_ref, wa_part(y, core, 0, 512), 155, partner)
        go(wpo_ref, wp_part(y, core, 0, 256), 156, partner)

    def weights_middle():
        got(wa_part(y_down, core, 0, 512), 147)
        got(wp_part(y_down, core, 0, 256), 148)
        go(wa_part(y_down, core, 0, 256), wa_part(y_down, core, 0, 256), 151, to["yp"])
        go(wp_part(y_down, core, 0, 128), wp_part(y_down, core, 0, 128), 152, to["yp"])
        got(wa_part(y_up, core, 0, 512), 149)
        got(wp_part(y_up, core, 0, 256), 150)
        go(wa_part(y_up, core, 256, 256), wa_part(y_up, core, 256, 256), 153, to["ym"])
        go(wp_part(y_up, core, 128, 128), wp_part(y_up, core, 128, 128), 154, to["ym"])
        share(y_down, 157)
        share(y_up, 159)

    def weights_late():
        got(wa_part(y_far, core, 0, 256), 151)
        got(wp_part(y_far, core, 0, 128), 152)
        got(wa_part(y_far, core, 256, 256), 153)
        got(wp_part(y_far, core, 128, 128), 154)
        share(y_far, 161)

    def weights_end():
        shared(y, 155)
        shared(y_down, 157)
        shared(y_up, 159)
        shared(y_far, 161)

    mine_at = pl.ds(pl.multiple_of(core * HALF, HALF), HALF)
    other_at = pl.ds(pl.multiple_of((1 - core) * HALF, HALF), HALF)

    def turned(block):
        return block.astype(jnp.float32).T.astype(jnp.bfloat16)

    def forward(a, r):
        return pltpu.make_async_remote_copy(
            src_ref=recv_s.at[r, a * 64 : a * 64 + 64, :],
            dst_ref=other_s.at[r, a * 64 : a * 64 + 64, :],
            send_sem=send.at[200 + a * 16 + r], recv_sem=recv.at[200 + a * 16 + r],
            device_id=partner, device_id_type=MESH,
        )

    def place(a, r, block, at):
        if a == 0:
            k_s[r, at, 0:64] = turned(block)
        elif a == 1:
            v_s[r, :, at] = block
        else:
            q_s[r, 0:64, :] = block

    def take(a):
        def pair(n, unused):
            places_now = [(sp + 2 * n) % BLOCKS, (sp + 2 * n + 1) % BLOCKS]
            for r in places_now:
                @pl.when(jnp.logical_not(stays & (r == sp)))
                def _():
                    head_copy(a, 0, 0, r).wait_recv()

                if a < 2:
                    forward(a, r).start()
            for r in places_now:
                place(a, r, recv_s[r, a * 64 : a * 64 + 64, :], mine_at)
            return unused

        lax.fori_loop(0, BLOCKS // 2, pair, 0)

    def take_other(a):
        def pair(n, unused):
            places_now = [(sp + 2 * n) % BLOCKS, (sp + 2 * n + 1) % BLOCKS]
            for r in places_now:
                forward(a, r).wait_recv()
            for r in places_now:
                place(a, r, other_s[r, a * 64 : a * 64 + 64, :], other_at)
            return unused

        lax.fori_loop(0, BLOCKS // 2, pair, 0)

    scale = LOG2E / math.sqrt(HEAD_DIM)
    half = core
    offset_m[...] = jnp.zeros_like(offset_m)
    offset_m[:, 0:8] = jnp.broadcast_to(offset_ref[...], (8, 8))
    gains_m[:, 0:256] = jnp.broadcast_to(pg_ref[...].reshape(1, 256), (16, 256))
    gains_m[:, 256:768] = jnp.broadcast_to(ag_ref[...].reshape(1, 512), (16, 512))
    tri_s[...] = jnp.where(
        lax.broadcasted_iota(jnp.int32, (HALF, HALF), 0)
        <= lax.broadcasted_iota(jnp.int32, (HALF, HALF), 1),
        1.0,
        0.0,
    ).astype(jnp.bfloat16)
    row = lax.broadcasted_iota(jnp.int32, (64, HALF), 0)
    ones = jnp.where(row < 3, 1.0, 0.0).astype(jnp.bfloat16)
    mask_s[...] = jnp.where(
        lax.broadcasted_iota(jnp.int32, (BLOCK, HALF), 0)
        < lax.broadcasted_iota(jnp.int32, (BLOCK, HALF), 1) + half * HALF,
        0.0,
        -1e30,
    )
    acc_s[...] = jnp.zeros_like(acc_s)
    carry_s[...] = jnp.zeros_like(carry_s)

    def fill_queries(r, unused):
        q_s[r, 64:128, :] = ones
        return unused

    lax.fori_loop(0, BLOCKS, fill_queries, 0)
    for load in loads:
        load.wait()
    pl.semaphore_wait(barrier, 7)
    def tell(stage, *targets):
        for target in targets:
            pl.semaphore_signal(
                known.at[stage], inc=1, device_id=target, device_id_type=MESH
            )

    direct(0)
    go(tok_ref, tok_s, 94, partner)
    tell(0, to["xp"], to["xm"])
    direct(1)
    go(offset_m, offset_s, 163, partner)
    go(gains_m, gains_o, 146, partner)
    got(tok_s, 94)

    mine_f = tok_ref[...].astype(jnp.float32)
    other_f = tok_s[...].astype(jnp.float32)
    squares = jnp.sum(mine_f * mine_f, axis=1, keepdims=True) + jnp.sum(
        other_f * other_f, axis=1, keepdims=True
    )
    factor = lax.rsqrt(squares / 2048.0 + EPS)
    for j in range(2):
        columns = slice(512 * j, 512 * j + 512)
        at_mine = 2 * core + j
        at_other = 2 * (1 - core) + j
        x_s[at_mine] = (
            tok_ref[:, columns].astype(jnp.float32) * factor * gain_ref[at_mine]
        ).astype(jnp.bfloat16)
        x_s[at_other] = (
            tok_s[:, columns].astype(jnp.float32) * factor * gain_ref[at_other]
        ).astype(jnp.bfloat16)

    pl.semaphore_wait(known.at[0], 2)
    tell(1, to["zp"], to["zm"])
    first(0)
    own(0)
    pl.semaphore_wait(known.at[1], 2)
    tell(2, to["zp"], to["zm"])
    own(1)
    first(1)
    pl.semaphore_wait(known.at[2], 2)
    tell(3, partner)
    direct(2)
    second(0)
    own(2)
    third(0)
    second(1)
    first(2)
    query_direct()
    acc_p[...] = jnp.dot(x_s[y], wp_ref[...], preferred_element_type=jnp.float32)
    fourth(0)
    third(1)
    settle(0)
    pl.semaphore_wait(known.at[3], 1)
    deliver(0, rest(0, 0, 256))
    deliver(0, rest(0, 256, 512), 4)
    fourth(1)
    second(2)
    settle(1)
    deliver(1, rest(1, 0, 256))
    deliver(1, rest(1, 256, 512), 4)
    third(2)
    query_relay()
    pool_direct()
    got(offset_s, 163)
    of_core = jnp.where(sp // 8 == core, offset_m[0:1, :], offset_s[0:1, :])
    chosen = lax.broadcasted_iota(jnp.int32, (1, 128), 1) == sp % 8
    offset = jnp.sum(jnp.where(chosen, of_core, 0.0), axis=1, keepdims=True) * math.sqrt(HEAD_DIM)
    column = lax.broadcasted_iota(jnp.int32, (BLOCK, 64), 1)
    terms = split_terms(jnp.broadcast_to(offset, (BLOCK, 64)))
    extra = jnp.where(
        column == 0,
        terms[0].astype(jnp.float32),
        jnp.where(
            column == 1,
            terms[1].astype(jnp.float32),
            jnp.where(column == 2, terms[2].astype(jnp.float32), 0.0),
        ),
    ).astype(jnp.bfloat16)


    def fill(r, unused):
        k_s[r, :, 64:128] = extra
        return unused

    lax.fori_loop(0, BLOCKS, fill, 0)
    mine_half = pl.ds(pl.multiple_of(core * HALF, HALF), HALF)
    other_half = pl.ds(pl.multiple_of((1 - core) * HALF, HALF), HALF)
    fourth(2)
    take(0)
    settle(2)
    deliver(2, rest(2, 0, 256))
    query_settle()
    deliver(2, rest(2, 256, 512), 4)
    take(1)
    take_other(0)
    pool_relay()
    take_other(1)
    weights_start()
    stores = [
        pltpu.make_async_copy(wao_ref, wa_part(y, core, 0, 512), local.at[5]),
        pltpu.make_async_copy(wpo_ref, wp_part(y, core, 0, 256), local.at[6]),
    ]
    for store in stores:
        store.start()

    def pool_tail():
        tail = pool_in.at[BLOCK - 16 : BLOCK, :]
        go(tail, before_s, 95, {"sp": (sp + 1) % BLOCKS, "fs": y, "tp": core})

    def pool_swap():
        go(pooled_s.at[other_at, :], pool_rows.at[core], 96, partner)

    def pool_project():
        pool_settle()
        total = acc_p[...]
        for q in quarters:
            total = total + jnp.dot(x_s[q], pbuf[q], preferred_element_type=jnp.float32)
        pool_in[...] = total.astype(jnp.bfloat16)
        pool_tail()

    def pool_windows():
        got(before_s, 95)
        current = pool_in[...].astype(jnp.float32)
        before = jnp.where(sp == 0, 0.0, before_s[...].astype(jnp.float32))

        def behind(values, count):
            return jnp.concatenate([jnp.zeros((count, values.shape[1]), jnp.float32), values[:-count]], axis=0)

        extended = jnp.concatenate([before, current], axis=0)
        sum_2 = extended + behind(extended, 1)
        sum_4 = sum_2 + behind(sum_2, 2)
        sum_8 = sum_4 + behind(sum_4, 4)
        sum_16 = sum_8 + behind(sum_8, 8)
        position = lax.broadcasted_iota(jnp.int32, (BLOCK, 128), 0) + (sp * BLOCK + 1)
        for group in range(2):
            columns = slice(128 * group, 128 * group + 128)
            low, high = ((sum_2, sum_8), (sum_4, sum_16))[group]
            window = jnp.where(core == 0, 2 << group, 8 << group)
            summed = jnp.where(core == 0, low[16:, columns], high[16:, columns])
            counted = jnp.minimum(position, window).astype(jnp.float32)
            centered = (summed / counted - current[:, columns]).astype(jnp.bfloat16)
            mixed = jnp.dot(centered, mix_ref[group], preferred_element_type=jnp.float32)
            pooled_s[:, columns] = (mixed * scale_ref[:, columns]).astype(jnp.bfloat16)
        pool_swap()
        pool_rows[core] = pooled_s[mine_at, :]

    pool_project()
    take(2)
    zs, ls, ws = (z0, z1, z2), (l0, l1, l2), (w0, w1, w2)

    first_row = jnp.where(sp == BLOCKS - 1, 1, sp + 1)

    def places(state):
        step, r, distance = state
        row_at = jnp.where((step < 0) | (step >= 136), BLOCKS, r)
        return (row_at, r, jnp.maximum(r - distance, 0))

    def advance(state):
        step, r, distance = state
        diagonal = step < BLOCKS - 1
        turn = step == BLOCKS - 1
        done = distance >= r
        next_row = jnp.where(r == BLOCKS - 1, 1, r + 1)
        r_after = jnp.where(
            diagonal,
            jnp.maximum(step + 1, 0),
            jnp.where(turn, first_row, jnp.where(done, next_row, r)),
        )
        after = jnp.where(diagonal, 0, jnp.where(turn | done, 1, distance + 1))
        return (step + 1, r_after, after)

    def scores(state, b, masked):
        unused_row, r, g = places(state)
        z = jnp.dot(k_s[g], q_s[r], preferred_element_type=jnp.float32) * scale
        if masked:
            z = z + mask_s[...]
        zs[b][...] = z

    def soften(b):
        ls[b][...] = jnp.log2(1.0 + jnp.exp2(zs[b][...])).astype(jnp.bfloat16)

    def weigh(state, b):
        row_at = places(state)[0]
        late = jnp.dot(tri_s[...], ls[b][HALF:, :], preferred_element_type=jnp.float32)
        early = jnp.dot(tri_s[...], ls[b][:HALF, :], preferred_element_type=jnp.float32)
        carry = carry_s[row_at][0:1]
        before = carry + late[0:1]
        ws[b][HALF:, :] = jnp.exp2(zs[b][HALF:, :] - (late + carry)).astype(jnp.bfloat16)
        ws[b][:HALF, :] = jnp.exp2(zs[b][:HALF, :] - (early + before)).astype(jnp.bfloat16)
        carry_s[row_at] = jnp.broadcast_to(before + early[0:1], (8, HALF))

    def gather_values(state, b):
        row_at, unused_row, g = places(state)
        acc_s[row_at] = acc_s[row_at] + jnp.dot(
            v_s[g], ws[b][...], preferred_element_type=jnp.float32
        )

    def return_row(state):
        step, r, distance = state

        @pl.when((distance == r) & (step >= 0) & (step < 136))
        def _():
            done_s[r] = acc_s[r].astype(jnp.bfloat16)

            @pl.when(r != sp)
            def _():
                pltpu.make_async_remote_copy(
                    src_ref=done_s.at[r], dst_ref=o_ref.at[sp], send_sem=send.at[180 + r],
                    recv_sem=recv.at[180 + sp], device_id={"sp": r, "fs": y, "tp": core}, device_id_type=MESH,
                ).start()

    hooks = ((1, pool_windows), (6, weights_middle), (11, weights_late))

    def steps(masked):
        def body(n, states):
            if not masked:
                for turn, hook in hooks:
                    pl.when(n == turn)(hook)
            states = list(states)
            for unused_step in range(9):
                states.append(advance(states[-1]))
            for u in range(9):
                gather_values(states[u], (u + 2) % 3)
                weigh(states[u + 1], u % 3)
                soften((u + 1) % 3)
                scores(states[u + 3], (u + 2) % 3, masked)
            finished = functools.reduce(
                jnp.logical_or, [distance == r for unused_step, r, distance in states[:9]]
            )

            @pl.when(finished)
            def _():
                for u in range(9):
                    return_row(states[u])

            return tuple(states[9:])

        return body

    first_states = tuple(
        (jnp.int32(step), jnp.int32(0), jnp.int32(0)) for step in (-5, -4, -3, -2)
    )
    states = lax.fori_loop(0, 2, steps(True), first_states)
    mode[0] = "hook"
    lax.fori_loop(0, 14, steps(False), states)
    mode[0] = "start"
    for store in stores:
        store.wait()
    o_ref[sp] = done_s[sp]
    weights_end()
    got(gains_o, 146)
    got(pool_rows.at[1 - core], 96)

    def gain_rows(columns):
        mine_gain = gains_m[0:1, columns].astype(jnp.float32)
        other_gain = gains_o[0:1, columns].astype(jnp.float32)
        low = jnp.where(core == 0, mine_gain, other_gain)
        high = jnp.where(core == 0, other_gain, mine_gain)
        return jnp.concatenate([low, high], axis=1)

    pooled = jnp.concatenate([pool_rows[0], pool_rows[1]], axis=1).astype(jnp.float32)
    factor = lax.rsqrt(jnp.mean(pooled * pooled, axis=1, keepdims=True) + EPS)
    pool_normed = (pooled * factor * gain_rows(slice(0, 256))).astype(jnp.bfloat16)
    for j in range(4):
        acc[j // 2, 256 * (j % 2) : 256 * (j % 2) + 256, :] = jnp.dot(
            pool_normed, wp_all[:, 512 * j : 512 * j + 512], preferred_element_type=jnp.float32
        )

    def settle_row(i, unused):
        r = (sp + i) % BLOCKS
        copy = pltpu.make_async_remote_copy(
            src_ref=done_s.at[r], dst_ref=o_ref.at[r], send_sem=send.at[180 + r],
            recv_sem=recv.at[180 + r], device_id={"sp": r, "fs": y, "tp": core},
            device_id_type=MESH,
        )
        copy.wait_send()
        copy.wait_recv()
        return unused

    lax.fori_loop(1, BLOCKS, settle_row, 0)

    attended = o_ref[...].reshape(HEADS * HEAD_DIM, HALF).astype(jnp.float32).T
    factor = lax.rsqrt(jnp.mean(attended * attended, axis=1, keepdims=True) + EPS)
    attn_normed = (attended * factor * gain_rows(slice(256, 768))).astype(jnp.bfloat16)
    for j in range(4):
        columns = slice(512 * j, 512 * j + 512)
        side = (left_ref, right_ref)[j // 2]
        side[:, 512 * (j % 2) : 512 * (j % 2) + 512] = (
            acc[j // 2, 256 * (j % 2) : 256 * (j % 2) + 256, :]
            + jnp.dot(attn_normed, wa_all[:, columns], preferred_element_type=jnp.float32)
        ).astype(jnp.bfloat16)

    for copy in started:
        copy.wait_send()
    mode[0] = "wait"
    for resend in (pool_swap, weights_middle, weights_late):
        resend()

    def settle_heads(i, unused):
        for a in range(3):
            @pl.when(leaves(i // 2, i % 2))
            def _():
                head_copy(a, i // 2, i % 2, sp).wait_send()

        for a in range(2):
            forward(a, i).wait_send()
        return unused

    lax.fori_loop(0, BLOCKS, settle_heads, 0)


def mixer(*operands):
    vmem = pl.BlockSpec(memory_space=pltpu.VMEM)
    here = pl.BlockSpec(memory_space=pl.ANY)
    return pl.pallas_call(
        mixer_kernel,
        out_shape=(jax.ShapeDtypeStruct((HALF, 1024), jnp.bfloat16),) * 2,
        in_specs=[here, vmem, here, here, here, here, *[vmem] * 5, here, here, vmem, vmem],
        out_specs=(vmem, vmem),
        scratch_shapes=[
            pltpu.VMEM((512, 1024), jnp.bfloat16),
            *[pltpu.VMEM((512, 512), jnp.bfloat16)] * 3,
            pltpu.VMEM((512, 256), jnp.bfloat16),
            pltpu.VMEM((3, 4, 512, 512), jnp.bfloat16),
            pltpu.VMEM((4, 512, 256), jnp.bfloat16),
            pltpu.VMEM((512, 1024), jnp.bfloat16),
            pltpu.VMEM((4, 512, 512), jnp.bfloat16),
            pltpu.VMEM((3, 512, 512), jnp.float32),
            pltpu.VMEM((512, 256), jnp.float32),
            pltpu.VMEM((3, 8, 2, HEAD_DIM, HALF), jnp.bfloat16),
            pltpu.VMEM((512, 256), jnp.bfloat16),
            pltpu.VMEM((16, 256), jnp.bfloat16),
            pltpu.VMEM((512, 256), jnp.bfloat16),
            pltpu.VMEM((2, HALF, 256), jnp.bfloat16),
            pltpu.VMEM((BLOCKS, 3 * HEAD_DIM, HALF), jnp.bfloat16),
            pltpu.VMEM((BLOCKS, 2 * HEAD_DIM, HALF), jnp.bfloat16),
            pltpu.VMEM((BLOCKS, HEAD_DIM, HALF), jnp.bfloat16),
            pltpu.VMEM((512, 2048), jnp.bfloat16),
            pltpu.VMEM((1024, 2048), jnp.bfloat16),
            pltpu.VMEM((16, 768), jnp.bfloat16),
            pltpu.VMEM((16, 768), jnp.bfloat16),
            pltpu.VMEM((8, 128), jnp.float32),
            pltpu.VMEM((8, 128), jnp.float32),
            pltpu.VMEM((BLOCKS, 128, HALF), jnp.bfloat16),
            pltpu.VMEM((BLOCKS, BLOCK, 128), jnp.bfloat16),
            pltpu.VMEM((BLOCKS, HEAD_DIM, BLOCK), jnp.bfloat16),
            pltpu.VMEM((HALF, HALF), jnp.bfloat16),
            pltpu.VMEM((BLOCK, HALF), jnp.float32),
            pltpu.VMEM((BLOCKS + 1, HEAD_DIM, HALF), jnp.float32),
            pltpu.VMEM((BLOCKS + 1, 8, HALF), jnp.float32),
            pltpu.VMEM((BLOCKS, HEAD_DIM, HALF), jnp.bfloat16),
            *[pltpu.VMEM((BLOCK, HALF), jnp.float32)] * 3,
            *[pltpu.VMEM((BLOCK, HALF), jnp.bfloat16)] * 6,
            pltpu.SemaphoreType.DMA((236,)),
            pltpu.SemaphoreType.DMA((236,)),
            pltpu.SemaphoreType.DMA((7,)),
            pltpu.SemaphoreType.REGULAR((4,)),
        ],
        compiler_params=pltpu.CompilerParams(
            collective_id=0, has_side_effects=True, vmem_limit_bytes=62 * 1024 * 1024,
        ),
        cost_estimate=pl.CostEstimate(
            flops=45_000_000_000, bytes_accessed=8_000_000, transcendentals=50_000_000
        ),
        name="token_mixer",
    )(*operands)


def join_kernel(left_ref, right_ref, joined_ref):
    joined_ref[:, :1024] = left_ref[...]
    joined_ref[:, 1024:] = right_ref[...]


def join(left, right):
    side = pl.BlockSpec((HALF, 1024), lambda i: (i, 0))
    return pl.pallas_call(
        join_kernel,
        grid=(1,),
        out_shape=jax.ShapeDtypeStruct((HALF, 2048), jnp.bfloat16),
        in_specs=[side, side],
        out_specs=pl.BlockSpec((HALF, 2048), lambda i: (i, 0)),
        name="join_sides",
    )(left, right)


def shards(
    tokens,
    norm_gain,
    w_pool_in,
    w_query,
    w_key,
    w_value,
    query_gain,
    key_gain,
    stick_offset,
    pool_mix,
    pool_scale,
    pool_gain,
    attn_gain,
    w_out_pool,
    w_out_attn,
):
    left, right = mixer(
        tokens[0], norm_gain.reshape(4, 1, 512), w_key, w_value, w_query, w_pool_in,
        key_gain.reshape(1, HEAD_DIM), query_gain.reshape(1, HEAD_DIM), pool_mix,
        pool_scale.reshape(1, 256), stick_offset.reshape(1, 8), w_out_pool, w_out_attn,
        pool_gain, attn_gain,
    )
    return join(left, right)[None]


def solution(mesh):
    in_specs = (
        P("fs", "sp", "tp"),
        P(),
        P("fs", "tp"),
        P("fs", "tp"),
        P("fs", "tp"),
        P("fs", "tp"),
        P(),
        P(),
        P("tp"),
        P("tp", None, None),
        P("tp"),
        P("tp"),
        P("tp"),
        P("tp", "fs"),
        P("tp", "fs"),
    )
    out_specs = P("fs", ("sp", "tp"), None)
    return jax.shard_map(shards, mesh=mesh, in_specs=in_specs, out_specs=out_specs, check_vma=False)
```

```python
import functools
import math

import jax
import jax.numpy as jnp
from jax import lax
from jax.experimental import pallas as pl
from jax.experimental.pallas import tpu as pltpu
from jax.sharding import PartitionSpec as P

HEADS = 16
HEAD_DIM = 64
POOL = 512
POOL_GROUPS = 4
BLOCKS = 16
HALF = 256
BLOCK = 512

EPS = 1e-06
LOG2E = 1.4426950408889634


def split_terms(value):
    high = value.astype(jnp.bfloat16)
    rest = value - high.astype(jnp.float32)
    middle = rest.astype(jnp.bfloat16)
    low = (rest - middle.astype(jnp.float32)).astype(jnp.bfloat16)
    return (high, middle, low)


MESH = pl.DeviceIdType.MESH


def mixer_kernel(
    tok_hbm, gain_ref, wk_hbm, wv_hbm, wq_hbm, wp_hbm, kg_ref, qg_ref, mix_ref, scale_ref,
    offset_ref, wpo_ref, wao_ref, pg_ref, ag_ref,
    left_ref, right_ref,
    tok_ref, wk_ref, wv_ref, wq_ref, wp_ref,
    buf, pbuf, tok_s, x_s, acc, acc_p, heads_s, pool_in, before_s, pooled_s, pool_rows,
    recv_s, other_s, o_ref, wp_all, wa_all, gains_m, gains_o, offset_m, offset_s,
    q_s, k_s, v_s, tri_s, mask_s, acc_s, carry_s, done_s,
    z0, z1, z2, l0, l1, l2, w0, w1, w2, send, recv, local, known,
):
    sp, y, core = lax.axis_index("sp"), lax.axis_index("fs"), lax.axis_index("tp")
    z, x = sp // 4, sp % 4
    y_up, y_down, y_far = (y + 1) % 4, (y + 3) % 4, (y + 2) % 4
    x_up, x_down, x_far = (x + 1) % 4, (x + 3) % 4, (x + 2) % 4
    z_up, z_down, z_far = (z + 1) % 4, (z + 3) % 4, (z + 2) % 4

    def at(z_to, x_to, y_to, core_to):
        return {"sp": z_to * 4 + x_to, "fs": y_to, "tp": core_to}

    partner = at(z, x, y, 1 - core)
    to = {
        "yp": at(z, x, y_up, core), "ym": at(z, x, y_down, core),
        "xp": at(z, x_up, y, core), "xm": at(z, x_down, y, core),
        "zp": at(z_up, x, y, core), "zm": at(z_down, x, y, core),
    }

    barrier = pltpu.get_barrier_semaphore()
    for target in (partner, *to.values()):
        pl.semaphore_signal(barrier, inc=1, device_id=target, device_id_type=MESH)
    loads = [
        pltpu.make_async_copy(source, target, local.at[i])
        for i, (source, target) in enumerate(
            (
                (tok_hbm, tok_ref), (wk_hbm, wk_ref), (wv_hbm, wv_ref), (wq_hbm, wq_ref),
                (wp_hbm, wp_ref),
            )
        )
    ]
    for load in loads:
        load.start()

    started = []

    def remote(source, target_ref, index, target):
        return pltpu.make_async_remote_copy(
            src_ref=source, dst_ref=target_ref, send_sem=send.at[index],
            recv_sem=recv.at[index], device_id=target, device_id_type=MESH,
        )

    mode = ["start"]

    def go(source, target_ref, index, target):
        copy = remote(source, target_ref, index, target)
        if mode[0] == "wait":
            copy.wait_send()
            return
        copy.start()
        if mode[0] == "start":
            started.append(copy)

    def got(target_ref, index):
        if mode[0] != "wait":
            remote(target_ref, target_ref, index, partner).wait_recv()

    def rows(start, count=64):
        return pl.ds(pl.multiple_of(start, 32), count)

    weights = (wk_ref, wv_ref, wq_ref)
    quarters = (y_down, y_up, y_far)

    widths = (512, 512, 256)

    def part(a, quarter, start, count=64):
        return buf.at[a, quarter, rows(start, count), 0 : widths[a]]

    def direct(a):
        base = a * 30
        own_x, own_z = 64 * x, 256 + 64 * z
        w = weights[a]
        go(w.at[rows(own_x), 0 : widths[a]], part(a, y, own_x), base + 0, to["yp"])
        go(w.at[rows(own_z), 0 : widths[a]], part(a, y, own_z), base + 1, to["ym"])
        go(w.at[rows(own_x), 0 : widths[a]], part(a, y, own_x), base + 2, to["ym"])
        go(w.at[rows(own_z), 0 : widths[a]], part(a, y, own_z), base + 3, to["yp"])

    def ring_base(a, item, ring):
        return a * 30 + 6 + item * 8 + ring * 4

    own_row = (64 * x, 256 + 64 * z)
    down_row = (64 * x_down, 256 + 64 * z_down)
    up_row = (64 * x_up, 256 + 64 * z_up)
    far_row = (64 * x_far, 256 + 64 * z_far)
    ups = ("xp", "zp")
    downs = ("xm", "zm")

    def spread(a, item, ring):
        base = ring_base(a, item, ring)
        piece = part(a, quarters[item], own_row[ring])
        go(piece, piece, base + 0, to[ups[ring]])
        go(piece, piece, base + 1, to[downs[ring]])

    def relay(a, item, ring):
        base = ring_base(a, item, ring)
        q = quarters[item]
        got(part(a, q, down_row[ring]), base + 0)
        piece = part(a, q, down_row[ring], 32)
        go(piece, piece, base + 2, to[ups[ring]])
        got(part(a, q, up_row[ring]), base + 1)
        piece = part(a, q, up_row[ring] + 32, 32)
        go(piece, piece, base + 3, to[downs[ring]])

    def settle(a):
        for item in range(3):
            for ring in range(2):
                base = ring_base(a, item, ring)
                q = quarters[item]
                got(part(a, q, far_row[ring], 32), base + 2)
                got(part(a, q, far_row[ring] + 32, 32), base + 3)

    def first(a):
        base = a * 30
        piece = part(a, y_down, own_row[0])
        got(piece, base + 0)
        go(piece, piece, base + 4, to["yp"])
        spread(a, 0, 0)
        piece = part(a, y_up, own_row[1])
        got(piece, base + 1)
        go(piece, piece, base + 5, to["ym"])
        spread(a, 1, 1)
        got(part(a, y_up, own_row[0]), base + 2)
        spread(a, 1, 0)
        got(part(a, y_down, own_row[1]), base + 3)
        spread(a, 0, 1)

    def second(a):
        relay(a, 0, 0)
        relay(a, 1, 1)

    def third(a):
        base = a * 30
        got(part(a, y_far, own_row[0]), base + 4)
        spread(a, 2, 0)
        got(part(a, y_far, own_row[1]), base + 5)
        spread(a, 2, 1)
        relay(a, 1, 0)
        relay(a, 0, 1)

    def fourth(a):
        relay(a, 2, 0)
        relay(a, 2, 1)

    def query_part(quarter, start, count):
        return buf.at[2, quarter, start : start + count, 256:512]

    def query_direct():
        go(wq_ref.at[:, 256:512], query_part(y, 0, 512), 232, to["yp"])
        go(wq_ref.at[:, 256:512], query_part(y, 0, 512), 233, to["ym"])

    def query_relay():
        got(query_part(y_down, 0, 512), 232)
        go(query_part(y_down, 0, 256), query_part(y_down, 0, 256), 234, to["yp"])
        got(query_part(y_up, 0, 512), 233)
        go(query_part(y_up, 256, 256), query_part(y_up, 256, 256), 235, to["ym"])

    def query_settle():
        got(query_part(y_far, 0, 256), 234)
        got(query_part(y_far, 256, 256), 235)

    pool_base = 90

    def pool_direct():
        go(wp_ref, pbuf.at[y], pool_base + 0, to["yp"])
        go(wp_ref, pbuf.at[y], pool_base + 1, to["ym"])

    def pool_relay():
        got(pbuf.at[y_down], pool_base + 0)
        piece = pbuf.at[y_down, 0:256, :]
        go(piece, piece, pool_base + 2, to["yp"])
        got(pbuf.at[y_up], pool_base + 1)
        piece = pbuf.at[y_up, 256:512, :]
        go(piece, piece, pool_base + 3, to["ym"])

    def pool_settle():
        got(pbuf.at[y_far, 0:256, :], pool_base + 2)
        got(pbuf.at[y_far, 256:512, :], pool_base + 3)

    def own(a):
        acc[a] = jnp.dot(x_s[y], weights[a][...], preferred_element_type=jnp.float32)

    def rest(a, low=0, high=512):
        total = acc[a][:, low:high]
        for q in quarters:
            total = total + jnp.dot(
                x_s[q], buf[a, q, :, low:high], preferred_element_type=jnp.float32
            )
        return total

    stays = sp // 8 == core

    def head_copy(a, h, of_core, source):
        return pltpu.make_async_remote_copy(
            src_ref=heads_s.at[a, h, of_core],
            dst_ref=recv_s.at[source, a * 64 : a * 64 + 64, :],
            send_sem=send.at[97 + a * 16 + h * 2 + of_core],
            recv_sem=recv.at[97 + a * 16 + source],
            device_id={"sp": 8 * core + h, "fs": y, "tp": of_core}, device_id_type=MESH,
        )

    def leaves(h, of_core):
        return jnp.logical_not(stays & (h == sp % 8) & (of_core == core))

    def deliver(a, total, low=0):
        count = total.shape[1] // HEAD_DIM
        turned = total.T.reshape(count, HEAD_DIM, BLOCK)
        if a != 1:
            factor = lax.rsqrt(jnp.mean(turned * turned, axis=1, keepdims=True) + EPS)
            gain_row = (kg_ref if a == 0 else qg_ref)[...]
            gain = jnp.broadcast_to(gain_row, (HEAD_DIM, HEAD_DIM)).T[:, 0:1]
            turned = turned * factor * gain[None]
        turned = turned.astype(jnp.bfloat16)
        heads_s[a, low : low + count, 0] = turned[:, :, :HALF]
        heads_s[a, low : low + count, 1] = turned[:, :, HALF:]

        def send_head(i, unused):
            h, of_core = low + (sp + i // 2 + 2 * core) % count, i % 2

            @pl.when(leaves(h, of_core))
            def _():
                head_copy(a, h, of_core, sp).start()

            return unused

        lax.fori_loop(0, 2 * count, send_head, 0)

        @pl.when(stays & (sp % 8 >= low) & (sp % 8 < low + count))
        def _():
            recv_s[sp, a * 64 : a * 64 + 64, :] = heads_s[a, sp % 8, core]

    def wa_part(quarter, of_core, start, count):
        return wa_all.at[
            pl.ds(pl.multiple_of(of_core * 512 + start, 128), count),
            pl.ds(pl.multiple_of(quarter * 512, 512), 512),
        ]

    def wp_part(quarter, of_core, start, count):
        return wp_all.at[
            pl.ds(pl.multiple_of(of_core * 256 + start, 128), count),
            pl.ds(pl.multiple_of(quarter * 512, 512), 512),
        ]

    def share(quarter, index):
        go(wa_part(quarter, core, 0, 512), wa_part(quarter, core, 0, 512), index, partner)
        go(wp_part(quarter, core, 0, 256), wp_part(quarter, core, 0, 256), index + 1, partner)

    def shared(quarter, index):
        got(wa_part(quarter, 1 - core, 0, 512), index)
        got(wp_part(quarter, 1 - core, 0, 256), index + 1)

    def weights_start():
        go(wao_ref, wa_part(y, core, 0, 512), 147, to["yp"])
        go(wpo_ref, wp_part(y, core, 0, 256), 148, to["yp"])
        go(wao_ref, wa_part(y, core, 0, 512), 149, to["ym"])
        go(wpo_ref, wp_part(y, core, 0, 256), 150, to["ym"])
        go(wao_ref, wa_part(y, core, 0, 512), 155, partner)
        go(wpo_ref, wp_part(y, core, 0, 256), 156, partner)

    def weights_middle():
        got(wa_part(y_down, core, 0, 512), 147)
        got(wp_part(y_down, core, 0, 256), 148)
        go(wa_part(y_down, core, 0, 256), wa_part(y_down, core, 0, 256), 151, to["yp"])
        go(wp_part(y_down, core, 0, 128), wp_part(y_down, core, 0, 128), 152, to["yp"])
        got(wa_part(y_up, core, 0, 512), 149)
        got(wp_part(y_up, core, 0, 256), 150)
        go(wa_part(y_up, core, 256, 256), wa_part(y_up, core, 256, 256), 153, to["ym"])
        go(wp_part(y_up, core, 128, 128), wp_part(y_up, core, 128, 128), 154, to["ym"])
        share(y_down, 157)
        share(y_up, 159)

    def weights_late():
        got(wa_part(y_far, core, 0, 256), 151)
        got(wp_part(y_far, core, 0, 128), 152)
        got(wa_part(y_far, core, 256, 256), 153)
        got(wp_part(y_far, core, 128, 128), 154)
        share(y_far, 161)

    def weights_end():
        shared(y, 155)
        shared(y_down, 157)
        shared(y_up, 159)
        shared(y_far, 161)

    mine_at = pl.ds(pl.multiple_of(core * HALF, HALF), HALF)
    other_at = pl.ds(pl.multiple_of((1 - core) * HALF, HALF), HALF)

    def turned(block):
        return block.astype(jnp.float32).T.astype(jnp.bfloat16)

    def forward(a, r):
        return pltpu.make_async_remote_copy(
            src_ref=recv_s.at[r, a * 64 : a * 64 + 64, :],
            dst_ref=other_s.at[r, a * 64 : a * 64 + 64, :],
            send_sem=send.at[200 + a * 16 + r], recv_sem=recv.at[200 + a * 16 + r],
            device_id=partner, device_id_type=MESH,
        )

    def place(a, r, block, at):
        if a == 0:
            k_s[r, at, 0:64] = turned(block)
        elif a == 1:
            v_s[r, :, at] = block
        else:
            q_s[r, 0:64, :] = block

    def take(a):
        def pair(n, unused):
            places_now = [(sp + 2 * n) % BLOCKS, (sp + 2 * n + 1) % BLOCKS]
            for r in places_now:
                @pl.when(jnp.logical_not(stays & (r == sp)))
                def _():
                    head_copy(a, 0, 0, r).wait_recv()

                if a < 2:
                    forward(a, r).start()
            for r in places_now:
                place(a, r, recv_s[r, a * 64 : a * 64 + 64, :], mine_at)
            return unused

        lax.fori_loop(0, BLOCKS // 2, pair, 0)

    def take_other(a):
        def pair(n, unused):
            places_now = [(sp + 2 * n) % BLOCKS, (sp + 2 * n + 1) % BLOCKS]
            for r in places_now:
                forward(a, r).wait_recv()
            for r in places_now:
                place(a, r, other_s[r, a * 64 : a * 64 + 64, :], other_at)
            return unused

        lax.fori_loop(0, BLOCKS // 2, pair, 0)

    scale = LOG2E / math.sqrt(HEAD_DIM)
    half = core
    offset_m[...] = jnp.zeros_like(offset_m)
    offset_m[:, 0:8] = jnp.broadcast_to(offset_ref[...], (8, 8))
    gains_m[:, 0:256] = jnp.broadcast_to(pg_ref[...].reshape(1, 256), (16, 256))
    gains_m[:, 256:768] = jnp.broadcast_to(ag_ref[...].reshape(1, 512), (16, 512))
    tri_s[...] = jnp.where(
        lax.broadcasted_iota(jnp.int32, (HALF, HALF), 0)
        <= lax.broadcasted_iota(jnp.int32, (HALF, HALF), 1),
        1.0,
        0.0,
    ).astype(jnp.bfloat16)
    row = lax.broadcasted_iota(jnp.int32, (64, HALF), 0)
    ones = jnp.where(row < 3, 1.0, 0.0).astype(jnp.bfloat16)
    mask_s[...] = jnp.where(
        lax.broadcasted_iota(jnp.int32, (BLOCK, HALF), 0)
        < lax.broadcasted_iota(jnp.int32, (BLOCK, HALF), 1) + half * HALF,
        0.0,
        -1e30,
    )
    acc_s[...] = jnp.zeros_like(acc_s)
    carry_s[...] = jnp.zeros_like(carry_s)

    def fill_queries(r, unused):
        q_s[r, 64:128, :] = ones
        return unused

    lax.fori_loop(0, BLOCKS, fill_queries, 0)
    for load in loads:
        load.wait()
    pl.semaphore_wait(barrier, 7)
    def tell(stage, *targets):
        for target in targets:
            pl.semaphore_signal(
                known.at[stage], inc=1, device_id=target, device_id_type=MESH
            )

    direct(0)
    go(tok_ref, tok_s, 94, partner)
    tell(0, to["xp"], to["xm"])
    direct(1)
    go(offset_m, offset_s, 163, partner)
    go(gains_m, gains_o, 146, partner)
    got(tok_s, 94)

    mine_f = tok_ref[...].astype(jnp.float32)
    other_f = tok_s[...].astype(jnp.float32)
    squares = jnp.sum(mine_f * mine_f, axis=1, keepdims=True) + jnp.sum(
        other_f * other_f, axis=1, keepdims=True
    )
    factor = lax.rsqrt(squares / 2048.0 + EPS)
    for j in range(2):
        columns = slice(512 * j, 512 * j + 512)
        at_mine = 2 * core + j
        at_other = 2 * (1 - core) + j
        x_s[at_mine] = (
            tok_ref[:, columns].astype(jnp.float32) * factor * gain_ref[at_mine]
        ).astype(jnp.bfloat16)
        x_s[at_other] = (
            tok_s[:, columns].astype(jnp.float32) * factor * gain_ref[at_other]
        ).astype(jnp.bfloat16)

    pl.semaphore_wait(known.at[0], 2)
    tell(1, to["zp"], to["zm"])
    first(0)
    own(0)
    pl.semaphore_wait(known.at[1], 2)
    tell(2, to["zp"], to["zm"])
    own(1)
    first(1)
    pl.semaphore_wait(known.at[2], 2)
    tell(3, partner)
    direct(2)
    second(0)
    own(2)
    third(0)
    second(1)
    first(2)
    query_direct()
    acc_p[...] = jnp.dot(x_s[y], wp_ref[...], preferred_element_type=jnp.float32)
    fourth(0)
    third(1)
    settle(0)
    pl.semaphore_wait(known.at[3], 1)
    deliver(0, rest(0, 0, 256))
    deliver(0, rest(0, 256, 512), 4)
    fourth(1)
    second(2)
    settle(1)
    deliver(1, rest(1, 0, 256))
    deliver(1, rest(1, 256, 512), 4)
    third(2)
    query_relay()
    pool_direct()
    got(offset_s, 163)
    of_core = jnp.where(sp // 8 == core, offset_m[0:1, :], offset_s[0:1, :])
    chosen = lax.broadcasted_iota(jnp.int32, (1, 128), 1) == sp % 8
    offset = jnp.sum(jnp.where(chosen, of_core, 0.0), axis=1, keepdims=True) * math.sqrt(HEAD_DIM)
    column = lax.broadcasted_iota(jnp.int32, (BLOCK, 64), 1)
    terms = split_terms(jnp.broadcast_to(offset, (BLOCK, 64)))
    extra = jnp.where(
        column == 0,
        terms[0].astype(jnp.float32),
        jnp.where(
            column == 1,
            terms[1].astype(jnp.float32),
            jnp.where(column == 2, terms[2].astype(jnp.float32), 0.0),
        ),
    ).astype(jnp.bfloat16)


    def fill(r, unused):
        k_s[r, :, 64:128] = extra
        return unused

    lax.fori_loop(0, BLOCKS, fill, 0)
    mine_half = pl.ds(pl.multiple_of(core * HALF, HALF), HALF)
    other_half = pl.ds(pl.multiple_of((1 - core) * HALF, HALF), HALF)
    fourth(2)
    take(0)
    settle(2)
    deliver(2, rest(2, 0, 256))
    query_settle()
    deliver(2, rest(2, 256, 512), 4)
    take(1)
    take_other(0)
    pool_relay()
    take_other(1)
    weights_start()
    stores = [
        pltpu.make_async_copy(wao_ref, wa_part(y, core, 0, 512), local.at[5]),
        pltpu.make_async_copy(wpo_ref, wp_part(y, core, 0, 256), local.at[6]),
    ]
    for store in stores:
        store.start()

    def pool_tail():
        tail = pool_in.at[BLOCK - 16 : BLOCK, :]
        go(tail, before_s, 95, {"sp": (sp + 1) % BLOCKS, "fs": y, "tp": core})

    def pool_swap():
        go(pooled_s.at[other_at, :], pool_rows.at[core], 96, partner)

    def pool_project():
        pool_settle()
        total = acc_p[...]
        for q in quarters:
            total = total + jnp.dot(x_s[q], pbuf[q], preferred_element_type=jnp.float32)
        pool_in[...] = total.astype(jnp.bfloat16)
        pool_tail()

    def pool_windows():
        got(before_s, 95)
        current = pool_in[...].astype(jnp.float32)
        before = jnp.where(sp == 0, 0.0, before_s[...].astype(jnp.float32))

        def behind(values, count):
            return jnp.concatenate([jnp.zeros((count, values.shape[1]), jnp.float32), values[:-count]], axis=0)

        extended = jnp.concatenate([before, current], axis=0)
        sum_2 = extended + behind(extended, 1)
        sum_4 = sum_2 + behind(sum_2, 2)
        sum_8 = sum_4 + behind(sum_4, 4)
        sum_16 = sum_8 + behind(sum_8, 8)
        position = lax.broadcasted_iota(jnp.int32, (BLOCK, 128), 0) + (sp * BLOCK + 1)
        for group in range(2):
            columns = slice(128 * group, 128 * group + 128)
            low, high = ((sum_2, sum_8), (sum_4, sum_16))[group]
            window = jnp.where(core == 0, 2 << group, 8 << group)
            summed = jnp.where(core == 0, low[16:, columns], high[16:, columns])
            counted = jnp.minimum(position, window).astype(jnp.float32)
            centered = (summed / counted - current[:, columns]).astype(jnp.bfloat16)
            mixed = jnp.dot(centered, mix_ref[group], preferred_element_type=jnp.float32)
            pooled_s[:, columns] = (mixed * scale_ref[:, columns]).astype(jnp.bfloat16)
        pool_swap()
        pool_rows[core] = pooled_s[mine_at, :]

    pool_project()
    take(2)
    zs, ls, ws = (z0, z1, z2), (l0, l1, l2), (w0, w1, w2)

    first_row = jnp.where(sp == BLOCKS - 1, 1, sp + 1)

    def places(state):
        step, r, distance = state
        row_at = jnp.where((step < 0) | (step >= 136), BLOCKS, r)
        return (row_at, r, jnp.maximum(r - distance, 0))

    def advance(state):
        step, r, distance = state
        diagonal = step < BLOCKS - 1
        turn = step == BLOCKS - 1
        done = distance >= r
        next_row = jnp.where(r == BLOCKS - 1, 1, r + 1)
        r_after = jnp.where(
            diagonal,
            jnp.maximum(step + 1, 0),
            jnp.where(turn, first_row, jnp.where(done, next_row, r)),
        )
        after = jnp.where(diagonal, 0, jnp.where(turn | done, 1, distance + 1))
        return (step + 1, r_after, after)

    def scores(state, b, masked):
        unused_row, r, g = places(state)
        z = jnp.dot(k_s[g], q_s[r], preferred_element_type=jnp.float32) * scale
        if masked:
            z = z + mask_s[...]
        zs[b][...] = z

    def soften(b):
        ls[b][...] = jnp.log2(1.0 + jnp.exp2(zs[b][...])).astype(jnp.bfloat16)

    def weigh(state, b):
        row_at = places(state)[0]
        late = jnp.dot(tri_s[...], ls[b][HALF:, :], preferred_element_type=jnp.float32)
        early = jnp.dot(tri_s[...], ls[b][:HALF, :], preferred_element_type=jnp.float32)
        carry = carry_s[row_at][0:1]
        before = carry + late[0:1]
        ws[b][HALF:, :] = jnp.exp2(zs[b][HALF:, :] - (late + carry)).astype(jnp.bfloat16)
        ws[b][:HALF, :] = jnp.exp2(zs[b][:HALF, :] - (early + before)).astype(jnp.bfloat16)
        carry_s[row_at] = jnp.broadcast_to(before + early[0:1], (8, HALF))

    def gather_values(state, b):
        row_at, unused_row, g = places(state)
        acc_s[row_at] = acc_s[row_at] + jnp.dot(
            v_s[g], ws[b][...], preferred_element_type=jnp.float32
        )

    def return_row(state):
        step, r, distance = state

        @pl.when((distance == r) & (step >= 0) & (step < 136))
        def _():
            done_s[r] = acc_s[r].astype(jnp.bfloat16)

            @pl.when(r != sp)
            def _():
                pltpu.make_async_remote_copy(
                    src_ref=done_s.at[r], dst_ref=o_ref.at[sp], send_sem=send.at[180 + r],
                    recv_sem=recv.at[180 + sp], device_id={"sp": r, "fs": y, "tp": core}, device_id_type=MESH,
                ).start()

    hooks = ((1, pool_windows), (6, weights_middle), (11, weights_late))

    def steps(masked):
        def body(n, states):
            if not masked:
                for turn, hook in hooks:
                    pl.when(n == turn)(hook)
            states = list(states)
            for unused_step in range(9):
                states.append(advance(states[-1]))
            for u in range(9):
                gather_values(states[u], (u + 2) % 3)
                weigh(states[u + 1], u % 3)
                soften((u + 1) % 3)
                scores(states[u + 3], (u + 2) % 3, masked)
            finished = functools.reduce(
                jnp.logical_or, [distance == r for unused_step, r, distance in states[:9]]
            )

            @pl.when(finished)
            def _():
                for u in range(9):
                    return_row(states[u])

            return tuple(states[9:])

        return body

    first_states = tuple(
        (jnp.int32(step), jnp.int32(0), jnp.int32(0)) for step in (-5, -4, -3, -2)
    )
    states = lax.fori_loop(0, 2, steps(True), first_states)
    mode[0] = "hook"
    lax.fori_loop(0, 14, steps(False), states)
    mode[0] = "start"
    for store in stores:
        store.wait()
    o_ref[sp] = done_s[sp]
    weights_end()
    got(gains_o, 146)
    got(pool_rows.at[1 - core], 96)

    def gain_rows(columns):
        mine_gain = gains_m[0:1, columns].astype(jnp.float32)
        other_gain = gains_o[0:1, columns].astype(jnp.float32)
        low = jnp.where(core == 0, mine_gain, other_gain)
        high = jnp.where(core == 0, other_gain, mine_gain)
        return jnp.concatenate([low, high], axis=1)

    pooled = jnp.concatenate([pool_rows[0], pool_rows[1]], axis=1).astype(jnp.float32)
    factor = lax.rsqrt(jnp.mean(pooled * pooled, axis=1, keepdims=True) + EPS)
    pool_normed = (pooled * factor * gain_rows(slice(0, 256))).astype(jnp.bfloat16)
    for j in range(4):
        acc[j // 2, 256 * (j % 2) : 256 * (j % 2) + 256, :] = jnp.dot(
            pool_normed, wp_all[:, 512 * j : 512 * j + 512], preferred_element_type=jnp.float32
        )

    def settle_row(i, unused):
        r = (sp + i) % BLOCKS
        copy = pltpu.make_async_remote_copy(
            src_ref=done_s.at[r], dst_ref=o_ref.at[r], send_sem=send.at[180 + r],
            recv_sem=recv.at[180 + r], device_id={"sp": r, "fs": y, "tp": core},
            device_id_type=MESH,
        )
        copy.wait_send()
        copy.wait_recv()
        return unused

    lax.fori_loop(1, BLOCKS, settle_row, 0)

    attended = o_ref[...].reshape(HEADS * HEAD_DIM, HALF).astype(jnp.float32).T
    factor = lax.rsqrt(jnp.mean(attended * attended, axis=1, keepdims=True) + EPS)
    attn_normed = (attended * factor * gain_rows(slice(256, 768))).astype(jnp.bfloat16)
    for j in range(4):
        columns = slice(512 * j, 512 * j + 512)
        side = (left_ref, right_ref)[j // 2]
        side[:, 512 * (j % 2) : 512 * (j % 2) + 512] = (
            acc[j // 2, 256 * (j % 2) : 256 * (j % 2) + 256, :]
            + jnp.dot(attn_normed, wa_all[:, columns], preferred_element_type=jnp.float32)
        ).astype(jnp.bfloat16)

    for copy in started:
        copy.wait_send()
    mode[0] = "wait"
    for resend in (pool_swap, weights_middle, weights_late):
        resend()

    def settle_heads(i, unused):
        for a in range(3):
            @pl.when(leaves(i // 2, i % 2))
            def _():
                head_copy(a, i // 2, i % 2, sp).wait_send()

        for a in range(2):
            forward(a, i).wait_send()
        return unused

    lax.fori_loop(0, BLOCKS, settle_heads, 0)


def mixer(*operands):
    vmem = pl.BlockSpec(memory_space=pltpu.VMEM)
    here = pl.BlockSpec(memory_space=pl.ANY)
    return pl.pallas_call(
        mixer_kernel,
        out_shape=(jax.ShapeDtypeStruct((HALF, 1024), jnp.bfloat16),) * 2,
        in_specs=[here, vmem, here, here, here, here, *[vmem] * 5, here, here, vmem, vmem],
        out_specs=(vmem, vmem),
        scratch_shapes=[
            pltpu.VMEM((512, 1024), jnp.bfloat16),
            *[pltpu.VMEM((512, 512), jnp.bfloat16)] * 3,
            pltpu.VMEM((512, 256), jnp.bfloat16),
            pltpu.VMEM((3, 4, 512, 512), jnp.bfloat16),
            pltpu.VMEM((4, 512, 256), jnp.bfloat16),
            pltpu.VMEM((512, 1024), jnp.bfloat16),
            pltpu.VMEM((4, 512, 512), jnp.bfloat16),
            pltpu.VMEM((3, 512, 512), jnp.float32),
            pltpu.VMEM((512, 256), jnp.float32),
            pltpu.VMEM((3, 8, 2, HEAD_DIM, HALF), jnp.bfloat16),
            pltpu.VMEM((512, 256), jnp.bfloat16),
            pltpu.VMEM((16, 256), jnp.bfloat16),
            pltpu.VMEM((512, 256), jnp.bfloat16),
            pltpu.VMEM((2, HALF, 256), jnp.bfloat16),
            pltpu.VMEM((BLOCKS, 3 * HEAD_DIM, HALF), jnp.bfloat16),
            pltpu.VMEM((BLOCKS, 2 * HEAD_DIM, HALF), jnp.bfloat16),
            pltpu.VMEM((BLOCKS, HEAD_DIM, HALF), jnp.bfloat16),
            pltpu.VMEM((512, 2048), jnp.bfloat16),
            pltpu.VMEM((1024, 2048), jnp.bfloat16),
            pltpu.VMEM((16, 768), jnp.bfloat16),
            pltpu.VMEM((16, 768), jnp.bfloat16),
            pltpu.VMEM((8, 128), jnp.float32),
            pltpu.VMEM((8, 128), jnp.float32),
            pltpu.VMEM((BLOCKS, 128, HALF), jnp.bfloat16),
            pltpu.VMEM((BLOCKS, BLOCK, 128), jnp.bfloat16),
            pltpu.VMEM((BLOCKS, HEAD_DIM, BLOCK), jnp.bfloat16),
            pltpu.VMEM((HALF, HALF), jnp.bfloat16),
            pltpu.VMEM((BLOCK, HALF), jnp.float32),
            pltpu.VMEM((BLOCKS + 1, HEAD_DIM, HALF), jnp.float32),
            pltpu.VMEM((BLOCKS + 1, 8, HALF), jnp.float32),
            pltpu.VMEM((BLOCKS, HEAD_DIM, HALF), jnp.bfloat16),
            *[pltpu.VMEM((BLOCK, HALF), jnp.float32)] * 3,
            *[pltpu.VMEM((BLOCK, HALF), jnp.bfloat16)] * 6,
            pltpu.SemaphoreType.DMA((236,)),
            pltpu.SemaphoreType.DMA((236,)),
            pltpu.SemaphoreType.DMA((7,)),
            pltpu.SemaphoreType.REGULAR((4,)),
        ],
        compiler_params=pltpu.CompilerParams(
            collective_id=0, has_side_effects=True, vmem_limit_bytes=62 * 1024 * 1024,
        ),
        cost_estimate=pl.CostEstimate(
            flops=45_000_000_000, bytes_accessed=8_000_000, transcendentals=50_000_000
        ),
        name="token_mixer",
    )(*operands)


def join_kernel(left_ref, right_ref, joined_ref):
    joined_ref[:, :1024] = left_ref[...]
    joined_ref[:, 1024:] = right_ref[...]


def join(left, right):
    side = pl.BlockSpec((HALF, 1024), lambda i: (i, 0))
    return pl.pallas_call(
        join_kernel,
        grid=(1,),
        out_shape=jax.ShapeDtypeStruct((HALF, 2048), jnp.bfloat16),
        in_specs=[side, side],
        out_specs=pl.BlockSpec((HALF, 2048), lambda i: (i, 0)),
        name="join_sides",
    )(left, right)


def shards(
    tokens,
    norm_gain,
    w_pool_in,
    w_query,
    w_key,
    w_value,
    query_gain,
    key_gain,
    stick_offset,
    pool_mix,
    pool_scale,
    pool_gain,
    attn_gain,
    w_out_pool,
    w_out_attn,
):
    left, right = mixer(
        tokens[0], norm_gain.reshape(4, 1, 512), w_key, w_value, w_query, w_pool_in,
        key_gain.reshape(1, HEAD_DIM), query_gain.reshape(1, HEAD_DIM), pool_mix,
        pool_scale.reshape(1, 256), stick_offset.reshape(1, 8), w_out_pool, w_out_attn,
        pool_gain, attn_gain,
    )
    return join(left, right)[None]


def solution(mesh):
    in_specs = (
        P("fs", "sp", "tp"),
        P(),
        P("fs", "tp"),
        P("fs", "tp"),
        P("fs", "tp"),
        P("fs", "tp"),
        P(),
        P(),
        P("tp"),
        P("tp", None, None),
        P("tp"),
        P("tp"),
        P("tp"),
        P("tp", "fs"),
        P("tp", "fs"),
    )
    out_specs = P("fs", ("sp", "tp"), None)
    return jax.shard_map(shards, mesh=mesh, in_specs=in_specs, out_specs=out_specs, check_vma=False)
```
